128 devices in a mesh: sp: 16 (over z, y), tp: 8 (over x, core).
Axes of the slice: x: 4, y: 4, z: 4, core: 2. Of those that a mesh axis runs over, the one named last changes fastest.
Arguments:
- tokens: bfloat16 [16384, 2048], P('sp'), may hold values from -6 to 6
- norm_gain: bfloat16 [2048], replicated, may hold values from 0.099609375 to 1.8984375
- query_weight: bfloat16 [2048, 2048], P(None, 'tp'), may hold values from -0.125 to 0.125
- key_weight: bfloat16 [2048, 512], P(None, 'tp'), may hold values from -0.125 to 0.125
- value_weight: bfloat16 [2048, 512], P(None, 'tp'), may hold values from -0.125 to 0.125
- query_gain: float32 [64], replicated, may hold values from 1 to 14
- key_gain: float32 [64], replicated, may hold values from 1 to 14
- sink_logit: float32 [32], P('tp'), may hold values from 4 to 10
- gate_weight: bfloat16 [2048, 4096], P(None, 'tp'), may hold values from -0.125 to 0.125
- inner_weight: bfloat16 [2048, 4096], P(None, 'tp'), may hold values from -0.125 to 0.125
- input_map: bfloat16 [2048, 1024], P(None, 'tp'), may hold values from -0.125 to 0.125
- output_map: bfloat16 [2048, 1024], P(None, 'tp'), may hold values from -0.125 to 0.125
- step_weight: bfloat16 [2048, 2, 64], P(None, None, 'tp'), may hold values from -0.125 to 0.125
- conv_inner: bfloat16 [5, 4096], P(None, 'tp'), may hold values from -2.5 to 2.5
- conv_pair: bfloat16 [5, 2, 1024], P(None, None, 'tp'), may hold values from -2.5 to 2.5
- decay_rate: float32 [2, 64], P(None, 'tp'), may hold values from 1.8310547e-06 to 0.05
- decay_jump: float32 [16384, 2, 64], P('sp', None, 'tp'), may hold values from -1.4000854 to 0
- inner_gain: bfloat16 [4096], P('tp'), may hold values from 0.099609375 to 1.8984375
- attn_out_weight: bfloat16 [2048, 2048], P('tp'), may hold values from -0.25 to 0.25
- ssm_out_weight: bfloat16 [4096, 2048], P('tp'), may hold values from -0.09375 to 0.09375
Outputs:
- mixed: bfloat16 [16384, 2048], P(('sp', 'tp'))
The draws below stay inside these ranges and needn't reach their ends.
All inputs are finite; a program needn't handle non-finite values.
Results may differ from the reference program's by a relative error of at most 0.025.
The reference program's roundings to bfloat16 on the way count: a program that leaves them out, or rounds other values in their place, can miss the bound.
Values may be sent and summed in bfloat16 or wider, within the bound.
No kernel may reach another device: no remote copies, remote signals or barrier semaphores. Data moves between devices by JAX's collectives and lax.ppermute only.
A program may use at most 128 MiB of HBM per device.

```python
import math
import jax
import jax.numpy as jnp
from jax import lax

MODEL_WIDTH = 2048
HEAD_SIZE = 64
QUERY_HEADS = 32
KEY_HEADS = 8
SSM_INNER = 4096
SSM_GROUPS = 8
STATE_SIZE = 128
CONV_TAPS = 5
WINDOW = 128
BLOCK_ROWS = 256
LOCAL_TOKENS = 1024
DUALITY_CHANNELS = 64
ORDERED_ENTRIES = 16384
N_TP = 8


def draw_query_gain(key, part):
    gain_key = jax.random.fold_in(key, 11)
    return jax.random.uniform(gain_key, (HEAD_SIZE,), jnp.float32, 1.0, 2.0)


def draw_key_gain(key, part):
    gain_key = jax.random.fold_in(key, 17)
    return jax.random.uniform(gain_key, (HEAD_SIZE,), jnp.float32, 1.0, 2.0)


def draw_decay_rate(key, part):
    coin_key, fast_key, slow_key = jax.random.split(jax.random.fold_in(key, 23), 3)
    shape_pair = (2, DUALITY_CHANNELS)
    fast_rate = jnp.exp(jax.random.uniform(fast_key, shape_pair, jnp.float32, math.log(0.015), math.log(0.05)))
    slow_rate = jnp.exp(jax.random.uniform(slow_key, shape_pair, jnp.float32, math.log(0.05 / ORDERED_ENTRIES), math.log(0.3 / ORDERED_ENTRIES)))
    picked = jax.random.bernoulli(coin_key, 0.5, shape_pair)
    return jnp.where(picked, fast_rate, slow_rate)


def draw_decay_jump(key, part):
    pace_key, spot_key, depth_key = jax.random.split(jax.random.fold_in(key, 37), 3)
    columns = 2 * DUALITY_CHANNELS
    blocks = ORDERED_ENTRIES // BLOCK_ROWS
    pace = jax.random.uniform(pace_key, (blocks, 1, columns), jnp.float32, 0.0, 1.4 / ORDERED_ENTRIES)
    increment_matrix_lines = jnp.broadcast_to(pace, (blocks, BLOCK_ROWS, columns)).reshape(ORDERED_ENTRIES, columns)
    drawn_locations = jax.random.randint(spot_key, (2, columns), 0, ORDERED_ENTRIES, dtype=jnp.int32)
    stack_level_count = jnp.log(jax.random.uniform(depth_key, (2, columns), jnp.float32, 0.5, 0.8))
    entry_ordinal = jnp.arange(ORDERED_ENTRIES, dtype=jnp.int32)[:, None]
    cluster_bunches = jnp.where(entry_ordinal == drawn_locations[0][None, :], stack_level_count[0][None, :], 0.0)
    cluster_bunches = cluster_bunches + jnp.where(entry_ordinal == drawn_locations[1][None, :], stack_level_count[1][None, :], 0.0)
    return (cluster_bunches - increment_matrix_lines).reshape(ORDERED_ENTRIES, 2, DUALITY_CHANNELS)


def shard_levels(key, dims, shards, smallest, high):
    loudness, own = 1.0, jax.random.fold_in(key, 6)
    for dim, shards_of in shards:
        draws = jnp.exp(jax.random.uniform(jax.random.fold_in(own, dim), (shards_of,), jnp.float32, smallest / len(shards), high / len(shards)))
        loudness = loudness * jnp.repeat(draws, dims[dim] // shards_of).reshape([-1 if axis == dim else 1 for axis in range(len(dims))])
    return loudness


def bell_draw(key, extent, width, limit, shards=(), kind=jnp.bfloat16):
    values = jax.random.normal(key, extent, jnp.float32) * width
    if len(shards) > 0:
        values = shard_levels(key, extent, shards, -0.22, 0.18) * values
    return jnp.clip(values, min=-limit, max=limit).astype(kind)


def setup_inputs(seed: int = 0) -> dict:
    splits = jax.random.split(jax.random.key(seed), 21)
    return {
        "tokens": bell_draw(splits[0], (ORDERED_ENTRIES, MODEL_WIDTH), 1.0, 6.0, ((0, 16),)),
        "norm_gain": jnp.clip(1.0 + 0.18 * jax.random.normal(splits[1], (MODEL_WIDTH,), jnp.float32), 0.099609375, 1.8984375).astype(jnp.bfloat16),
        "query_weight": bell_draw(splits[2], (MODEL_WIDTH, QUERY_HEADS * HEAD_SIZE), MODEL_WIDTH ** -0.5, 0.125, ((1, 8),)),
        "key_weight": bell_draw(splits[3], (MODEL_WIDTH, KEY_HEADS * HEAD_SIZE), MODEL_WIDTH ** -0.5, 0.125, ((1, 8),)),
        "value_weight": bell_draw(splits[4], (MODEL_WIDTH, KEY_HEADS * HEAD_SIZE), MODEL_WIDTH ** -0.5, 0.125, ((1, 8),)),
        "query_gain": draw_query_gain(jax.random.fold_in(splits[20], 71), 0),
        "key_gain": draw_key_gain(jax.random.fold_in(splits[20], 71), 0),
        "sink_logit": jnp.clip(4.0 + 6.0 * jax.random.uniform(splits[7], (QUERY_HEADS,), jnp.float32) ** shard_levels(splits[7], (QUERY_HEADS,), ((0, 8),), -0.2, 0.2), 4.0, 10.0),
        "gate_weight": bell_draw(splits[8], (MODEL_WIDTH, SSM_INNER), MODEL_WIDTH ** -0.5, 0.125, ((1, 8),)),
        "inner_weight": bell_draw(splits[9], (MODEL_WIDTH, SSM_INNER), MODEL_WIDTH ** -0.5, 0.125, ((1, 8),)),
        "input_map": bell_draw(splits[10], (MODEL_WIDTH, SSM_GROUPS * STATE_SIZE), MODEL_WIDTH ** -0.5, 0.125, ((1, 8),)),
        "output_map": bell_draw(splits[11], (MODEL_WIDTH, SSM_GROUPS * STATE_SIZE), MODEL_WIDTH ** -0.5, 0.125, ((1, 8),)),
        "step_weight": bell_draw(splits[12], (MODEL_WIDTH, 2, DUALITY_CHANNELS), MODEL_WIDTH ** -0.5, 0.125, ((2, 8),)),
        "conv_inner": bell_draw(splits[13], (CONV_TAPS, SSM_INNER), CONV_TAPS ** -0.5, 2.5, ((1, 8),)),
        "conv_pair": bell_draw(splits[14], (CONV_TAPS, 2, SSM_GROUPS * STATE_SIZE), CONV_TAPS ** -0.5, 2.5, ((2, 8),)),
        "decay_rate": draw_decay_rate(jax.random.fold_in(splits[20], 71), 0),
        "decay_jump": draw_decay_jump(jax.random.fold_in(splits[20], 71), 0),
        "inner_gain": jnp.clip(1.0 + 0.18 * jax.random.normal(splits[17], (SSM_INNER,), jnp.float32), 0.099609375, 1.8984375).astype(jnp.bfloat16),
        "attn_out_weight": bell_draw(splits[18], (QUERY_HEADS * HEAD_SIZE, MODEL_WIDTH), (QUERY_HEADS * HEAD_SIZE // 4) ** -0.5, 0.25, ((0, 8),)),
        "ssm_out_weight": bell_draw(splits[19], (SSM_INNER, MODEL_WIDTH), SSM_INNER ** -0.5, 0.09375, ((0, 8),)),
    }


NORM_EPS = 1e-05
ROPE_BASE = 500000.0
NEG_FILL = -1e+30

def rms_rows(values, scales):
    return values * lax.rsqrt(lax.optimization_barrier(jnp.mean(values * values, axis=-1, keepdims=True)) + NORM_EPS) * scales

def rotate(head_rows, positions):
    head_size = head_rows.shape[-1]
    half_size = head_size // 2
    frequency = ROPE_BASE ** (-jnp.arange(0, head_size, 2, dtype=jnp.float32) / head_size)
    angles = positions.astype(jnp.float32)[:, None] * frequency
    cosine = jnp.cos(angles)[:, None, :]
    sine_part = jnp.sin(angles)[:, None, :]
    first_half = head_rows[..., :half_size]
    second_half = head_rows[..., half_size:]
    return jnp.concatenate([first_half * cosine - second_half * sine_part, second_half * cosine + first_half * sine_part], axis=-1)

def attend(query, keyed, value, sink_logit):
    seq_total = query.shape[0]
    group_ratio = QUERY_HEADS // KEY_HEADS
    qblock = 512 if LOCAL_TOKENS % 512 == 0 else LOCAL_TOKENS
    key_reach = qblock + 2 * WINDOW
    rim_pad = ((WINDOW, WINDOW), (0, 0), (0, 0))
    padded_keys = jnp.pad(keyed, rim_pad)
    padded_values = jnp.pad(value, rim_pad)
    sink_table = sink_logit.astype(jnp.float32).reshape(KEY_HEADS, group_ratio)[:, :, None, None]

    def one_block(block_index):
        first_row = block_index * qblock
        block_query = lax.dynamic_slice_in_dim(query, first_row, qblock, 0)
        block_query = block_query.reshape(qblock, KEY_HEADS, group_ratio, HEAD_SIZE)
        key_part = lax.dynamic_slice_in_dim(padded_keys, first_row, key_reach, 0)
        value_part = lax.dynamic_slice_in_dim(padded_values, first_row, key_reach, 0)
        scores = jnp.einsum('qkrd,skd->krqs', block_query.astype(jnp.float32), key_part.astype(jnp.float32)) * HEAD_SIZE ** (-0.5)
        query_pos = first_row + jnp.arange(qblock, dtype=jnp.int32)
        key_pos = first_row - WINDOW + jnp.arange(key_reach, dtype=jnp.int32)
        allowed = (jnp.abs(query_pos[:, None] - key_pos[None, :]) <= WINDOW) & (key_pos[None, :] >= 0) & (key_pos[None, :] < seq_total)
        scores = jnp.where(allowed, scores, NEG_FILL)
        ceiling = jnp.maximum(lax.optimization_barrier(jnp.max(scores, axis=-1, keepdims=True)), sink_table)
        raised = jnp.exp(scores - ceiling)
        weights = raised / (lax.optimization_barrier(jnp.sum(raised, axis=-1, keepdims=True)) + jnp.exp(sink_table - ceiling))
        weights = lax.optimization_barrier(weights.astype(jnp.bfloat16))
        mixed_rows = jnp.einsum('krqs,skd->qkrd', weights.astype(jnp.float32), value_part.astype(jnp.float32))
        return mixed_rows.astype(jnp.bfloat16).reshape(qblock, QUERY_HEADS * HEAD_SIZE)
    blocks_out = lax.map(one_block, jnp.arange(seq_total // qblock, dtype=jnp.int32))
    return blocks_out.reshape(seq_total, QUERY_HEADS * HEAD_SIZE)

def ssd_pass(scaled, log_decay, in_state, out_state):
    seq_total, groups_all, ssm_ratio, head_size = scaled.shape
    state_size = in_state.shape[-1]
    blocks = seq_total // BLOCK_ROWS
    scaled_blocks = scaled.reshape(blocks, BLOCK_ROWS, groups_all, ssm_ratio, head_size)
    decay_blocks = log_decay.reshape(blocks, BLOCK_ROWS, groups_all, ssm_ratio)
    in_blocks = in_state.reshape(blocks, BLOCK_ROWS, groups_all, state_size)
    out_blocks = out_state.reshape(blocks, BLOCK_ROWS, groups_all, state_size)
    row_order = jnp.arange(BLOCK_ROWS)
    lower_mask = row_order[:, None] >= row_order[None, :]
    highest_precision = lax.Precision.HIGHEST

    def advance(carried, block_parts):
        local_scaled, decay_here, local_input, out_here = block_parts
        inside = jnp.cumsum(jnp.transpose(decay_here, (1, 2, 0)), axis=-1)
        weights_in = jnp.exp(jnp.where(lower_mask, inside[..., :, None] - inside[..., None, :], -jnp.inf))
        intersection = jnp.einsum('sgn,tgn->gst', out_here, local_input, precision=highest_precision)
        within = jnp.einsum('gst,grst,tgrp->sgrp', intersection, weights_in, local_scaled, precision=highest_precision)
        across = jnp.einsum('sgn,grpn,grs->sgrp', out_here, carried, jnp.exp(inside), precision=highest_precision)
        remaining_length = jnp.exp(inside[..., -1:] - inside)
        fresh_state = jnp.einsum('dle,lwd,dlwu->lwue', local_input, remaining_length, local_scaled, precision=highest_precision)
        updated = jnp.exp(inside[..., -1])[..., None, None] * carried + fresh_state
        return (updated, within + across)
    start_state = jnp.zeros((groups_all, ssm_ratio, head_size, state_size), jnp.float32)
    unused, outputs = lax.scan(advance, start_state, (scaled_blocks, decay_blocks, in_blocks, out_blocks))
    return outputs.reshape(seq_total, groups_all, ssm_ratio, head_size)

def reference(tokens, norm_gain, query_weight, key_weight, value_weight, query_gain, key_gain, sink_logit, gate_weight, inner_weight, input_map, output_map, step_weight, conv_inner, conv_pair, decay_rate, decay_jump, inner_gain, attn_out_weight, ssm_out_weight):
    seq_total = tokens.shape[0]
    positions = jnp.arange(seq_total, dtype=jnp.int32)
    normed = rms_rows(tokens.astype(jnp.float32), norm_gain.astype(jnp.float32)).astype(jnp.bfloat16)

    def project(weight):
        result = jnp.dot(normed, weight, preferred_element_type=jnp.float32)
        return lax.optimization_barrier(result.astype(jnp.bfloat16))
    query = project(query_weight).reshape(seq_total, QUERY_HEADS, HEAD_SIZE)
    keyed = project(key_weight).reshape(seq_total, KEY_HEADS, HEAD_SIZE)
    value = project(value_weight).reshape(seq_total, KEY_HEADS, HEAD_SIZE)
    query = rotate(rms_rows(query.astype(jnp.float32), query_gain), positions)
    query = lax.optimization_barrier(query.astype(jnp.bfloat16))
    keyed = rotate(rms_rows(keyed.astype(jnp.float32), key_gain), positions)
    keyed = lax.optimization_barrier(keyed.astype(jnp.bfloat16))
    attn_out = attend(query, keyed, value, sink_logit)
    ssm_ratio = DUALITY_CHANNELS // SSM_GROUPS
    gate_rows = project(gate_weight)
    carried_in = jnp.concatenate([project(inner_weight), project(input_map), project(output_map)], axis=1)
    carried_in = carried_in.astype(jnp.float32)
    conv_table = jnp.concatenate([conv_inner, conv_pair.reshape(CONV_TAPS, -1)], axis=1).astype(jnp.float32)
    half_taps = CONV_TAPS // 2
    rimmed = jnp.pad(carried_in, ((half_taps, half_taps), (0, 0)))
    filtered = rimmed[0:seq_total] * conv_table[0]
    for offset in range(1, CONV_TAPS):
        filtered = filtered + rimmed[offset:offset + seq_total] * conv_table[offset]
    activated = jax.nn.silu(filtered)
    map_width = SSM_GROUPS * STATE_SIZE
    signal = activated[:, :SSM_INNER].reshape(seq_total, SSM_GROUPS, ssm_ratio, HEAD_SIZE)
    in_state = activated[:, SSM_INNER:SSM_INNER + map_width].reshape(seq_total, SSM_GROUPS, STATE_SIZE)
    out_state = activated[:, SSM_INNER + map_width:].reshape(seq_total, SSM_GROUPS, STATE_SIZE)
    step_rows = project(step_weight.reshape(MODEL_WIDTH, 2 * DUALITY_CHANNELS))
    step = jax.nn.softplus(step_rows.astype(jnp.float32)).reshape(seq_total, 2, SSM_GROUPS, ssm_ratio)
    log_decay = -decay_rate.reshape(2, SSM_GROUPS, ssm_ratio) * step + decay_jump.reshape(seq_total, 2, SSM_GROUPS, ssm_ratio)
    forward_y = ssd_pass(signal * step[:, 0, :, :, None], log_decay[:, 0], in_state, out_state)
    backward_y = jnp.flip(ssd_pass(jnp.flip(signal * step[:, 1, :, :, None], 0), jnp.flip(log_decay[:, 1], 0), jnp.flip(in_state, 0), jnp.flip(out_state, 0)), 0)
    combined = (forward_y + backward_y).reshape(seq_total, SSM_INNER) * jax.nn.silu(gate_rows.astype(jnp.float32))
    grouped = rms_rows(combined.reshape(seq_total, SSM_GROUPS, -1), 1.0).reshape(seq_total, SSM_INNER)
    ssm_out = (grouped * inner_gain.astype(jnp.float32)).astype(jnp.bfloat16)
    attn_group = QUERY_HEADS * HEAD_SIZE // N_TP
    ssm_group = SSM_INNER // N_TP
    summed = jnp.zeros((seq_total, MODEL_WIDTH), jnp.float32)
    for group_index in range(N_TP):
        attn_cols = attn_out[:, group_index * attn_group:(group_index + 1) * attn_group]
        ssm_cols = ssm_out[:, group_index * ssm_group:(group_index + 1) * ssm_group]
        partial_sum = jnp.dot(attn_cols, attn_out_weight[group_index * attn_group:(group_index + 1) * attn_group], preferred_element_type=jnp.float32)
        partial_sum = partial_sum + jnp.dot(ssm_cols, ssm_out_weight[group_index * ssm_group:(group_index + 1) * ssm_group], preferred_element_type=jnp.float32)
        rounded = lax.optimization_barrier(partial_sum.astype(jnp.bfloat16))
        summed = summed + rounded.astype(jnp.float32)
    return summed.astype(jnp.bfloat16)
```

```python
import jax
import jax.numpy as jnp
import numpy as np
from jax import lax
from jax.experimental import pallas as pl
from jax.experimental.pallas import tpu as pltpu
from jax.sharding import Mesh
from jax.sharding import PartitionSpec as P

SP = ("z", "y")
SP_TP = ("z", "y", "x", "c")
ROWS = 1024
WIDTH = 2048
SEQ = 16384
HEADS = 8
STATE = 128
INNER = 512
CONV = INNER + 2 * STATE
CHUNK = 128
CHUNKS = ROWS // CHUNK
EDGE = 16
WINDOW = 128
HEAD = 64
HALF = 32
QHEADS = 4
LINE = 4
PACK = 2 * STATE + 16

NORM_EPS = 1e-05
ROPE_BASE = 500000.0
NEG_FILL = -1e30
F32 = jnp.float32
BF16 = jnp.bfloat16


def rope_tables():
    frequency = ROPE_BASE ** (-np.arange(0, HEAD, 2, dtype=np.float64) / HEAD)
    offsets = np.arange(-WINDOW, ROWS + WINDOW, dtype=np.float64)
    near = frequency[:, None] * offsets[None, :]
    far = frequency[None, :] * (ROWS * np.arange(SEQ // ROWS, dtype=np.float64))[:, None]
    near_table = np.concatenate([np.cos(near), np.sin(near)], axis=0).astype(np.float32)
    far_table = np.concatenate([np.cos(far), np.sin(far)], axis=1).astype(np.float32)
    return near_table, far_table[:, :, None]


def head_spread():
    spread = np.repeat(np.eye(HEADS, dtype=np.float32), INNER // HEADS, axis=1)
    return np.concatenate([spread, spread], axis=0)


def dot(a, b):
    return jnp.dot(a, b, preferred_element_type=F32)


def dot_nt(a, b):
    return lax.dot_general(a, b, (((1,), (1,)), ((), ())), preferred_element_type=F32)


def dot_tn(a, b):
    return lax.dot_general(a, b, (((0,), (0,)), ((), ())), preferred_element_type=F32)


def silu(v):
    return v * (1.0 / (1.0 + jnp.exp(-v)))


def normalise(tokens, gain):
    t = tokens.astype(F32)
    mean = jnp.mean(t * t, axis=-1, keepdims=True)
    return (t * lax.rsqrt(mean + NORM_EPS) * gain).astype(BF16)


def widen(rows, spread):
    high = rows.astype(BF16)
    low = (rows - high.astype(F32)).astype(BF16)
    return dot_tn(jnp.concatenate([high, low], axis=0), spread)


def front_kernel(
    ids, tok, gain, low, high, w_inner, w_in, w_out, w_step, taps, rate, jump, spread,
    normed_ref, x_ref, b_ref, c_ref, cum_ref, step_ref, run_ref, enter_ref, back_ref, state_ref,
    rows, raw,
):
    i = pl.program_id(0)
    g = gain[...]

    def project(n):
        return [dot(n, w[...]).astype(BF16).astype(F32) for w in (w_inner, w_in, w_out)]

    n = normalise(tok[...], g)
    normed_ref[...] = n
    a, b, c = project(n)
    start = pl.multiple_of(EDGE + i * 256, 16)
    rows[pl.ds(start, 256), :INNER] = a
    rows[pl.ds(start, 256), INNER : INNER + STATE] = b
    rows[pl.ds(start, 256), INNER + STATE :] = c
    raw[:, pl.ds(pl.multiple_of(i * 256, 128), 256)] = dot_nt(w_step[...], n).astype(BF16).astype(F32)

    @pl.when(i == pl.num_programs(0) - 1)
    def _():
        edge = normalise(jnp.concatenate([low[...], high[...]], axis=0), g)
        ea, eb, ec = project(edge)
        for value, lo, hi in ((ea, 0, INNER), (eb, INNER, INNER + STATE), (ec, INNER + STATE, CONV)):
            rows[0:EDGE, lo:hi] = value[:EDGE]
            rows[EDGE + ROWS :, lo:hi] = value[EDGE:]
        v = raw[...]
        step = jnp.maximum(v, 0.0) + jnp.log1p(jnp.exp(-jnp.abs(v)))
        step_ref[...] = step
        decay = jump[...] - rate[...] * step
        lane = lax.broadcasted_iota(jnp.int32, (HEADS, CHUNK), 1)
        cums = []
        for k in range(CHUNKS):
            f = decay[:HEADS, k * CHUNK : (k + 1) * CHUNK]
            r = decay[HEADS:, k * CHUNK : (k + 1) * CHUNK]
            for shift in (1, 2, 4, 8, 16, 32, 64):
                f = f + jnp.where(lane >= shift, pltpu.roll(f, shift, 1), 0.0)
                r = r + jnp.where(lane < CHUNK - shift, pltpu.roll(r, CHUNK - shift, 1), 0.0)
            cums.append((f, r))
            cum_ref[:HEADS, k * CHUNK : (k + 1) * CHUNK] = f
            cum_ref[HEADS:, k * CHUNK : (k + 1) * CHUNK] = r
        totals = [(f[:, CHUNK - 1 :], r[:, :1]) for f, r in cums]
        zero = jnp.zeros((HEADS, 1), F32)
        ahead = zero
        for k in range(CHUNKS):
            run_ref[:HEADS, k * CHUNK : (k + 1) * CHUNK] = cums[k][0] + ahead
            ahead = ahead + totals[k][0]
        behind = zero
        for k in reversed(range(CHUNKS)):
            run_ref[HEADS:, k * CHUNK : (k + 1) * CHUNK] = cums[k][1] + behind
            behind = behind + totals[k][1]
        sp = spread[...]
        state_f = jnp.zeros((STATE, INNER), F32)
        state_b = jnp.zeros((STATE, INNER), F32)
        passed = zero
        for k in range(CHUNKS):
            base = EDGE + k * CHUNK - 2
            acc = rows[base : base + CHUNK, :] * taps[0:1, :]
            for t in range(1, 5):
                acc = acc + rows[base + t : base + t + CHUNK, :] * taps[t : t + 1, :]
            act = silu(acc)
            here = slice(k * CHUNK, (k + 1) * CHUNK)
            x = act[:, :INNER].astype(BF16)
            bm = act[:, INNER : INNER + STATE].astype(BF16)
            x_ref[here, :] = x
            b_ref[here, :] = bm
            c_ref[here, :] = act[:, INNER + STATE :].astype(BF16)
            f, r = cums[k]
            tf, tr = totals[k]
            wf = jnp.exp(tf - f) * step[:HEADS, here]
            wr = jnp.exp(tr - r) * step[HEADS:, here]
            df = jnp.broadcast_to(jnp.exp(tf), (HEADS, CHUNK))
            dr = jnp.broadcast_to(jnp.exp(passed), (HEADS, CHUNK))
            wide = widen(jnp.concatenate([wf, wr, df, dr], axis=1), sp)
            xf = act[:, :INNER]
            fresh_f = dot_tn(bm, (xf * wide[:CHUNK]).astype(BF16))
            fresh_b = dot_tn(bm, (xf * wide[CHUNK : 2 * CHUNK]).astype(BF16))
            enter_ref[k] = state_f.astype(BF16)
            back_ref[k] = fresh_b.astype(BF16)
            state_f = state_f * wide[2 * CHUNK : 3 * CHUNK] + fresh_f
            state_b = state_b + fresh_b * wide[3 * CHUNK :]
            passed = passed + tr
        state_ref[:STATE, :] = state_f.astype(BF16)
        state_ref[STATE : 2 * STATE, :] = state_b.astype(BF16)
        parts = jnp.zeros((HEADS, CHUNK), F32)
        column = 0
        for total in (ahead, passed):
            rest = total
            for _ in range(3):
                piece = rest.astype(BF16).astype(F32)
                rest = rest - piece
                parts = jnp.where(lane == column, piece, parts)
                column += 1
        state_ref[2 * STATE :, :] = dot_tn(parts.astype(BF16), sp[:HEADS]).astype(BF16)[:16]


def logs_of(ref):
    tail = ref[2 * STATE :, :].astype(F32)
    return tail[0:1] + tail[1:2] + tail[2:3], tail[3:4] + tail[4:5] + tail[5:6]


def line_kernel(ids, own, d1, d2, d3, total_ref, part_ref):
    place = ids[2]
    got = (own, d1, d2, d3)
    logs = [logs_of(r) for r in got]
    state = lambda r, back: r[STATE * back : STATE * (back + 1), :].astype(F32)
    out_logs = []
    for back in (0, 1):
        near = (lambda d: d) if back == 0 else (lambda d: LINE - d)
        count = place if back == 0 else LINE - 1 - place
        far_count = LINE - 1 - count
        prefix = jnp.zeros((STATE, INNER), F32)
        log_prefix = jnp.zeros((1, INNER), F32)
        for d in range(1, LINE):
            r = near(d)
            live = d <= count
            weight = jnp.where(live, jnp.exp(log_prefix), 0.0)
            prefix = prefix + weight * state(got[r], back)
            log_prefix = log_prefix + jnp.where(live, logs[r][back], 0.0)
        total = jnp.zeros((STATE, INNER), F32)
        suffix = jnp.zeros((1, INNER), F32)
        for e in reversed(range(1, LINE)):
            r = near(LINE - e)
            live = e <= far_count
            weight = jnp.where(live, jnp.exp(suffix), 0.0)
            total = total + weight * state(got[r], back)
            suffix = suffix + jnp.where(live, logs[r][back], 0.0)
        total = total + jnp.exp(suffix) * state(own, back)
        suffix = suffix + logs[0][back]
        total = total + jnp.exp(suffix) * prefix
        total_ref[STATE * back : STATE * (back + 1), :] = total.astype(BF16)
        part_ref[STATE * back : STATE * (back + 1), :] = prefix
        part_ref[2 * STATE + back : 2 * STATE + back + 1, :] = log_prefix
        out_logs.append(suffix + log_prefix)
    pieces = []
    for total in out_logs:
        rest = total
        for _ in range(3):
            piece = rest.astype(BF16).astype(F32)
            rest = rest - piece
            pieces.append(piece)
    pieces.append(jnp.zeros((10, INNER), F32))
    total_ref[2 * STATE :, :] = jnp.concatenate(pieces, axis=0).astype(BF16)


def attend_kernel(
    ids, sink, normed, low, high, gain, w_q, w_k, w_v, w_g, q_gain, k_gain, near, far,
    gate_ref, attn_ref, qs, ks, vs,
):
    i = pl.program_id(0)
    n = normed[...]
    far_cos = far[0, :HALF, :]
    far_sin = far[0, HALF:, :]

    def turn(head, at, size):
        co = near[:HALF, pl.ds(at, size)]
        so = near[HALF:, pl.ds(at, size)]
        cos = far_cos * co - far_sin * so
        sin = far_sin * co + far_cos * so
        u, w = head[:HALF], head[HALF:]
        return jnp.concatenate([u * cos - w * sin, w * cos + u * sin], axis=0)

    def head_norm(head, scale):
        mean = jnp.mean(head * head, axis=0, keepdims=True)
        return head * lax.rsqrt(mean + NORM_EPS) * scale

    def keys_values(m, at, size):
        k = dot_nt(w_k[...], m).astype(BF16).astype(F32)
        ks[:, pl.ds(at, size)] = turn(head_norm(k, k_gain[...]), at, size).astype(BF16)
        vs[:, pl.ds(at, size)] = dot_nt(w_v[...], m).astype(BF16)

    at = pl.multiple_of(WINDOW + i * 256, 128)
    gate_ref[...] = dot(n, w_g[...]).astype(BF16)
    keys_values(n, at, 256)
    q = dot(n, w_q[...]).astype(BF16).astype(F32).T
    for h in range(QHEADS):
        head = turn(head_norm(q[h * HEAD : (h + 1) * HEAD], q_gain[...]), at, 256)
        qs[h * HEAD : (h + 1) * HEAD, pl.ds(pl.multiple_of(i * 256, 128), 256)] = (
            head.astype(BF16) * jnp.asarray(HEAD**-0.5, BF16)
        )

    @pl.when(i == pl.num_programs(0) - 1)
    def _():
        g = gain[...]
        keys_values(normalise(low[...], g), 0, WINDOW)
        keys_values(normalise(high[...], g), WINDOW + ROWS, WINDOW)
        reach = 3 * WINDOW
        span = QHEADS * WINDOW
        sinks = jnp.concatenate([jnp.full((1, WINDOW), sink[h], F32) for h in range(QHEADS)], axis=1)
        jj = lax.broadcasted_iota(jnp.int32, (reach, span), 0)
        ii = lax.broadcasted_iota(jnp.int32, (reach, span), 1) % WINDOW
        band = (jj >= ii) & (jj <= ii + 2 * WINDOW)
        first = ids[0] * ROWS - WINDOW

        def block(j, _):
            here = pl.multiple_of(j * WINDOW, 128)
            kb = ks[:, pl.ds(here, reach)]
            vb = vs[:, pl.ds(here, reach)]
            qb = jnp.concatenate(
                [qs[h * HEAD : (h + 1) * HEAD, pl.ds(here, WINDOW)] for h in range(QHEADS)], axis=1
            )
            s = dot_tn(kb, qb)
            position = jj + (first + j * WINDOW)
            s = jnp.where(band & (position >= 0) & (position < SEQ), s, NEG_FILL)
            top = jnp.maximum(jnp.max(s, axis=0, keepdims=True), sinks)
            p = jnp.exp(s - top)
            scale = 1.0 / (jnp.sum(p, axis=0, keepdims=True) + jnp.exp(sinks - top))
            o = dot(vb, (p * scale).astype(BF16))
            o = jnp.concatenate(
                [o[:, h * WINDOW : (h + 1) * WINDOW] for h in range(QHEADS)], axis=0
            )
            attn_ref[pl.ds(here, WINDOW), :] = o.T.astype(BF16)
            return 0

        lax.fori_loop(0, ROWS // WINDOW, block, 0)


def mixer_kernel(x_ref, b_ref, c_ref, cum_ref, step_ref, enter_ref, back_ref, spread, y_ref, state):
    @pl.when(pl.program_id(0) == 0)
    def _():
        state[...] = jnp.zeros_like(state)

    x = x_ref[...]
    c = c_ref[...]
    scores = dot_nt(c, b_ref[...])
    cum = cum_ref[...]
    step = step_ref[...]
    f, r = cum[:HEADS], cum[HEADS:]
    sf, sr = step[:HEADS], step[HEADS:]
    row_f = jnp.log(sf) - f
    row_r = jnp.log(sr) - r
    row_d = jnp.log(sf + sr)
    columns = cum.T
    tt = lax.broadcasted_iota(jnp.int32, (CHUNK, CHUNK), 0)
    ss = lax.broadcasted_iota(jnp.int32, (CHUNK, CHUNK), 1)
    below, same = tt > ss, tt == ss
    left = lax.broadcasted_iota(jnp.int32, (CHUNK, CHUNK), 1) < HEAD

    def weights(h):
        lower = columns[:, h : h + 1] + row_f[h : h + 1]
        upper = columns[:, HEADS + h : HEADS + h + 1] + row_r[h : h + 1]
        power = jnp.where(below, lower, jnp.where(same, row_d[h : h + 1], upper))
        return (jnp.exp(power) * scores).astype(BF16)

    wide = widen(jnp.concatenate([jnp.exp(f), jnp.exp(r)], axis=1), spread[...])
    across = wide[:CHUNK] * dot(c, enter_ref[0])
    across = across + wide[CHUNK:] * dot(c, state[...].astype(BF16))
    nothing = jnp.zeros((CHUNK, CHUNK), BF16)
    for pair in range(HEADS // 2):
        cols = slice(pair * 2 * HEAD, (pair + 1) * 2 * HEAD)
        both = jnp.concatenate([weights(2 * pair), weights(2 * pair + 1)], axis=1)
        xp = x[:, cols]
        stacked = jnp.concatenate([jnp.where(left, xp, nothing), jnp.where(left, nothing, xp)], axis=0)
        y_ref[:, cols] = dot(both, stacked) + across[:, cols]
    state[...] = state[...] * wide[CHUNK : CHUNK + 1] + back_ref[0].astype(F32)


def finish_kernel(
    ids, part, d1, d2, d3, y_ref, c_ref, run_ref, gate_ref, attn_ref, gain, spread,
    mine_ref, theirs_ref, from_low, from_high, rows,
):
    @pl.when(pl.program_id(0) == 0)
    def _():
        got = (None, d1, d2, d3)
        for back, keep in ((0, from_low), (1, from_high)):
            count = ids[1] if back == 0 else LINE - 1 - ids[1]
            prefix = jnp.zeros((STATE, INNER), F32)
            log_prefix = jnp.zeros((1, INNER), F32)
            for d in range(1, LINE):
                r = got[d if back == 0 else LINE - d]
                live = d <= count
                weight = jnp.where(live, jnp.exp(log_prefix), 0.0)
                prefix = prefix + weight * r[STATE * back : STATE * (back + 1), :].astype(F32)
                log_prefix = log_prefix + jnp.where(live, logs_of(r)[back], 0.0)
            own = part[STATE * back : STATE * (back + 1), :]
            reach = jnp.exp(part[2 * STATE + back : 2 * STATE + back + 1, :])
            keep[...] = (own + reach * prefix).astype(BF16)

    c = c_ref[...]
    run = jnp.exp(run_ref[...])
    size = c.shape[0]
    wide = widen(jnp.concatenate([run[:HEADS], run[HEADS:]], axis=1), spread[...])
    y = y_ref[...] + wide[:size] * dot(c, from_low[...]) + wide[size:] * dot(c, from_high[...])
    y = y * silu(gate_ref[...].astype(F32))
    mean = jnp.mean(y * y, axis=-1, keepdims=True)
    out = (y * lax.rsqrt(mean + NORM_EPS) * gain[...]).astype(BF16)
    rows[:, : QHEADS * HEAD] = attn_ref[...]
    rows[:, QHEADS * HEAD :] = out
    mine_ref[0] = rows[pl.ds(pl.multiple_of(ids[4] * 128, 128), 128), :]
    theirs_ref[0] = rows[pl.ds(pl.multiple_of((1 - ids[4]) * 128, 128), 128), :]


def project_kernel(ids, mine, theirs, wa, ws, pa, ps, o0, o1, o2, o3):
    split = QHEADS * HEAD

    def partial(v, a, b):
        return (dot(v[:, :split], a[...]) + dot(v[:, split:], b[...])).astype(BF16).astype(F32)

    value = (partial(mine[0], wa, ws) + partial(theirs[0], pa, ps)).astype(BF16)
    for k, ref in enumerate((o0, o1, o2, o3)):

        @pl.when(pl.program_id(0) == k)
        def _(ref=ref):
            ref[...] = value


def fixed(shape):
    return pl.BlockSpec(shape, lambda i, *_: (0,) * len(shape))


def params():
    return pltpu.CompilerParams(dimension_semantics=("arbitrary",), vmem_limit_bytes=56 << 20)


def cost(flops):
    return pl.CostEstimate(flops=int(flops), transcendentals=0, bytes_accessed=8 << 20)


def shaped(shape, dtype):
    return jax.ShapeDtypeStruct(shape, dtype)


def local(
    tokens, norm_gain, query_weight, key_weight, value_weight, query_gain, key_gain, sink_logit,
    gate_weight, inner_weight, input_map, output_map, step_weight, conv_inner, conv_pair,
    decay_rate, decay_jump, inner_gain, attn_out_weight, ssm_out_weight,
):
    ids = jnp.stack(
        [lax.axis_index(SP), lax.axis_index("z"), lax.axis_index("y"), lax.axis_index("x"),
         lax.axis_index("c")]
    ).astype(jnp.int32)
    up = [(k, k + 1) for k in range(15)]
    down = [(k + 1, k) for k in range(15)]
    swap = [(0, 1), (1, 0)]
    edge_low = lax.ppermute(tokens[ROWS - EDGE :], SP, up)
    edge_high = lax.ppermute(tokens[:EDGE], SP, down)
    halo_low = lax.ppermute(tokens[ROWS - WINDOW :], SP, up)
    halo_high = lax.ppermute(tokens[:WINDOW], SP, down)
    attn_partner = lax.ppermute(attn_out_weight, "c", swap)
    ssm_partner = lax.ppermute(ssm_out_weight, "c", swap)

    gain = norm_gain.astype(F32)[None, :]
    taps = jnp.concatenate([conv_inner, conv_pair.reshape(5, -1)], axis=1).astype(F32)
    spread = jnp.asarray(head_spread(), BF16)
    step_rows = jnp.transpose(step_weight, (1, 2, 0)).reshape(2 * HEADS, WIDTH)
    jump = jnp.transpose(decay_jump, (1, 2, 0)).reshape(2 * HEADS, ROWS)
    rate = decay_rate.reshape(2 * HEADS, 1)
    normed, x, b, c, cum, step, run, enter, back, state = pl.pallas_call(
        front_kernel,
        grid_spec=pltpu.PrefetchScalarGridSpec(
            num_scalar_prefetch=1,
            grid=(4,),
            in_specs=[
                pl.BlockSpec((256, WIDTH), lambda i, _: (i, 0)),
                fixed((1, WIDTH)), fixed((EDGE, WIDTH)), fixed((EDGE, WIDTH)),
                fixed((WIDTH, INNER)), fixed((WIDTH, STATE)), fixed((WIDTH, STATE)),
                fixed((2 * HEADS, WIDTH)), fixed((5, CONV)), fixed((2 * HEADS, 1)),
                fixed((2 * HEADS, ROWS)), fixed((2 * HEADS, INNER)),
            ],
            out_specs=[
                pl.BlockSpec((256, WIDTH), lambda i, _: (i, 0)),
                fixed((ROWS, INNER)), fixed((ROWS, STATE)), fixed((ROWS, STATE)),
                fixed((2 * HEADS, ROWS)), fixed((2 * HEADS, ROWS)), fixed((2 * HEADS, ROWS)),
                fixed((CHUNKS, STATE, INNER)), fixed((CHUNKS, STATE, INNER)), fixed((PACK, INNER)),
            ],
            scratch_shapes=[
                pltpu.VMEM((ROWS + 2 * EDGE, CONV), F32),
                pltpu.VMEM((2 * HEADS, ROWS), F32),
            ],
        ),
        out_shape=[
            shaped((ROWS, WIDTH), BF16), shaped((ROWS, INNER), BF16), shaped((ROWS, STATE), BF16),
            shaped((ROWS, STATE), BF16), shaped((2 * HEADS, ROWS), F32),
            shaped((2 * HEADS, ROWS), F32), shaped((2 * HEADS, ROWS), F32),
            shaped((CHUNKS, STATE, INNER), BF16), shaped((CHUNKS, STATE, INNER), BF16),
            shaped((PACK, INNER), BF16),
        ],
        compiler_params=params(),
        cost_estimate=cost(10e9),
        name="front",
    )(ids, tokens, gain, edge_low, edge_high, inner_weight, input_map, output_map, step_rows, taps,
      rate, jump, spread)

    def along(value, axis):
        return [
            lax.ppermute(value, axis, [(k, (k + d) % LINE) for k in range(LINE)]) for d in (1, 2, 3)
        ]

    got = along(state, "y")

    near, far = (jnp.asarray(t) for t in rope_tables())
    gate, attn = pl.pallas_call(
        attend_kernel,
        grid_spec=pltpu.PrefetchScalarGridSpec(
            num_scalar_prefetch=2,
            grid=(4,),
            in_specs=[
                pl.BlockSpec((256, WIDTH), lambda i, *_: (i, 0)),
                fixed((WINDOW, WIDTH)), fixed((WINDOW, WIDTH)), fixed((1, WIDTH)),
                fixed((WIDTH, QHEADS * HEAD)), fixed((HEAD, WIDTH)), fixed((HEAD, WIDTH)),
                fixed((WIDTH, INNER)), fixed((HEAD, 1)), fixed((HEAD, 1)),
                fixed((HEAD, ROWS + 2 * WINDOW)),
                pl.BlockSpec((1, HEAD, 1), lambda i, ids, _: (ids[0], 0, 0)),
            ],
            out_specs=[
                pl.BlockSpec((256, INNER), lambda i, *_: (i, 0)),
                fixed((ROWS, QHEADS * HEAD)),
            ],
            scratch_shapes=[
                pltpu.VMEM((QHEADS * HEAD, ROWS), BF16),
                pltpu.VMEM((HEAD, ROWS + 2 * WINDOW), BF16),
                pltpu.VMEM((HEAD, ROWS + 2 * WINDOW), BF16),
            ],
        ),
        out_shape=[shaped((ROWS, INNER), BF16), shaped((ROWS, QHEADS * HEAD), BF16)],
        compiler_params=params(),
        cost_estimate=cost(12e9),
        name="attend",
    )(ids, sink_logit, normed, halo_low, halo_high, gain, query_weight, key_weight.T, value_weight.T,
      gate_weight, query_gain[:, None], key_gain[:, None], near, far)

    total, part = pl.pallas_call(
        line_kernel,
        grid_spec=pltpu.PrefetchScalarGridSpec(
            num_scalar_prefetch=1,
            grid=(1,),
            in_specs=[fixed((PACK, INNER))] * 4,
            out_specs=[fixed((PACK, INNER)), fixed((PACK, INNER))],
        ),
        out_shape=[shaped((PACK, INNER), BF16), shaped((PACK, INNER), F32)],
        compiler_params=params(),
        name="line",
    )(ids, state, *got)

    far_got = along(total, "z")

    down_by = lambda i, *_: (CHUNKS - 1 - i, 0)
    lanes_by = lambda i, *_: (0, CHUNKS - 1 - i)
    y = pl.pallas_call(
        mixer_kernel,
        grid_spec=pltpu.PrefetchScalarGridSpec(
            num_scalar_prefetch=0,
            grid=(CHUNKS,),
            in_specs=[
                pl.BlockSpec((CHUNK, INNER), down_by), pl.BlockSpec((CHUNK, STATE), down_by),
                pl.BlockSpec((CHUNK, STATE), down_by), pl.BlockSpec((2 * HEADS, CHUNK), lanes_by),
                pl.BlockSpec((2 * HEADS, CHUNK), lanes_by),
                pl.BlockSpec((1, STATE, INNER), lambda i: (CHUNKS - 1 - i, 0, 0)),
                pl.BlockSpec((1, STATE, INNER), lambda i: (CHUNKS - 1 - i, 0, 0)),
                fixed((2 * HEADS, INNER)),
            ],
            out_specs=pl.BlockSpec((CHUNK, INNER), down_by),
            scratch_shapes=[pltpu.VMEM((STATE, INNER), F32)],
        ),
        out_shape=shaped((ROWS, INNER), F32),
        compiler_params=params(),
        cost_estimate=cost(10e9),
        name="mixer",
    )(x, b, c, cum, step, enter, back, spread)

    depth = QHEADS * HEAD + INNER
    mine, theirs = pl.pallas_call(
        finish_kernel,
        grid_spec=pltpu.PrefetchScalarGridSpec(
            num_scalar_prefetch=1,
            grid=(4,),
            in_specs=[
                fixed((PACK, INNER)), fixed((PACK, INNER)), fixed((PACK, INNER)), fixed((PACK, INNER)),
                pl.BlockSpec((256, INNER), lambda i, _: (i, 0)),
                pl.BlockSpec((256, STATE), lambda i, _: (i, 0)),
                pl.BlockSpec((2 * HEADS, 256), lambda i, _: (0, i)),
                pl.BlockSpec((256, INNER), lambda i, _: (i, 0)),
                pl.BlockSpec((256, QHEADS * HEAD), lambda i, _: (i, 0)),
                fixed((1, INNER)), fixed((2 * HEADS, INNER)),
            ],
            out_specs=[pl.BlockSpec((1, 128, depth), lambda i, _: (i, 0, 0))] * 2,
            scratch_shapes=[
                pltpu.VMEM((STATE, INNER), BF16), pltpu.VMEM((STATE, INNER), BF16),
                pltpu.VMEM((256, depth), BF16),
            ],
        ),
        out_shape=[shaped((4, 128, depth), BF16)] * 2,
        compiler_params=params(),
        cost_estimate=cost(4e9),
        name="finish",
    )(ids, part, *far_got, y, c, run, gate, attn, inner_gain.astype(F32)[None, :], spread)

    theirs = lax.ppermute(theirs, "c", swap)
    block = lambda i, ids: ((ids[3] + (i + 1)) % 4, 0, 0)
    one, two, three, own = pl.pallas_call(
        project_kernel,
        grid_spec=pltpu.PrefetchScalarGridSpec(
            num_scalar_prefetch=1,
            grid=(4,),
            in_specs=[
                pl.BlockSpec((1, 128, depth), block), pl.BlockSpec((1, 128, depth), block),
                fixed((QHEADS * HEAD, WIDTH)), fixed((INNER, WIDTH)),
                fixed((QHEADS * HEAD, WIDTH)), fixed((INNER, WIDTH)),
            ],
            out_specs=[fixed((128, WIDTH))] * 4,
        ),
        out_shape=[shaped((128, WIDTH), BF16)] * 4,
        compiler_params=params(),
        cost_estimate=cost(4e9),
        name="project",
    )(ids, mine, theirs, attn_out_weight, ssm_out_weight, attn_partner, ssm_partner)

    result = own.astype(F32)
    for d, value in ((1, one), (2, two), (3, three)):
        sent = lax.ppermute(value, "x", [(k, (k + d) % 4) for k in range(4)])
        result = result + sent.astype(F32)
    return result.astype(BF16)


def solution(mesh):
    split = Mesh(mesh.devices.reshape(4, 4, 4, 2), SP_TP)
    tp = ("x", "c")
    placed = (
        P(SP, None), P(), P(None, tp), P(None, tp), P(None, tp), P(), P(), P(tp),
        P(None, tp), P(None, tp), P(None, tp), P(None, tp), P(None, None, tp), P(None, tp),
        P(None, None, tp), P(None, tp), P(SP, None, tp), P(tp), P(tp, None), P(tp, None),
    )
    return jax.shard_map(
        local, mesh=split, in_specs=placed, out_specs=P(SP_TP, None), check_vma=False
    )
```

```python
import jax
import jax.numpy as jnp
import numpy as np
from jax import lax
from jax.experimental import pallas as pl
from jax.experimental.pallas import tpu as pltpu
from jax.sharding import Mesh
from jax.sharding import PartitionSpec as P

SP = ("z", "y")
SP_TP = ("z", "y", "x", "c")
ROWS = 1024
WIDTH = 2048
SEQ = 16384
HEADS = 8
STATE = 128
INNER = 512
CONV = INNER + 2 * STATE
CHUNK = 128
CHUNKS = ROWS // CHUNK
EDGE = 16
WINDOW = 128
HEAD = 64
HALF = 32
QHEADS = 4
LINE = 4
PACK = 2 * STATE + 16

NORM_EPS = 1e-05
ROPE_BASE = 500000.0
NEG_FILL = -1e30
F32 = jnp.float32
BF16 = jnp.bfloat16


def rope_tables():
    frequency = ROPE_BASE ** (-np.arange(0, HEAD, 2, dtype=np.float64) / HEAD)
    offsets = np.arange(-WINDOW, ROWS + WINDOW, dtype=np.float64)
    near = frequency[:, None] * offsets[None, :]
    far = frequency[None, :] * (ROWS * np.arange(SEQ // ROWS, dtype=np.float64))[:, None]
    near_table = np.concatenate([np.cos(near), np.sin(near)], axis=0).astype(np.float32)
    far_table = np.concatenate([np.cos(far), np.sin(far)], axis=1).astype(np.float32)
    return near_table, far_table[:, None, :]


def head_spread():
    spread = np.repeat(np.eye(HEADS, dtype=np.float32), INNER // HEADS, axis=1)
    return np.concatenate([spread, spread], axis=0)


def dot(a, b):
    return jnp.dot(a, b, preferred_element_type=F32)


def dot_nt(a, b):
    return lax.dot_general(a, b, (((1,), (1,)), ((), ())), preferred_element_type=F32)


def dot_tn(a, b):
    return lax.dot_general(a, b, (((0,), (0,)), ((), ())), preferred_element_type=F32)


def silu(v):
    return v * (1.0 / (1.0 + jnp.exp(-v)))


def normalise(tokens, gain):
    t = tokens.astype(F32)
    mean = jnp.mean(t * t, axis=-1, keepdims=True)
    return (t * lax.rsqrt(mean + NORM_EPS) * gain).astype(BF16)


def lane_row(ref):
    value = ref[...].astype(F32)
    return jnp.concatenate([value[k : k + 1] for k in range(value.shape[0])], axis=1)


def column(row):
    size = row.shape[1]
    a = lax.broadcasted_iota(jnp.int32, (size, size), 0)
    b = lax.broadcasted_iota(jnp.int32, (size, size), 1)
    return jnp.sum(jnp.where(a == b, row, 0.0), axis=1, keepdims=True)


def fetch(pairs, sems):
    copies = [pltpu.make_async_copy(a, b, sems.at[k]) for k, (a, b) in enumerate(pairs)]
    for copy in copies:
        copy.start()
    return copies


def widen(rows, spread):
    high = rows.astype(BF16)
    low = (rows - high.astype(F32)).astype(BF16)
    return dot_tn(jnp.concatenate([high, low], axis=0), spread)


def edge_kernel(tok, low, high, sems):
    pairs = [(tok.at[pl.ds(ROWS - WINDOW, WINDOW)], low), (tok.at[pl.ds(0, WINDOW)], high)]
    for copy in fetch(pairs, sems):
        copy.wait()


BLOCK = 256


def front_kernel(
    gain, tok, h_inner, h_in, h_out, h_gate, h_step, h_q, h_k, h_v, h_attn, h_ssm,
    normed, rows, raw, gate, w_inner, w_in, w_out, w_q, w_kv, w_attn, w_ssm,
    w_gate, w_step, sems,
):
    blocks = [pl.ds(k * BLOCK, BLOCK) for k in range(ROWS // BLOCK)]
    copies = fetch(
        [(tok.at[blocks[0]], normed.at[blocks[0]]), (h_inner, w_inner), (h_in, w_in), (h_out, w_out)]
        + [(tok.at[b], normed.at[b]) for b in blocks[1:]]
        + [
            (h_gate, w_gate), (h_step, w_step), (h_q, w_q), (h_k, w_kv.at[pl.ds(0, HEAD)]),
            (h_v, w_kv.at[pl.ds(HEAD, HEAD)]), (h_attn, w_attn), (h_ssm, w_ssm),
        ],
        sems,
    )
    g = lane_row(gain)
    for i, block in enumerate(blocks):
        copies[0 if i == 0 else 3 + i].wait()
        n = normalise(normed[block, :], g)
        normed[block, :] = n
        if i == 0:
            for k in (1, 2, 3):
                copies[k].wait()
        for k in range(0, INNER, 2 * STATE):
            value = dot(n, w_inner[:, k : k + 2 * STATE]).astype(BF16).astype(F32)
            rows[k // STATE, block, :] = value[:, :STATE]
            rows[k // STATE + 1, block, :] = value[:, STATE:]
        pair = jnp.concatenate([w_in[...], w_out[...]], axis=1)
        value = dot(n, pair).astype(BF16).astype(F32)
        rows[INNER // STATE, block, :] = value[:, :STATE]
        rows[INNER // STATE + 1, block, :] = value[:, STATE:]
        if i == 0:
            copies[7].wait()
            copies[8].wait()
        gate[block, :] = dot(n, w_gate[...]).astype(BF16)
        raw[:, block] = dot_nt(w_step[...], n).astype(BF16).astype(F32)
    for copy in copies[9:]:
        copy.wait()


def state_kernel(
    rate, rows, raw, low, high, gain, w_inner, w_in, w_out, h_inner_taps, h_pair_taps, h_jump, h_spread,
    x_ref, b_ref, c_ref, cum_ref, step_ref, run_ref, enter_ref, back_ref, state_ref, spread,
    first, last, jump, inner_taps, pair_taps, sems,
):
    copies = fetch(
        [(h_jump, jump), (h_spread, spread), (h_inner_taps, inner_taps), (h_pair_taps, pair_taps)], sems
    )
    g = lane_row(gain)
    edge = normalise(jnp.concatenate([low[WINDOW - EDGE :, :], high[:EDGE, :]], axis=0), g)
    for k in range(CONV // STATE):
        if k < INNER // STATE:
            w = w_inner[:, k * STATE : (k + 1) * STATE]
        else:
            w = (w_in if k == INNER // STATE else w_out)[...]
        value = dot(edge, w).astype(BF16).astype(F32)
        first[k, :EDGE, :] = value[:EDGE]
        first[k, EDGE:, :] = rows[k, : CHUNK + EDGE, :]
        last[k, : CHUNK + EDGE, :] = rows[k, ROWS - CHUNK - EDGE :, :]
        last[k, CHUNK + EDGE :, :] = value[EDGE:]
    for copy in copies:
        copy.wait()
    taps = jnp.concatenate(
        [inner_taps[...].astype(F32)] + [pair_taps[:, k, :].astype(F32) for k in (0, 1)], axis=1
    )
    rates = [
        jnp.concatenate([jnp.full((1, CHUNK), rate[d, h], F32) for h in range(HEADS)], axis=0)
        for d in (0, 1)
    ]
    v = raw[...]
    step = jnp.maximum(v, 0.0) + jnp.log1p(jnp.exp(-jnp.abs(v)))
    step_ref[...] = step
    lane = lax.broadcasted_iota(jnp.int32, (HEADS, CHUNK), 1)
    cums = []
    for k in range(CHUNKS):
        at = slice(k * CHUNK, (k + 1) * CHUNK)
        f = jump[:HEADS, at] - rates[0] * step[:HEADS, at]
        r = jump[HEADS:, at] - rates[1] * step[HEADS:, at]
        for shift in (1, 2, 4, 8, 16, 32, 64):
            f = f + jnp.where(lane >= shift, pltpu.roll(f, shift, 1), 0.0)
            r = r + jnp.where(lane < CHUNK - shift, pltpu.roll(r, CHUNK - shift, 1), 0.0)
        cums.append((f, r))
        cum_ref[:HEADS, k * CHUNK : (k + 1) * CHUNK] = f
        cum_ref[HEADS:, k * CHUNK : (k + 1) * CHUNK] = r
    totals = [(f[:, CHUNK - 1 :], r[:, :1]) for f, r in cums]
    zero = jnp.zeros((HEADS, 1), F32)
    ahead = zero
    for k in range(CHUNKS):
        run_ref[:HEADS, k * CHUNK : (k + 1) * CHUNK] = cums[k][0] + ahead
        ahead = ahead + totals[k][0]
    behind = zero
    for k in reversed(range(CHUNKS)):
        run_ref[HEADS:, k * CHUNK : (k + 1) * CHUNK] = cums[k][1] + behind
        behind = behind + totals[k][1]
    sp = spread[...]
    state_f = jnp.zeros((STATE, INNER), F32)
    state_b = jnp.zeros((STATE, INNER), F32)
    passed = zero
    for k in range(CHUNKS):
        if k == 0:
            source, base = first, EDGE - 2
        elif k == CHUNKS - 1:
            source, base = last, EDGE - 2
        else:
            source, base = rows, k * CHUNK - 2
        here = slice(k * CHUNK, (k + 1) * CHUNK)
        act = []
        for lanes in range(CONV // STATE):
            cols = slice(lanes * STATE, (lanes + 1) * STATE)
            acc = source[lanes, base : base + CHUNK, :] * taps[0:1, cols]
            for t in range(1, 5):
                acc = acc + source[lanes, base + t : base + t + CHUNK, :] * taps[t : t + 1, cols]
            act.append(silu(acc))
        bm = act[-2].astype(BF16)
        b_ref[here, :] = bm
        c_ref[here, :] = act[-1].astype(BF16)
        xf = jnp.concatenate(act[:-2], axis=1)
        x_ref[here, :] = xf.astype(BF16)
        f, r = cums[k]
        tf, tr = totals[k]
        wf = jnp.exp(tf - f) * step[:HEADS, here]
        wr = jnp.exp(tr - r) * step[HEADS:, here]
        df = jnp.broadcast_to(jnp.exp(tf), (HEADS, CHUNK))
        dr = jnp.broadcast_to(jnp.exp(passed), (HEADS, CHUNK))
        wide = widen(jnp.concatenate([wf, wr, df, dr], axis=1), sp)
        fresh_f = dot_tn(bm, (xf * wide[:CHUNK]).astype(BF16))
        fresh_b = dot_tn(bm, (xf * wide[CHUNK : 2 * CHUNK]).astype(BF16))
        enter_ref[k] = state_f.astype(BF16)
        back_ref[k] = fresh_b.astype(BF16)
        state_f = state_f * wide[2 * CHUNK : 3 * CHUNK] + fresh_f
        state_b = state_b + fresh_b * wide[3 * CHUNK :]
        passed = passed + tr
    state_ref[:STATE, :] = state_f.astype(BF16)
    state_ref[STATE : 2 * STATE, :] = state_b.astype(BF16)
    parts = jnp.zeros((HEADS, CHUNK), F32)
    column = 0
    for total in (ahead, passed):
        rest = total
        for _ in range(3):
            piece = rest.astype(BF16).astype(F32)
            rest = rest - piece
            parts = jnp.where(lane == column, piece, parts)
            column += 1
    state_ref[2 * STATE :, :] = dot_tn(parts.astype(BF16), sp[:HEADS]).astype(BF16)[:16]


def logs_of(ref):
    tail = ref[2 * STATE :, :].astype(F32)
    return tail[0:1] + tail[1:2] + tail[2:3], tail[3:4] + tail[4:5] + tail[5:6]


def line_kernel(own, d1, d2, d3, m1, m2, m3, part_ref):
    place, level = lax.axis_index("y"), lax.axis_index("z")
    got = (own, d1, d2, d3)
    logs = [logs_of(r) for r in got]
    state = lambda r, back: r[STATE * back : STATE * (back + 1), :].astype(F32)
    totals = []
    for back in (0, 1):
        near = (lambda d: d) if back == 0 else (lambda d: LINE - d)
        count = place if back == 0 else LINE - 1 - place
        far_count = LINE - 1 - count
        prefix = jnp.zeros((STATE, INNER), F32)
        log_prefix = jnp.zeros((1, INNER), F32)
        for d in range(1, LINE):
            r = near(d)
            live = d <= count
            weight = jnp.where(live, jnp.exp(log_prefix), 0.0)
            prefix = prefix + weight * state(got[r], back)
            log_prefix = log_prefix + jnp.where(live, logs[r][back], 0.0)
        total = jnp.zeros((STATE, INNER), F32)
        suffix = jnp.zeros((1, INNER), F32)
        for e in reversed(range(1, LINE)):
            r = near(LINE - e)
            live = e <= far_count
            weight = jnp.where(live, jnp.exp(suffix), 0.0)
            total = total + weight * state(got[r], back)
            suffix = suffix + jnp.where(live, logs[r][back], 0.0)
        total = total + jnp.exp(suffix) * state(own, back)
        suffix = suffix + logs[0][back]
        total = total + jnp.exp(suffix) * prefix
        part_ref[STATE * back : STATE * (back + 1), :] = prefix
        part_ref[2 * STATE + back : 2 * STATE + back + 1, :] = log_prefix
        rest = suffix + log_prefix
        pieces = []
        for _ in range(3):
            piece = rest.astype(BF16).astype(F32)
            rest = rest - piece
            pieces.append(piece)
        pieces.append(jnp.zeros((13, INNER), F32))
        totals.append((total.astype(BF16), jnp.concatenate(pieces, axis=0).astype(BF16)))
    for d, ref in ((1, m1), (2, m2), (3, m3)):
        for back in (0, 1):

            @pl.when(level + d < LINE if back == 0 else level + d >= LINE)
            def _(ref=ref, back=back):
                ref[:STATE, :] = totals[back][0]
                ref[STATE:, :] = totals[back][1]


def heads_kernel(
    normed, low, high, gain, w_q, w_kv, q_row, k_row, h_near, h_far, qs, ks, vs, near, far, sems
):
    copies = fetch([(h_near, near), (h_far.at[lax.axis_index(SP)], far)], sems)
    q_gain, k_gain = column(q_row[...]), column(k_row[...])
    for copy in copies:
        copy.wait()
    turns = column(far[...])
    far_cos = turns[:HALF, :]
    far_sin = turns[HALF:, :]
    scale = jnp.asarray(HEAD**-0.5, BF16)

    def turn(head, at, size):
        co = near[:HALF, at : at + size]
        so = near[HALF:, at : at + size]
        cos = far_cos * co - far_sin * so
        sin = far_sin * co + far_cos * so
        u, w = head[:HALF], head[HALF:]
        return jnp.concatenate([u * cos - w * sin, w * cos + u * sin], axis=0)

    def head_norm(head, scale):
        mean = jnp.mean(head * head, axis=0, keepdims=True)
        return head * lax.rsqrt(mean + NORM_EPS) * scale

    def keys_values(m, at, size):
        kv = dot_nt(w_kv[...], m).astype(BF16)
        k = head_norm(kv[:HEAD].astype(F32), k_gain)
        ks[:, at : at + size] = turn(k, at, size).astype(BF16)
        vs[:, at : at + size] = kv[HEAD:]

    for i in range(4):
        at = WINDOW + i * 256
        n = normed[i * 256 : (i + 1) * 256, :]
        keys_values(n, at, 256)
        q = dot(n, w_q[...]).astype(BF16).astype(F32).T
        for h in range(QHEADS):
            head = turn(head_norm(q[h * HEAD : (h + 1) * HEAD], q_gain), at, 256)
            qs[h * HEAD : (h + 1) * HEAD, i * 256 : (i + 1) * 256] = head.astype(BF16) * scale
    g = lane_row(gain)
    keys_values(normalise(low[...], g), 0, WINDOW)
    keys_values(normalise(high[...], g), WINDOW + ROWS, WINDOW)


def attend_kernel(sink, qs, ks, vs, attn_ref):
    reach = 3 * WINDOW
    span = QHEADS * WINDOW
    sinks = jnp.concatenate([jnp.full((1, WINDOW), sink[h], F32) for h in range(QHEADS)], axis=1)
    jj = lax.broadcasted_iota(jnp.int32, (reach, span), 0)
    ii = lax.broadcasted_iota(jnp.int32, (reach, span), 1) % WINDOW
    band = (jj >= ii) & (jj <= ii + 2 * WINDOW)
    first = lax.axis_index(SP) * ROWS - WINDOW

    def block(j, _):
        here = pl.multiple_of(j * WINDOW, 128)
        kb = ks[:, pl.ds(here, reach)]
        vb = vs[:, pl.ds(here, reach)]
        qb = jnp.concatenate(
            [qs[h * HEAD : (h + 1) * HEAD, pl.ds(here, WINDOW)] for h in range(QHEADS)], axis=1
        )
        s = dot_tn(kb, qb)
        position = jj + (first + j * WINDOW)
        s = jnp.where(band & (position >= 0) & (position < SEQ), s, NEG_FILL)
        top = jnp.maximum(jnp.max(s, axis=0, keepdims=True), sinks)
        p = jnp.exp(s - top)
        scale = 1.0 / (jnp.sum(p, axis=0, keepdims=True) + jnp.exp(sinks - top))
        o = dot(vb, (p * scale).astype(BF16))
        o = jnp.concatenate([o[:, h * WINDOW : (h + 1) * WINDOW] for h in range(QHEADS)], axis=0)
        attn_ref[pl.ds(here, WINDOW), :] = o.T.astype(BF16)
        return 0

    lax.fori_loop(0, ROWS // WINDOW, block, 0)


def mixer_kernel(x_ref, b_ref, c_ref, cum_ref, step_ref, enter_ref, back_ref, spread, y_ref, state):
    @pl.when(pl.program_id(0) == 0)
    def _():
        state[...] = jnp.zeros_like(state)

    x = x_ref[...]
    c = c_ref[...]
    scores = dot_nt(c, b_ref[...])
    cum = cum_ref[...]
    step = step_ref[...]
    f, r = cum[:HEADS], cum[HEADS:]
    sf, sr = step[:HEADS], step[HEADS:]
    row_f = jnp.log(sf) - f
    row_r = jnp.log(sr) - r
    row_d = jnp.log(sf + sr)
    columns = cum.T
    tt = lax.broadcasted_iota(jnp.int32, (CHUNK, CHUNK), 0)
    ss = lax.broadcasted_iota(jnp.int32, (CHUNK, CHUNK), 1)
    below, same = tt > ss, tt == ss
    left = lax.broadcasted_iota(jnp.int32, (CHUNK, CHUNK), 1) < HEAD

    def weights(h):
        lower = columns[:, h : h + 1] + row_f[h : h + 1]
        upper = columns[:, HEADS + h : HEADS + h + 1] + row_r[h : h + 1]
        power = jnp.where(below, lower, jnp.where(same, row_d[h : h + 1], upper))
        return (jnp.exp(power) * scores).astype(BF16)

    wide = widen(jnp.concatenate([jnp.exp(f), jnp.exp(r)], axis=1), spread[...])
    across = wide[:CHUNK] * dot(c, enter_ref[0])
    across = across + wide[CHUNK:] * dot(c, state[...].astype(BF16))
    nothing = jnp.zeros((CHUNK, CHUNK), BF16)
    for pair in range(HEADS // 2):
        cols = slice(pair * 2 * HEAD, (pair + 1) * 2 * HEAD)
        both = jnp.concatenate([weights(2 * pair), weights(2 * pair + 1)], axis=1)
        xp = x[:, cols]
        stacked = jnp.concatenate([jnp.where(left, xp, nothing), jnp.where(left, nothing, xp)], axis=0)
        y_ref[:, cols] = dot(both, stacked) + across[:, cols]
    state[...] = state[...] * wide[CHUNK : CHUNK + 1] + back_ref[0].astype(F32)


def finish_kernel(
    part, d1, d2, d3, y_ref, c_ref, run_ref, gate_ref, attn_ref, gain, spread,
    mine_ref, theirs_ref, from_low, from_high, rows,
):
    @pl.when(pl.program_id(0) == 0)
    def _():
        got = (None, d1, d2, d3)
        for back, keep in ((0, from_low), (1, from_high)):
            level = lax.axis_index("z")
            count = level if back == 0 else LINE - 1 - level
            prefix = jnp.zeros((STATE, INNER), F32)
            log_prefix = jnp.zeros((1, INNER), F32)
            for d in range(1, LINE):
                r = got[d if back == 0 else LINE - d]
                live = d <= count
                weight = jnp.where(live, jnp.exp(log_prefix), 0.0)
                prefix = prefix + weight * r[:STATE, :].astype(F32)
                tail = r[STATE:, :].astype(F32)
                log = tail[0:1] + tail[1:2] + tail[2:3]
                log_prefix = log_prefix + jnp.where(live, log, 0.0)
            own = part[STATE * back : STATE * (back + 1), :]
            reach = jnp.exp(part[2 * STATE + back : 2 * STATE + back + 1, :])
            keep[...] = (own + reach * prefix).astype(BF16)

    c = c_ref[...]
    run = jnp.exp(run_ref[...])
    size = c.shape[0]
    wide = widen(jnp.concatenate([run[:HEADS], run[HEADS:]], axis=1), spread[...])
    y = y_ref[...] + wide[:size] * dot(c, from_low[...]) + wide[size:] * dot(c, from_high[...])
    y = y * silu(gate_ref[...].astype(F32))
    mean = jnp.mean(y * y, axis=-1, keepdims=True)
    out = (y * lax.rsqrt(mean + NORM_EPS) * lane_row(gain)).astype(BF16)
    rows[:, : QHEADS * HEAD] = attn_ref[...]
    rows[:, QHEADS * HEAD :] = out
    core = lax.axis_index("c")
    mine_ref[0] = rows[pl.ds(pl.multiple_of(core * 128, 128), 128), :]
    theirs_ref[0] = rows[pl.ds(pl.multiple_of((1 - core) * 128, 128), 128), :]


def chunk_partial(order, mine, theirs, wa, ws, pa, ps):
    split = QHEADS * HEAD

    def partial(v, a, b):
        return (dot(v[:, :split], a[...]) + dot(v[:, split:], b[...])).astype(BF16).astype(F32)

    join = lambda ref: jnp.concatenate([ref[index] for index in order], axis=0)
    return partial(join(mine), wa, ws) + partial(join(theirs), pa, ps)


HALVES = 64


def opposite_kernel(mine, theirs, wa, ws, pa, ps, right, left):
    index = (lax.axis_index("x") + 2) % LINE
    value = chunk_partial([index], mine, theirs, wa, ws, pa, ps).astype(BF16)
    right[...] = value[:HALVES]
    left[...] = value[HALVES:]


def beside_kernel(mine, theirs, wa, ws, pa, ps, right, left, keep_right, keep_left, own):
    x = lax.axis_index("x")
    order = [(x + 1) % LINE, (x + 3) % LINE, x]
    value = chunk_partial(order, mine, theirs, wa, ws, pa, ps)
    keep_right[...] = value[:HALVES]
    right[...] = value[HALVES : 2 * HALVES].astype(BF16)
    left[...] = value[2 * HALVES : 3 * HALVES].astype(BF16)
    keep_left[...] = value[3 * HALVES : 4 * HALVES]
    own[...] = value[4 * HALVES :]


HBM = pl.BlockSpec(memory_space=pltpu.HBM)


def whole(count):
    return [pl.BlockSpec(memory_space=pltpu.VMEM)] * count


SCALARS = pl.BlockSpec(memory_space=pltpu.SMEM)


def plain(kernel, name, inputs, outs, scalars=0, remote=0, scratch=(), size=8, flops=1e9):
    return pl.pallas_call(
        kernel,
        in_specs=[SCALARS] * scalars + whole(inputs) + [HBM] * remote,
        out_specs=whole(len(outs)),
        out_shape=outs,
        scratch_shapes=list(scratch),
        compiler_params=pltpu.CompilerParams(vmem_limit_bytes=size << 20),
        cost_estimate=cost(flops),
        name=name,
    )


def fixed(shape):
    return pl.BlockSpec(memory_space=pltpu.VMEM)


def params(size):
    return pltpu.CompilerParams(dimension_semantics=("arbitrary",), vmem_limit_bytes=size << 20)


def cost(flops):
    return pl.CostEstimate(flops=int(flops), transcendentals=0, bytes_accessed=8 << 20)


def shaped(shape, dtype):
    return jax.ShapeDtypeStruct(shape, dtype)


def local(
    tokens, norm_gain, query_weight, key_weight, value_weight, query_gain, key_gain, sink_logit,
    gate_weight, inner_weight, input_map, output_map, step_weight, conv_inner, conv_pair,
    decay_rate, decay_jump, inner_gain, attn_out_weight, ssm_out_weight,
):
    up = [(k, k + 1) for k in range(15)]
    down = [(k + 1, k) for k in range(15)]
    swap = [(0, 1), (1, 0)]
    pin = lambda v: pltpu.with_memory_space_constraint(v, pltpu.HBM)
    edge_low, edge_high = plain(
        edge_kernel, "edge", 0, [shaped((WINDOW, WIDTH), BF16)] * 2, remote=1,
        scratch=[pltpu.SemaphoreType.DMA((2,))], size=2, flops=1e6,
    )(pin(tokens))
    halo_low = lax.ppermute(edge_low, SP, up)
    halo_high = lax.ppermute(edge_high, SP, down)
    attn_partner = lax.ppermute(attn_out_weight, "c", swap)
    ssm_partner = lax.ppermute(ssm_out_weight, "c", swap)

    gain = norm_gain.reshape(WIDTH // 128, 128)
    spread = jnp.asarray(head_spread(), BF16)
    step_rows = jnp.transpose(step_weight, (1, 2, 0)).reshape(2 * HEADS, WIDTH)
    jump = jnp.transpose(decay_jump, (1, 2, 0)).reshape(2 * HEADS, ROWS)
    normed, rows, raw, gate, w_inner, w_in, w_out, w_q, w_kv, w_attn, w_ssm = plain(
        front_kernel, "front", 1,
        [
            shaped((ROWS, WIDTH), BF16), shaped((CONV // STATE, ROWS, STATE), F32),
            shaped((2 * HEADS, ROWS), F32), shaped((ROWS, INNER), BF16),
            shaped((WIDTH, INNER), BF16), shaped((WIDTH, STATE), BF16), shaped((WIDTH, STATE), BF16),
            shaped((WIDTH, QHEADS * HEAD), BF16), shaped((2 * HEAD, WIDTH), BF16),
            shaped((QHEADS * HEAD, WIDTH), BF16), shaped((INNER, WIDTH), BF16),
        ],
        remote=11,
        scratch=[
            pltpu.VMEM((WIDTH, INNER), BF16), pltpu.VMEM((2 * HEADS, WIDTH), BF16),
            pltpu.SemaphoreType.DMA((14,)),
        ],
        size=8, flops=10e9,
    )(gain, *map(pin, (tokens, inner_weight, input_map, output_map, gate_weight, step_rows, query_weight,
      key_weight.T, value_weight.T, attn_out_weight, ssm_out_weight)))

    x, b, c, cum, step, run, enter, back, state, spread = plain(
        state_kernel, "state", 8,
        [
            shaped((ROWS, INNER), BF16), shaped((ROWS, STATE), BF16),
            shaped((ROWS, STATE), BF16), shaped((2 * HEADS, ROWS), F32),
            shaped((2 * HEADS, ROWS), F32), shaped((2 * HEADS, ROWS), F32),
            shaped((CHUNKS, STATE, INNER), BF16), shaped((CHUNKS, STATE, INNER), BF16),
            shaped((PACK, INNER), BF16), shaped((2 * HEADS, INNER), BF16),
        ],
        scalars=1, remote=4,
        scratch=[pltpu.VMEM((CONV // STATE, CHUNK + 2 * EDGE, STATE), F32)] * 2
        + [
            pltpu.VMEM((2 * HEADS, ROWS), F32), pltpu.VMEM((5, INNER), BF16),
            pltpu.VMEM((5, 2, STATE), BF16), pltpu.SemaphoreType.DMA((4,)),
        ],
        size=8, flops=6e9,
    )(decay_rate, rows, raw, halo_low, halo_high, gain, w_inner, w_in, w_out, conv_inner, conv_pair,
      jump, spread)

    def along(values, axis):
        return [
            lax.ppermute(value, axis, [(k, (k + d) % LINE) for k in range(LINE)])
            for d, value in zip((1, 2, 3), values)
        ]

    got = along([state] * 3, "y")

    near, far = rope_tables()
    qs, ks, vs = plain(
        heads_kernel, "heads", 8,
        [
            shaped((QHEADS * HEAD, ROWS), BF16), shaped((HEAD, ROWS + 2 * WINDOW), BF16),
            shaped((HEAD, ROWS + 2 * WINDOW), BF16),
        ],
        remote=2,
        scratch=[
            pltpu.VMEM((HEAD, ROWS + 2 * WINDOW), F32), pltpu.VMEM((1, HEAD), F32),
            pltpu.SemaphoreType.DMA((2,)),
        ],
        size=6, flops=5e9,
    )(normed, halo_low, halo_high, gain, w_q, w_kv, query_gain[None, :], key_gain[None, :],
      jnp.asarray(near), jnp.asarray(far))

    *messages, part = plain(
        line_kernel, "line", 4,
        [shaped((STATE + 16, INNER), BF16)] * 3 + [shaped((PACK, INNER), F32)],
        size=4, flops=1e9,
    )(state, *got)

    far_got = along(messages, "z")

    attn = plain(
        attend_kernel, "attend", 3, [shaped((ROWS, QHEADS * HEAD), BF16)], scalars=1, size=8,
        flops=7e9,
    )(sink_logit, qs, ks, vs)[0]

    down_by = lambda i, *_: (CHUNKS - 1 - i, 0)
    lanes_by = lambda i, *_: (0, CHUNKS - 1 - i)
    y = pl.pallas_call(
        mixer_kernel,
        grid_spec=pltpu.PrefetchScalarGridSpec(
            num_scalar_prefetch=0,
            grid=(CHUNKS,),
            in_specs=[
                pl.BlockSpec((CHUNK, INNER), down_by), pl.BlockSpec((CHUNK, STATE), down_by),
                pl.BlockSpec((CHUNK, STATE), down_by), pl.BlockSpec((2 * HEADS, CHUNK), lanes_by),
                pl.BlockSpec((2 * HEADS, CHUNK), lanes_by),
                pl.BlockSpec((1, STATE, INNER), lambda i: (CHUNKS - 1 - i, 0, 0)),
                pl.BlockSpec((1, STATE, INNER), lambda i: (CHUNKS - 1 - i, 0, 0)),
                fixed((2 * HEADS, INNER)),
            ],
            out_specs=pl.BlockSpec((CHUNK, INNER), down_by),
            scratch_shapes=[pltpu.VMEM((STATE, INNER), F32)],
        ),
        out_shape=shaped((ROWS, INNER), F32),
        compiler_params=params(6),
        cost_estimate=cost(10e9),
        name="mixer",
    )(x, b, c, cum, step, enter, back, spread)

    depth = QHEADS * HEAD + INNER
    mine, theirs = pl.pallas_call(
        finish_kernel,
        grid=(4,),
        in_specs=whole(4) + [
            pl.BlockSpec((256, INNER), lambda i: (i, 0)),
            pl.BlockSpec((256, STATE), lambda i: (i, 0)),
            pl.BlockSpec((2 * HEADS, 256), lambda i: (0, i)),
            pl.BlockSpec((256, INNER), lambda i: (i, 0)),
            pl.BlockSpec((256, QHEADS * HEAD), lambda i: (i, 0)),
        ] + whole(2),
        out_specs=[pl.BlockSpec((1, 128, depth), lambda i: (i, 0, 0))] * 2,
        scratch_shapes=[
            pltpu.VMEM((STATE, INNER), BF16), pltpu.VMEM((STATE, INNER), BF16),
            pltpu.VMEM((256, depth), BF16),
        ],
        out_shape=[shaped((4, 128, depth), BF16)] * 2,
        compiler_params=params(8),
        cost_estimate=cost(4e9),
        name="finish",
    )(part, *far_got, y, c, run, gate, attn, inner_gain.reshape(INNER // 128, 128), spread)

    theirs = lax.ppermute(theirs, "c", swap)
    operands = (
        mine, theirs, w_attn, w_ssm, attn_partner, ssm_partner
    )
    sent = shaped((HALVES, WIDTH), BF16)
    kept = shaped((HALVES, WIDTH), F32)
    right = [(k, (k + 1) % LINE) for k in range(LINE)]
    left = [((k + 1) % LINE, k) for k in range(LINE)]
    shift_right = lambda value: lax.ppermute(value, "x", right)
    shift_left = lambda value: lax.ppermute(value, "x", left)
    relay_right, relay_left = plain(
        opposite_kernel, "opposite", 6, [sent, sent], flops=1e9
    )(*operands)
    relay_right = shift_right(relay_right)
    relay_left = shift_left(relay_left)
    direct_right, direct_left, keep_right, keep_left, own = plain(
        beside_kernel, "beside", 6, [sent, sent, kept, kept, shaped((2 * HALVES, WIDTH), F32)],
        flops=3e9,
    )(*operands)
    direct_right = shift_right(direct_right)
    direct_left = shift_left(direct_left)
    last_right = shift_right((keep_right + relay_right.astype(F32)).astype(BF16))
    last_left = shift_left((keep_left + relay_left.astype(F32)).astype(BF16))
    upper = own[:HALVES] + direct_left.astype(F32) + last_right.astype(F32)
    lower = own[HALVES:] + direct_right.astype(F32) + last_left.astype(F32)
    return jnp.concatenate([upper, lower], axis=0).astype(BF16)


def solution(mesh):
    split = Mesh(mesh.devices.reshape(4, 4, 4, 2), SP_TP)
    tp = ("x", "c")
    placed = (
        P(SP, None), P(), P(None, tp), P(None, tp), P(None, tp), P(), P(), P(tp),
        P(None, tp), P(None, tp), P(None, tp), P(None, tp), P(None, None, tp), P(None, tp),
        P(None, None, tp), P(None, tp), P(SP, None, tp), P(tp), P(tp, None), P(tp, None),
    )
    return jax.shard_map(
        local, mesh=split, in_specs=placed, out_specs=P(SP_TP, None), check_vma=False
    )
```

```python
import jax
import jax.numpy as jnp
import numpy as np
from jax import lax
from jax.experimental import pallas as pl
from jax.experimental.pallas import tpu as pltpu
from jax.sharding import Mesh
from jax.sharding import PartitionSpec as P

SP = ("z", "y")
SP_TP = ("z", "y", "x", "c")
ROWS = 1024
WIDTH = 2048
SEQ = 16384
HEADS = 8
STATE = 128
INNER = 512
CONV = INNER + 2 * STATE
CHUNK = 128
CHUNKS = ROWS // CHUNK
EDGE = 16
WINDOW = 128
HEAD = 64
HALF = 32
QHEADS = 4
LINE = 4
PACK = 2 * STATE + 16

NORM_EPS = 1e-05
ROPE_BASE = 500000.0
NEG_FILL = -1e30
F32 = jnp.float32
BF16 = jnp.bfloat16


def rope_tables():
    frequency = ROPE_BASE ** (-np.arange(0, HEAD, 2, dtype=np.float64) / HEAD)
    offsets = np.arange(-WINDOW, ROWS + WINDOW, dtype=np.float64)
    near = frequency[:, None] * offsets[None, :]
    far = frequency[None, :] * (ROWS * np.arange(SEQ // ROWS, dtype=np.float64))[:, None]
    near_table = np.concatenate([np.cos(near), np.sin(near)], axis=0).astype(np.float32)
    far_table = np.concatenate([np.cos(far), np.sin(far)], axis=1).astype(np.float32)
    return near_table, far_table[:, None, :]


def head_spread():
    spread = np.repeat(np.eye(HEADS, dtype=np.float32), INNER // HEADS, axis=1)
    return np.concatenate([spread, spread], axis=0)


def dot(a, b):
    return jnp.dot(a, b, preferred_element_type=F32)


def dot_nt(a, b):
    return lax.dot_general(a, b, (((1,), (1,)), ((), ())), preferred_element_type=F32)


def dot_tn(a, b):
    return lax.dot_general(a, b, (((0,), (0,)), ((), ())), preferred_element_type=F32)


def silu(v):
    half = 0.5 * v
    return half + half * jnp.tanh(half)


def normalise(tokens, gain):
    t = tokens.astype(F32)
    mean = jnp.mean(t * t, axis=-1, keepdims=True)
    return (t * lax.rsqrt(mean + NORM_EPS) * gain).astype(BF16)


def lane_row(ref):
    value = ref[...].astype(F32)
    return jnp.concatenate([value[k : k + 1] for k in range(value.shape[0])], axis=1)


def column(row):
    size = row.shape[1]
    a = lax.broadcasted_iota(jnp.int32, (size, size), 0)
    b = lax.broadcasted_iota(jnp.int32, (size, size), 1)
    return jnp.sum(jnp.where(a == b, row, 0.0), axis=1, keepdims=True)


def fetch(pairs, sems):
    copies = [pltpu.make_async_copy(a, b, sems.at[k]) for k, (a, b) in enumerate(pairs)]
    for copy in copies:
        copy.start()
    return copies


def widen(rows, spread):
    high = rows.astype(BF16)
    low = (rows - high.astype(F32)).astype(BF16)
    return dot_tn(jnp.concatenate([high, low], axis=0), spread)


def edge_kernel(h_gain, tok, h_k, h_v, low, high, edge, w_kv, gain, sems):
    copies = fetch(
        [
            (tok.at[pl.ds(ROWS - WINDOW, WINDOW)], edge.at[pl.ds(0, WINDOW)]),
            (tok.at[pl.ds(0, WINDOW)], edge.at[pl.ds(WINDOW, WINDOW)]),
            (h_k, w_kv.at[pl.ds(0, HEAD)]), (h_v, w_kv.at[pl.ds(HEAD, HEAD)]), (h_gain, gain),
        ],
        sems,
    )
    for copy in copies:
        copy.wait()
    g = lane_row(gain)
    kv = dot_nt(w_kv[...], normalise(edge[...], g)).astype(BF16)
    for ref, at, rows in ((low, 0, WINDOW - EDGE), (high, WINDOW, WINDOW)):
        ref[:EDGE, :] = edge[rows : rows + EDGE, :]
        for k in range(WIDTH // 128):
            ref[EDGE:, k * 128 : (k + 1) * 128] = kv[k * 8 : (k + 1) * 8, at : at + WINDOW]


BLOCK = 256


def front_kernel(
    gain, w_inner, w_in, w_out, tok, h_step, h_gate, h_q, h_k, h_v,
    normed, rows, raw, w_gate, w_q, w_kv, w_step, sems,
):
    blocks = [pl.ds(k * BLOCK, BLOCK) for k in range(ROWS // BLOCK)]
    waits = fetch(
        [(h_step, w_step)], sems
    )
    late = [
        pltpu.make_async_copy(a, b, sems.at[5 + k])
        for k, (a, b) in enumerate(
            [
                (h_gate, w_gate), (h_q, w_q), (h_k, w_kv.at[pl.ds(0, HEAD)]),
                (h_v, w_kv.at[pl.ds(HEAD, HEAD)]),
            ]
        )
    ]
    g = lane_row(gain)

    def prepare(i):
        normed[blocks[i], :] = normalise(tok[blocks[i], :], g)

    prepare(0)
    waits[0].wait()
    pair = jnp.concatenate([w_in[...], w_out[...]], axis=1)
    for i, block in enumerate(blocks):
        if i + 1 < len(blocks):
            prepare(i + 1)
        if i == 1:
            for copy in late:
                copy.start()
        n = normed[block, :]
        for k in range(0, INNER, 2 * STATE):
            value = dot(n, w_inner[:, k : k + 2 * STATE]).astype(BF16).astype(F32)
            rows[k // STATE, block, :] = value[:, :STATE]
            rows[k // STATE + 1, block, :] = value[:, STATE:]
        value = dot(n, pair).astype(BF16).astype(F32)
        rows[INNER // STATE, block, :] = value[:, :STATE]
        rows[INNER // STATE + 1, block, :] = value[:, STATE:]
        raw[:, block] = dot_nt(w_step[...], n).astype(BF16).astype(F32)
    for copy in late:
        copy.wait()


def state_kernel(
    rate, rows, raw, low, high, gain, w_inner, w_in, w_out, h_inner_taps, h_pair_taps, h_jump, h_spread,
    x_ref, b_ref, c_ref, cum_ref, step_ref, run_ref, enter_ref, back_ref, state_ref, spread,
    first, last, state_f, state_b, jump, inner_taps, pair_taps, sems,
):
    copies = fetch(
        [(h_jump, jump), (h_spread, spread), (h_inner_taps, inner_taps), (h_pair_taps, pair_taps)], sems
    )
    g = lane_row(gain)
    edge = normalise(jnp.concatenate([low[:EDGE, :], high[:EDGE, :]], axis=0), g)
    for k in range(CONV // STATE):
        if k < INNER // STATE:
            w = w_inner[:, k * STATE : (k + 1) * STATE]
        else:
            w = (w_in if k == INNER // STATE else w_out)[...]
        value = dot(edge, w).astype(BF16).astype(F32)
        first[k, :EDGE, :] = value[:EDGE]
        first[k, EDGE:, :] = rows[k, : CHUNK + EDGE, :]
        last[k, : CHUNK + EDGE, :] = rows[k, ROWS - CHUNK - EDGE :, :]
        last[k, CHUNK + EDGE :, :] = value[EDGE:]
    for copy in copies:
        copy.wait()
    taps = jnp.concatenate(
        [inner_taps[...].astype(F32)] + [pair_taps[:, k, :].astype(F32) for k in (0, 1)], axis=1
    )
    rates = [
        jnp.concatenate([jnp.full((1, CHUNK), rate[d, h], F32) for h in range(HEADS)], axis=0)
        for d in (0, 1)
    ]
    v = raw[...]
    step = jnp.maximum(v, 0.0) + jnp.log1p(jnp.exp(-jnp.abs(v)))
    step_ref[...] = step
    lane = lax.broadcasted_iota(jnp.int32, (HEADS, CHUNK), 1)
    cums = []
    for k in range(CHUNKS):
        at = slice(k * CHUNK, (k + 1) * CHUNK)
        f = jump[:HEADS, at] - rates[0] * step[:HEADS, at]
        r = jump[HEADS:, at] - rates[1] * step[HEADS:, at]
        for shift in (1, 2, 4, 8, 16, 32, 64):
            f = f + jnp.where(lane >= shift, pltpu.roll(f, shift, 1), 0.0)
            r = r + jnp.where(lane < CHUNK - shift, pltpu.roll(r, CHUNK - shift, 1), 0.0)
        cums.append((f, r))
        cum_ref[:HEADS, k * CHUNK : (k + 1) * CHUNK] = f
        cum_ref[HEADS:, k * CHUNK : (k + 1) * CHUNK] = r
    totals = [(f[:, CHUNK - 1 :], r[:, :1]) for f, r in cums]
    zero = jnp.zeros((HEADS, 1), F32)
    ahead = zero
    for k in range(CHUNKS):
        run_ref[:HEADS, k * CHUNK : (k + 1) * CHUNK] = cums[k][0] + ahead
        ahead = ahead + totals[k][0]
    behind = zero
    for k in reversed(range(CHUNKS)):
        run_ref[HEADS:, k * CHUNK : (k + 1) * CHUNK] = cums[k][1] + behind
        behind = behind + totals[k][1]
    sp = spread[...]
    state_f[...] = jnp.zeros_like(state_f)
    state_b[...] = jnp.zeros_like(state_b)
    passed = zero
    for k in range(CHUNKS):
        if k == 0:
            source, base = first, EDGE - 2
        elif k == CHUNKS - 1:
            source, base = last, EDGE - 2
        else:
            source, base = rows, k * CHUNK - 2
        here = slice(k * CHUNK, (k + 1) * CHUNK)

        def active(tile):
            cols = slice(tile * STATE, (tile + 1) * STATE)
            acc = source[tile, base : base + CHUNK, :] * taps[0:1, cols]
            for t in range(1, 5):
                acc = acc + source[tile, base + t : base + t + CHUNK, :] * taps[t : t + 1, cols]
            return silu(acc)

        f, r = cums[k]
        tf, tr = totals[k]
        wf = jnp.exp(tf - f) * step[:HEADS, here]
        wr = jnp.exp(tr - r) * step[HEADS:, here]
        df = jnp.where(lane == 0, jnp.exp(tf), jnp.exp(passed))
        bm = active(INNER // STATE).astype(BF16)
        b_ref[here, :] = bm
        c_ref[here, :] = active(INNER // STATE + 1).astype(BF16)
        xf = jnp.concatenate([active(tile) for tile in range(INNER // STATE)], axis=1)
        x_ref[here, :] = xf.astype(BF16)
        wide = widen(jnp.concatenate([wf, wr, df], axis=1), sp)
        fresh_f = dot_tn(bm, (xf * wide[:CHUNK]).astype(BF16))
        fresh_b = dot_tn(bm, (xf * wide[CHUNK : 2 * CHUNK]).astype(BF16))
        enter_ref[k] = state_f[...].astype(BF16)
        back_ref[k] = fresh_b.astype(BF16)
        state_f[...] = state_f[...] * wide[2 * CHUNK : 2 * CHUNK + 1] + fresh_f
        state_b[...] = state_b[...] + fresh_b * wide[2 * CHUNK + 1 : 2 * CHUNK + 2]
        passed = passed + tr
    state_ref[:STATE, :] = state_f[...].astype(BF16)
    state_ref[STATE : 2 * STATE, :] = state_b[...].astype(BF16)
    parts = jnp.zeros((HEADS, CHUNK), F32)
    column = 0
    for total in (ahead, passed):
        rest = total
        for _ in range(3):
            piece = rest.astype(BF16).astype(F32)
            rest = rest - piece
            parts = jnp.where(lane == column, piece, parts)
            column += 1
    state_ref[2 * STATE :, :] = dot_tn(parts.astype(BF16), sp[:HEADS]).astype(BF16)[:16]


def logs_of(ref):
    tail = ref[2 * STATE :, :].astype(F32)
    return tail[0:1] + tail[1:2] + tail[2:3], tail[3:4] + tail[4:5] + tail[5:6]


def line_kernel(own, d1, d2, d3, m1, m2, m3, part_ref):
    place, level = lax.axis_index("y"), lax.axis_index("z")
    got = (own, d1, d2, d3)
    logs = [logs_of(r) for r in got]
    state = lambda r, back: r[STATE * back : STATE * (back + 1), :].astype(F32)
    totals = []
    for back in (0, 1):
        near = (lambda d: d) if back == 0 else (lambda d: LINE - d)
        count = place if back == 0 else LINE - 1 - place
        far_count = LINE - 1 - count
        prefix = jnp.zeros((STATE, INNER), F32)
        log_prefix = jnp.zeros((1, INNER), F32)
        for d in range(1, LINE):
            r = near(d)
            live = d <= count
            weight = jnp.where(live, jnp.exp(log_prefix), 0.0)
            prefix = prefix + weight * state(got[r], back)
            log_prefix = log_prefix + jnp.where(live, logs[r][back], 0.0)
        total = jnp.zeros((STATE, INNER), F32)
        suffix = jnp.zeros((1, INNER), F32)
        for e in reversed(range(1, LINE)):
            r = near(LINE - e)
            live = e <= far_count
            weight = jnp.where(live, jnp.exp(suffix), 0.0)
            total = total + weight * state(got[r], back)
            suffix = suffix + jnp.where(live, logs[r][back], 0.0)
        total = total + jnp.exp(suffix) * state(own, back)
        suffix = suffix + logs[0][back]
        total = total + jnp.exp(suffix) * prefix
        part_ref[STATE * back : STATE * (back + 1), :] = prefix
        part_ref[2 * STATE + back : 2 * STATE + back + 1, :] = log_prefix
        rest = suffix + log_prefix
        pieces = []
        for _ in range(3):
            piece = rest.astype(BF16).astype(F32)
            rest = rest - piece
            pieces.append(piece)
        pieces.append(jnp.zeros((13, INNER), F32))
        totals.append((total.astype(BF16), jnp.concatenate(pieces, axis=0).astype(BF16)))
    for d, ref in ((1, m1), (2, m2), (3, m3)):
        for back in (0, 1):

            @pl.when(level + d < LINE if back == 0 else level + d >= LINE)
            def _(ref=ref, back=back):
                ref[:STATE, :] = totals[back][0]
                ref[STATE:, :] = totals[back][1]


def heads_kernel(
    normed, low, high, w_gate, w_q, w_kv, q_row, k_row, h_near, h_far, gate, qs, ks, vs, near, far, sems
):
    copies = fetch([(h_near, near), (h_far.at[lax.axis_index(SP)], far)], sems)
    q_gain, k_gain = column(q_row[...]), column(k_row[...])
    for copy in copies:
        copy.wait()
    turns = column(far[...])
    far_cos = turns[:HALF, :]
    far_sin = turns[HALF:, :]
    scale = jnp.asarray(HEAD**-0.5, BF16)

    def turn(head, at, size):
        co = near[:HALF, at : at + size]
        so = near[HALF:, at : at + size]
        cos = far_cos * co - far_sin * so
        sin = far_sin * co + far_cos * so
        u, w = head[:HALF], head[HALF:]
        return jnp.concatenate([u * cos - w * sin, w * cos + u * sin], axis=0)

    def head_norm(head, scale):
        mean = jnp.mean(head * head, axis=0, keepdims=True)
        return head * lax.rsqrt(mean + NORM_EPS) * scale

    def keys_values(kv, at, size):
        k = head_norm(kv[:HEAD].astype(F32), k_gain)
        ks[:, at : at + size] = turn(k, at, size).astype(BF16)
        vs[:, at : at + size] = kv[HEAD:]

    for i in range(4):
        at = WINDOW + i * 256
        n = normed[i * 256 : (i + 1) * 256, :]
        keys_values(dot_nt(w_kv[...], n).astype(BF16), at, 256)
        gate[i * 256 : (i + 1) * 256, :] = dot(n, w_gate[...]).astype(BF16)
        q = dot(n, w_q[...]).astype(BF16).astype(F32).T
        for h in range(QHEADS):
            head = turn(head_norm(q[h * HEAD : (h + 1) * HEAD], q_gain), at, 256)
            qs[h * HEAD : (h + 1) * HEAD, i * 256 : (i + 1) * 256] = head.astype(BF16) * scale
    for ref, at in ((low, 0), (high, WINDOW + ROWS)):
        tiles = [ref[EDGE:, k * 128 : (k + 1) * 128] for k in range(WIDTH // 128)]
        keys_values(jnp.concatenate(tiles, axis=0), at, WINDOW)


def attend_kernel(sink, qs, ks, vs, attn_ref, even_mask, odd_mask, even, odd):
    reach = 3 * WINDOW
    pairs = ROWS // WINDOW // 2
    jj = lax.broadcasted_iota(jnp.int32, (reach, WINDOW), 0)
    ii = lax.broadcasted_iota(jnp.int32, (reach, WINDOW), 1)
    band = (jj >= ii) & (jj <= ii + 2 * WINDOW)
    first = lax.axis_index(SP) * ROWS - WINDOW

    def set_mask(mask, j):
        position = jj + (first + j * WINDOW)
        mask[...] = jnp.where(band & (position >= 0) & (position < SEQ), 0.0, NEG_FILL)

    def scores(j, out):
        here = pl.multiple_of(j * WINDOW, 128)
        qb = jnp.concatenate(
            [qs[h * HEAD : (h + 1) * HEAD, pl.ds(here, WINDOW)] for h in range(QHEADS)], axis=1
        )
        out[...] = dot_tn(ks[:, pl.ds(here, reach)], qb)

    def outputs(j, mask, saved):
        here = pl.multiple_of(j * WINDOW, 128)
        weights = []
        for h in range(QHEADS):
            s = saved[:, h * WINDOW : (h + 1) * WINDOW] + mask[...]
            top = jnp.maximum(jnp.max(s, axis=0, keepdims=True), sink[h])
            p = jnp.exp(s - top)
            scale = 1.0 / (jnp.sum(p, axis=0, keepdims=True) + jnp.exp(sink[h] - top))
            weights.append((p * scale).astype(BF16))
        o = dot(vs[:, pl.ds(here, reach)], jnp.concatenate(weights, axis=1))
        o = jnp.concatenate([o[:, h * WINDOW : (h + 1) * WINDOW] for h in range(QHEADS)], axis=0)
        attn_ref[pl.ds(here, WINDOW), :] = o.T.astype(BF16)

    set_mask(even_mask, 0)
    set_mask(odd_mask, 1)
    scores(0, even)

    def pair(i, _):
        @pl.when(i == 1)
        def _():
            set_mask(even_mask, 2)

        @pl.when(i == pairs - 1)
        def _():
            set_mask(odd_mask, 2 * pairs - 1)

        scores(2 * i + 1, odd)
        outputs(2 * i, even_mask, even)
        scores(jnp.minimum(2 * i + 2, 2 * pairs - 1), even)
        outputs(2 * i + 1, odd_mask, odd)
        return 0

    lax.fori_loop(0, pairs, pair, 0)


def mixer_kernel(x_ref, b_ref, c_ref, cum_ref, step_ref, enter_ref, back_ref, spread, y_ref, state):
    state[...] = jnp.zeros_like(state)
    tt = lax.broadcasted_iota(jnp.int32, (CHUNK, CHUNK), 0)
    ss = lax.broadcasted_iota(jnp.int32, (CHUNK, CHUNK), 1)
    below, same, left = tt > ss, tt == ss, ss < HEAD
    nothing = jnp.zeros((CHUNK, CHUNK), BF16)

    def chunk(i, _):
        k = CHUNKS - 1 - i
        at = pl.ds(pl.multiple_of(k * CHUNK, 128), CHUNK)
        c = c_ref[at, :]
        scores = dot_nt(c, b_ref[at, :])
        cum = cum_ref[:, at]
        step = step_ref[:, at]
        f, r = cum[:HEADS], cum[HEADS:]
        sf, sr = step[:HEADS], step[HEADS:]
        row_f = jnp.log(sf) - f
        row_r = jnp.log(sr) - r
        row_d = jnp.log(sf + sr)
        columns = cum.T

        def weights(h):
            lower = columns[:, h : h + 1] + row_f[h : h + 1]
            upper = columns[:, HEADS + h : HEADS + h + 1] + row_r[h : h + 1]
            power = jnp.where(below, lower, jnp.where(same, row_d[h : h + 1], upper))
            return (jnp.exp(power) * scores).astype(BF16)

        wide = widen(jnp.concatenate([jnp.exp(f), jnp.exp(r)], axis=1), spread[...])
        across = wide[:CHUNK] * dot(c, enter_ref[k])
        across = across + wide[CHUNK:] * dot(c, state[...].astype(BF16))
        for pair in range(HEADS // 2):
            cols = slice(pair * 2 * HEAD, (pair + 1) * 2 * HEAD)
            both = jnp.concatenate([weights(2 * pair), weights(2 * pair + 1)], axis=1)
            xp = x_ref[at, cols]
            stacked = jnp.concatenate(
                [jnp.where(left, xp, nothing), jnp.where(left, nothing, xp)], axis=0
            )
            y_ref[at, cols] = dot(both, stacked) + across[:, cols]
        state[...] = state[...] * wide[CHUNK : CHUNK + 1] + back_ref[k].astype(F32)
        return 0

    lax.fori_loop(0, CHUNKS, chunk, 0)


def finish_rows(core, y, c, run, gate, attn, gain, spread, from_low, from_high, out):
    scales = lane_row(gain)
    for i in range(LINE):
        at = pl.ds(pl.multiple_of(i * 256 + core * 128, 128), 128)
        cm = c[at, :]
        reach = jnp.exp(run[:, at])
        wide = widen(jnp.concatenate([reach[:HEADS], reach[HEADS:]], axis=1), spread[...])
        v = y[at, :] + wide[:128] * dot(cm, from_low[...]) + wide[128:] * dot(cm, from_high[...])
        v = v * silu(gate[at, :].astype(F32))
        mean = jnp.mean(v * v, axis=-1, keepdims=True)
        out[i, :, : QHEADS * HEAD] = attn[at, :]
        out[i, :, QHEADS * HEAD :] = (v * lax.rsqrt(mean + NORM_EPS) * scales).astype(BF16)


def theirs_kernel(
    part, d1, d2, d3, y, c, run, gate, attn, gain, spread, theirs, from_low, from_high
):
    got = (None, d1, d2, d3)
    level = lax.axis_index("z")
    for back, keep in ((0, from_low), (1, from_high)):
        count = level if back == 0 else LINE - 1 - level
        prefix = jnp.zeros((STATE, INNER), F32)
        log_prefix = jnp.zeros((1, INNER), F32)
        for d in range(1, LINE):
            r = got[d if back == 0 else LINE - d]
            live = d <= count
            weight = jnp.where(live, jnp.exp(log_prefix), 0.0)
            prefix = prefix + weight * r[:STATE, :].astype(F32)
            tail = r[STATE:, :].astype(F32)
            log = tail[0:1] + tail[1:2] + tail[2:3]
            log_prefix = log_prefix + jnp.where(live, log, 0.0)
        own = part[STATE * back : STATE * (back + 1), :]
        reach = jnp.exp(part[2 * STATE + back : 2 * STATE + back + 1, :])
        keep[...] = (own + reach * prefix).astype(BF16)
    core = 1 - lax.axis_index("c")
    finish_rows(core, y, c, run, gate, attn, gain, spread, from_low, from_high, theirs)


def mine_kernel(y, c, run, gate, attn, gain, spread, from_low, from_high, wa, ws, mine, first):
    finish_rows(lax.axis_index("c"), y, c, run, gate, attn, gain, spread, from_low, from_high, mine)
    first[...] = partial(mine[(lax.axis_index("x") + 2) % LINE], wa, ws)


def sum_kernel(own, direct_right, direct_left, last_right, last_left, out):
    upper = own[:HALVES] + direct_left[...].astype(F32) + last_right[...].astype(F32)
    lower = own[HALVES:] + direct_right[...].astype(F32) + last_left[...].astype(F32)
    out[:HALVES] = upper.astype(BF16)
    out[HALVES:] = lower.astype(BF16)


def partial(v, a, b):
    split = QHEADS * HEAD
    return (dot(v[:, :split], a[...]) + dot(v[:, split:], b[...])).astype(BF16).astype(F32)


def chunk_partial(order, mine, theirs, wa, ws, pa, ps):
    join = lambda ref: jnp.concatenate([ref[index] for index in order], axis=0)
    return partial(join(mine), wa, ws) + partial(join(theirs), pa, ps)


HALVES = 64


def opposite_kernel(first, theirs, pa, ps, right, left):
    value = first[...] + partial(theirs[(lax.axis_index("x") + 2) % LINE], pa, ps)
    right[...] = value[:HALVES].astype(BF16)
    left[...] = value[HALVES:].astype(BF16)


def beside_kernel(mine, theirs, wa, ws, pa, ps, right, left, keep_right, keep_left, own):
    x = lax.axis_index("x")
    order = [(x + 1) % LINE, (x + 3) % LINE, x]
    value = chunk_partial(order, mine, theirs, wa, ws, pa, ps)
    keep_right[...] = value[:HALVES]
    right[...] = value[HALVES : 2 * HALVES].astype(BF16)
    left[...] = value[2 * HALVES : 3 * HALVES].astype(BF16)
    keep_left[...] = value[3 * HALVES : 4 * HALVES]
    own[...] = value[4 * HALVES :]


HBM = pl.BlockSpec(memory_space=pltpu.HBM)


def whole(count):
    return [pl.BlockSpec(memory_space=pltpu.VMEM)] * count


SCALARS = pl.BlockSpec(memory_space=pltpu.SMEM)


def plain(kernel, name, inputs, outs, scalars=0, remote=0, scratch=(), size=8, flops=1e9):
    return pl.pallas_call(
        kernel,
        in_specs=[SCALARS] * scalars + whole(inputs) + [HBM] * remote,
        out_specs=whole(len(outs)),
        out_shape=outs,
        scratch_shapes=list(scratch),
        compiler_params=pltpu.CompilerParams(vmem_limit_bytes=size << 20),
        cost_estimate=cost(flops),
        name=name,
    )


def fixed(shape):
    return pl.BlockSpec(memory_space=pltpu.VMEM)


def params(size):
    return pltpu.CompilerParams(dimension_semantics=("arbitrary",), vmem_limit_bytes=size << 20)


def cost(flops):
    return pl.CostEstimate(flops=int(flops), transcendentals=0, bytes_accessed=8 << 20)


def shaped(shape, dtype):
    return jax.ShapeDtypeStruct(shape, dtype)


def local(
    tokens, norm_gain, query_weight, key_weight, value_weight, query_gain, key_gain, sink_logit,
    gate_weight, inner_weight, input_map, output_map, step_weight, conv_inner, conv_pair,
    decay_rate, decay_jump, inner_gain, attn_out_weight, ssm_out_weight,
):
    up = [(k, k + 1) for k in range(15)]
    down = [(k + 1, k) for k in range(15)]
    swap = [(0, 1), (1, 0)]
    pin = lambda v: pltpu.with_memory_space_constraint(v, pltpu.HBM)
    gain = norm_gain.reshape(WIDTH // 128, 128)
    halo = shaped((EDGE + 8, WIDTH), BF16)
    edge_low, edge_high = plain(
        edge_kernel, "edge", 0, [halo, halo], remote=4,
        scratch=[
            pltpu.VMEM((2 * WINDOW, WIDTH), BF16), pltpu.VMEM((2 * HEAD, WIDTH), BF16),
            pltpu.VMEM((WIDTH // 128, 128), BF16), pltpu.SemaphoreType.DMA((5,)),
        ],
        size=6, flops=1e10,
    )(*map(pin, (gain, tokens, key_weight.T, value_weight.T)))
    halo_low = lax.ppermute(edge_low, SP, up)
    halo_high = lax.ppermute(edge_high, SP, down)
    attn_partner = lax.ppermute(attn_out_weight, "c", swap)
    ssm_partner = lax.ppermute(ssm_out_weight, "c", swap)

    spread = jnp.asarray(head_spread(), BF16)
    step_rows = jnp.transpose(step_weight, (1, 2, 0)).reshape(2 * HEADS, WIDTH)
    jump = jnp.transpose(decay_jump, (1, 2, 0)).reshape(2 * HEADS, ROWS)
    normed, rows, raw, w_gate, w_q, w_kv = plain(
        front_kernel, "front", 5,
        [
            shaped((ROWS, WIDTH), BF16), shaped((CONV // STATE, ROWS, STATE), F32),
            shaped((2 * HEADS, ROWS), F32), shaped((WIDTH, INNER), BF16),
            shaped((WIDTH, QHEADS * HEAD), BF16), shaped((2 * HEAD, WIDTH), BF16),
        ],
        remote=5,
        scratch=[pltpu.VMEM((2 * HEADS, WIDTH), BF16), pltpu.SemaphoreType.DMA((9,))],
        size=8, flops=10e9,
    )(gain, inner_weight, input_map, output_map, tokens, *map(pin, (step_rows, gate_weight, query_weight,
      key_weight.T, value_weight.T)))

    x, b, c, cum, step, run, enter, back, state, spread = plain(
        state_kernel, "state", 8,
        [
            shaped((ROWS, INNER), BF16), shaped((ROWS, STATE), BF16),
            shaped((ROWS, STATE), BF16), shaped((2 * HEADS, ROWS), F32),
            shaped((2 * HEADS, ROWS), F32), shaped((2 * HEADS, ROWS), F32),
            shaped((CHUNKS, STATE, INNER), BF16), shaped((CHUNKS, STATE, INNER), BF16),
            shaped((PACK, INNER), BF16), shaped((2 * HEADS, INNER), BF16),
        ],
        scalars=1, remote=4,
        scratch=[pltpu.VMEM((CONV // STATE, CHUNK + 2 * EDGE, STATE), F32)] * 2
        + [pltpu.VMEM((STATE, INNER), F32)] * 2
        + [
            pltpu.VMEM((2 * HEADS, ROWS), F32), pltpu.VMEM((5, INNER), BF16),
            pltpu.VMEM((5, 2, STATE), BF16), pltpu.SemaphoreType.DMA((4,)),
        ],
        size=8, flops=6e9,
    )(decay_rate, rows, raw, halo_low, halo_high, gain, inner_weight, input_map, output_map, conv_inner, conv_pair,
      jump, spread)

    def along(values, axis):
        sent = {
            d: lax.ppermute(values[d - 1], axis, [(k, (k + d) % LINE) for k in range(LINE)])
            for d in (1, 3, 2)
        }
        return [sent[d] for d in (1, 2, 3)]

    got = along([state] * 3, "y")

    near, far = rope_tables()
    gate, qs, ks, vs = plain(
        heads_kernel, "heads", 8,
        [
            shaped((ROWS, INNER), BF16), shaped((QHEADS * HEAD, ROWS), BF16), shaped((HEAD, ROWS + 2 * WINDOW), BF16),
            shaped((HEAD, ROWS + 2 * WINDOW), BF16),
        ],
        remote=2,
        scratch=[
            pltpu.VMEM((HEAD, ROWS + 2 * WINDOW), F32), pltpu.VMEM((1, HEAD), F32),
            pltpu.SemaphoreType.DMA((2,)),
        ],
        size=6, flops=7e9,
    )(normed, halo_low, halo_high, w_gate, w_q, w_kv, query_gain[None, :], key_gain[None, :],
      jnp.asarray(near), jnp.asarray(far))

    *messages, part = plain(
        line_kernel, "line", 4,
        [shaped((STATE + 16, INNER), BF16)] * 3 + [shaped((PACK, INNER), F32)],
        size=4, flops=1e9,
    )(state, *got)

    far_got = along(messages, "z")

    attn = plain(
        attend_kernel, "attend", 3, [shaped((ROWS, QHEADS * HEAD), BF16)], scalars=1,
        scratch=[pltpu.VMEM((3 * WINDOW, WINDOW), F32)] * 2
        + [pltpu.VMEM((3 * WINDOW, QHEADS * WINDOW), F32)] * 2,
        size=8, flops=7e9,
    )(sink_logit, qs, ks, vs)[0]

    y = plain(
        mixer_kernel, "mixer", 8, [shaped((ROWS, INNER), F32)],
        scratch=[pltpu.VMEM((STATE, INNER), F32)], flops=10e9,
    )(x, b, c, cum, step, enter, back, spread)[0]

    depth = QHEADS * HEAD + INNER
    rest = (y, c, run, gate, attn, inner_gain.reshape(INNER // 128, 128), spread)
    incoming = shaped((STATE, INNER), BF16)
    theirs, from_low, from_high = plain(
        theirs_kernel, "theirs", 11, [shaped((4, 128, depth), BF16), incoming, incoming], flops=2e9
    )(part, *far_got, *rest)
    theirs = lax.ppermute(theirs, "c", swap)
    mine, first = plain(
        mine_kernel, "mine", 11, [shaped((4, 128, depth), BF16), shaped((128, WIDTH), F32)], flops=2e9
    )(*rest, from_low, from_high, attn_out_weight, ssm_out_weight)
    operands = (
        mine, theirs, attn_out_weight, ssm_out_weight, attn_partner, ssm_partner
    )
    sent = shaped((HALVES, WIDTH), BF16)
    kept = shaped((HALVES, WIDTH), F32)
    right = [(k, (k + 1) % LINE) for k in range(LINE)]
    left = [((k + 1) % LINE, k) for k in range(LINE)]
    shift_right = lambda value: lax.ppermute(value, "x", right)
    shift_left = lambda value: lax.ppermute(value, "x", left)
    relay_right, relay_left = plain(
        opposite_kernel, "opposite", 4, [sent, sent], flops=1e9
    )(first, theirs, attn_partner, ssm_partner)
    relay_right = shift_right(relay_right)
    relay_left = shift_left(relay_left)
    direct_right, direct_left, keep_right, keep_left, own = plain(
        beside_kernel, "beside", 6, [sent, sent, kept, kept, shaped((2 * HALVES, WIDTH), F32)],
        flops=3e9,
    )(*operands)
    direct_right = shift_right(direct_right)
    direct_left = shift_left(direct_left)
    last_right = shift_right((keep_right + relay_right.astype(F32)).astype(BF16))
    last_left = shift_left((keep_left + relay_left.astype(F32)).astype(BF16))
    return plain(
        sum_kernel, "sum", 5, [shaped((2 * HALVES, WIDTH), BF16)], size=4, flops=1e6
    )(own, direct_right, direct_left, last_right, last_left)[0]


def solution(mesh):
    split = Mesh(mesh.devices.reshape(4, 4, 4, 2), SP_TP)
    tp = ("x", "c")
    placed = (
        P(SP, None), P(), P(None, tp), P(None, tp), P(None, tp), P(), P(), P(tp),
        P(None, tp), P(None, tp), P(None, tp), P(None, tp), P(None, None, tp), P(None, tp),
        P(None, None, tp), P(None, tp), P(SP, None, tp), P(tp), P(tp, None), P(tp, None),
    )
    return jax.shard_map(
        local, mesh=split, in_specs=placed, out_specs=P(SP_TP, None), check_vma=False
    )
```

```python
import jax
import jax.numpy as jnp
import numpy as np
from jax import lax
from jax.experimental import pallas as pl
from jax.experimental.pallas import tpu as pltpu
from jax.sharding import Mesh
from jax.sharding import PartitionSpec as P

SP = ("z", "y")
SP_TP = ("z", "y", "x", "c")
ROWS = 1024
WIDTH = 2048
SEQ = 16384
HEADS = 8
STATE = 128
INNER = 512
CONV = INNER + 2 * STATE
CHUNK = 128
CHUNKS = ROWS // CHUNK
EDGE = 16
WINDOW = 128
HEAD = 64
HALF = 32
QHEADS = 4
LINE = 4
PACK = 2 * STATE + 16

NORM_EPS = 1e-05
ROPE_BASE = 500000.0
NEG_FILL = -1e30
F32 = jnp.float32
BF16 = jnp.bfloat16


def rope_tables():
    frequency = ROPE_BASE ** (-np.arange(0, HEAD, 2, dtype=np.float64) / HEAD)
    offsets = np.arange(-WINDOW, ROWS + WINDOW, dtype=np.float64)
    near = frequency[:, None] * offsets[None, :]
    far = frequency[None, :] * (ROWS * np.arange(SEQ // ROWS, dtype=np.float64))[:, None]
    near_table = np.concatenate([np.cos(near), np.sin(near)], axis=0).astype(np.float32)
    far_table = np.concatenate([np.cos(far), np.sin(far)], axis=1).astype(np.float32)
    return near_table, far_table[:, None, :]


def head_spread():
    spread = np.repeat(np.eye(HEADS, dtype=np.float32), INNER // HEADS, axis=1)
    return np.concatenate([spread, spread], axis=0)


def dot(a, b):
    return jnp.dot(a, b, preferred_element_type=F32)


def dot_nt(a, b):
    return lax.dot_general(a, b, (((1,), (1,)), ((), ())), preferred_element_type=F32)


def dot_tn(a, b):
    return lax.dot_general(a, b, (((0,), (0,)), ((), ())), preferred_element_type=F32)


def silu(v):
    half = 0.5 * v
    return half + half * jnp.tanh(half)


def normalise(tokens, gain):
    t = tokens.astype(F32)
    mean = jnp.mean(t * t, axis=-1, keepdims=True)
    return (t * lax.rsqrt(mean + NORM_EPS) * gain).astype(BF16)


def lane_row(ref):
    value = ref[...].astype(F32)
    return jnp.concatenate([value[k : k + 1] for k in range(value.shape[0])], axis=1)


def column(row):
    size = row.shape[1]
    a = lax.broadcasted_iota(jnp.int32, (size, size), 0)
    b = lax.broadcasted_iota(jnp.int32, (size, size), 1)
    return jnp.sum(jnp.where(a == b, row, 0.0), axis=1, keepdims=True)


def fetch(pairs, sems):
    copies = [pltpu.make_async_copy(a, b, sems.at[k]) for k, (a, b) in enumerate(pairs)]
    for copy in copies:
        copy.start()
    return copies


def widen(rows, spread):
    high = rows.astype(BF16)
    low = (rows - high.astype(F32)).astype(BF16)
    return dot_tn(jnp.concatenate([high, low], axis=0), spread)


def edge_kernel(h_gain, tok, h_k, h_v, low, high, edge, w_kv, gain, sems):
    copies = fetch(
        [
            (tok.at[pl.ds(ROWS - WINDOW, WINDOW)], edge.at[pl.ds(0, WINDOW)]),
            (tok.at[pl.ds(0, WINDOW)], edge.at[pl.ds(WINDOW, WINDOW)]),
            (h_k, w_kv.at[pl.ds(0, HEAD)]), (h_v, w_kv.at[pl.ds(HEAD, HEAD)]), (h_gain, gain),
        ],
        sems,
    )
    for k in (4, 0, 1):
        copies[k].wait()
    n = normalise(edge[...], lane_row(gain))
    for k in (2, 3):
        copies[k].wait()
    kv = dot_nt(w_kv[...], n).astype(BF16)
    for ref, at, rows in ((low, 0, WINDOW - EDGE), (high, WINDOW, WINDOW)):
        ref[:EDGE, :] = edge[rows : rows + EDGE, :]
        for k in range(WIDTH // 128):
            ref[EDGE:, k * 128 : (k + 1) * 128] = kv[k * 8 : (k + 1) * 8, at : at + WINDOW]


BLOCK = 256


def front_kernel(
    gain, w_inner, w_in, w_out, tok, h_step, h_gate, h_q, h_k, h_v,
    normed, rows, raw, w_gate, w_q, w_kv, w_step, sems,
):
    blocks = [pl.ds(k * BLOCK, BLOCK) for k in range(ROWS // BLOCK)]
    waits = fetch(
        [(h_step, w_step)], sems
    )
    late = [
        pltpu.make_async_copy(a, b, sems.at[5 + k])
        for k, (a, b) in enumerate(
            [
                (h_gate, w_gate), (h_q, w_q), (h_k, w_kv.at[pl.ds(0, HEAD)]),
                (h_v, w_kv.at[pl.ds(HEAD, HEAD)]),
            ]
        )
    ]
    g = lane_row(gain)

    def prepare(i):
        normed[blocks[i], :] = normalise(tok[blocks[i], :], g)

    prepare(0)
    waits[0].wait()
    pair = jnp.concatenate([w_in[...], w_out[...]], axis=1)
    for i, block in enumerate(blocks):
        if i + 1 < len(blocks):
            prepare(i + 1)
        if i == 1:
            for copy in late:
                copy.start()
        n = normed[block, :]
        for k in range(0, INNER, 2 * STATE):
            value = dot(n, w_inner[:, k : k + 2 * STATE]).astype(BF16).astype(F32)
            rows[k // STATE, block, :] = value[:, :STATE]
            rows[k // STATE + 1, block, :] = value[:, STATE:]
        value = dot(n, pair).astype(BF16).astype(F32)
        rows[INNER // STATE, block, :] = value[:, :STATE]
        rows[INNER // STATE + 1, block, :] = value[:, STATE:]
        raw[:, block] = dot_nt(w_step[...], n).astype(BF16).astype(F32)
    for copy in late:
        copy.wait()


def state_kernel(
    rate, rows, raw, low, high, gain, w_inner, w_in, w_out, inner_taps, pair_taps, jump, spread,
    x_ref, b_ref, c_ref, cum_ref, step_ref, run_ref, enter_ref, back_ref, state_ref,
    first, last, state_f, state_b,
):
    g = lane_row(gain)
    edge = normalise(jnp.concatenate([low[:EDGE, :], high[:EDGE, :]], axis=0), g)
    for k in range(CONV // STATE):
        if k < INNER // STATE:
            w = w_inner[:, k * STATE : (k + 1) * STATE]
        else:
            w = (w_in if k == INNER // STATE else w_out)[...]
        value = dot(edge, w).astype(BF16).astype(F32)
        first[k, :EDGE, :] = value[:EDGE]
        first[k, EDGE:, :] = rows[k, : CHUNK + EDGE, :]
        last[k, : CHUNK + EDGE, :] = rows[k, ROWS - CHUNK - EDGE :, :]
        last[k, CHUNK + EDGE :, :] = value[EDGE:]
    taps = jnp.concatenate(
        [inner_taps[...].astype(F32)] + [pair_taps[:, k, :].astype(F32) for k in (0, 1)], axis=1
    )
    rates = [
        jnp.concatenate([jnp.full((1, CHUNK), rate[d, h], F32) for h in range(HEADS)], axis=0)
        for d in (0, 1)
    ]
    v = raw[...]
    step = jnp.maximum(v, 0.0) + jnp.log1p(jnp.exp(-jnp.abs(v)))
    step_ref[...] = step
    lane = lax.broadcasted_iota(jnp.int32, (HEADS, CHUNK), 1)
    cums = []
    for k in range(CHUNKS):
        at = slice(k * CHUNK, (k + 1) * CHUNK)
        f = jump[:HEADS, at] - rates[0] * step[:HEADS, at]
        r = jump[HEADS:, at] - rates[1] * step[HEADS:, at]
        for shift in (1, 2, 4, 8, 16, 32, 64):
            f = f + jnp.where(lane >= shift, pltpu.roll(f, shift, 1), 0.0)
            r = r + jnp.where(lane < CHUNK - shift, pltpu.roll(r, CHUNK - shift, 1), 0.0)
        cums.append((f, r))
        cum_ref[:HEADS, k * CHUNK : (k + 1) * CHUNK] = f
        cum_ref[HEADS:, k * CHUNK : (k + 1) * CHUNK] = r
    totals = [(f[:, CHUNK - 1 :], r[:, :1]) for f, r in cums]
    zero = jnp.zeros((HEADS, 1), F32)
    ahead = zero
    for k in range(CHUNKS):
        run_ref[:HEADS, k * CHUNK : (k + 1) * CHUNK] = cums[k][0] + ahead
        ahead = ahead + totals[k][0]
    behind = zero
    for k in reversed(range(CHUNKS)):
        run_ref[HEADS:, k * CHUNK : (k + 1) * CHUNK] = cums[k][1] + behind
        behind = behind + totals[k][1]
    sp = spread[...]
    state_f[...] = jnp.zeros_like(state_f)
    state_b[...] = jnp.zeros_like(state_b)
    passed = zero
    for k in range(CHUNKS):
        if k == 0:
            source, base = first, EDGE - 2
        elif k == CHUNKS - 1:
            source, base = last, EDGE - 2
        else:
            source, base = rows, k * CHUNK - 2
        here = slice(k * CHUNK, (k + 1) * CHUNK)

        def active(tile):
            cols = slice(tile * STATE, (tile + 1) * STATE)
            acc = source[tile, base : base + CHUNK, :] * taps[0:1, cols]
            for t in range(1, 5):
                acc = acc + source[tile, base + t : base + t + CHUNK, :] * taps[t : t + 1, cols]
            return silu(acc)

        f, r = cums[k]
        tf, tr = totals[k]
        wf = jnp.exp(tf - f) * step[:HEADS, here]
        wr = jnp.exp(tr - r) * step[HEADS:, here]
        df = jnp.where(lane == 0, jnp.exp(tf), jnp.exp(passed))
        bm = active(INNER // STATE).astype(BF16)
        b_ref[here, :] = bm
        c_ref[here, :] = active(INNER // STATE + 1).astype(BF16)
        xf = jnp.concatenate([active(tile) for tile in range(INNER // STATE)], axis=1)
        x_ref[here, :] = xf.astype(BF16)
        wide = widen(jnp.concatenate([wf, wr, df], axis=1), sp)
        fresh_f = dot_tn(bm, (xf * wide[:CHUNK]).astype(BF16))
        fresh_b = dot_tn(bm, (xf * wide[CHUNK : 2 * CHUNK]).astype(BF16))
        enter_ref[k] = state_f[...].astype(BF16)
        back_ref[k] = fresh_b.astype(BF16)
        state_f[...] = state_f[...] * wide[2 * CHUNK : 2 * CHUNK + 1] + fresh_f
        state_b[...] = state_b[...] + fresh_b * wide[2 * CHUNK + 1 : 2 * CHUNK + 2]
        passed = passed + tr
    state_ref[:STATE, :] = state_f[...].astype(BF16)
    state_ref[STATE : 2 * STATE, :] = state_b[...].astype(BF16)
    parts = jnp.zeros((HEADS, CHUNK), F32)
    column = 0
    for total in (ahead, passed):
        rest = total
        for _ in range(3):
            piece = rest.astype(BF16).astype(F32)
            rest = rest - piece
            parts = jnp.where(lane == column, piece, parts)
            column += 1
    state_ref[2 * STATE :, :] = dot_tn(parts.astype(BF16), sp[:HEADS]).astype(BF16)[:16]


def logs_of(ref):
    tail = ref[2 * STATE :, :].astype(F32)
    return tail[0:1] + tail[1:2] + tail[2:3], tail[3:4] + tail[4:5] + tail[5:6]


def line_kernel(own, d1, d2, d3, m1, m2, m3, part_ref):
    place, level = lax.axis_index("y"), lax.axis_index("z")
    got = (own, d1, d2, d3)
    logs = [logs_of(r) for r in got]
    state = lambda r, back: r[STATE * back : STATE * (back + 1), :].astype(F32)
    totals = []
    for back in (0, 1):
        near = (lambda d: d) if back == 0 else (lambda d: LINE - d)
        count = place if back == 0 else LINE - 1 - place
        far_count = LINE - 1 - count
        prefix = jnp.zeros((STATE, INNER), F32)
        log_prefix = jnp.zeros((1, INNER), F32)
        for d in range(1, LINE):
            r = near(d)
            live = d <= count
            weight = jnp.where(live, jnp.exp(log_prefix), 0.0)
            prefix = prefix + weight * state(got[r], back)
            log_prefix = log_prefix + jnp.where(live, logs[r][back], 0.0)
        total = jnp.zeros((STATE, INNER), F32)
        suffix = jnp.zeros((1, INNER), F32)
        for e in reversed(range(1, LINE)):
            r = near(LINE - e)
            live = e <= far_count
            weight = jnp.where(live, jnp.exp(suffix), 0.0)
            total = total + weight * state(got[r], back)
            suffix = suffix + jnp.where(live, logs[r][back], 0.0)
        total = total + jnp.exp(suffix) * state(own, back)
        suffix = suffix + logs[0][back]
        total = total + jnp.exp(suffix) * prefix
        part_ref[STATE * back : STATE * (back + 1), :] = prefix
        part_ref[2 * STATE + back : 2 * STATE + back + 1, :] = log_prefix
        rest = suffix + log_prefix
        pieces = []
        for _ in range(3):
            piece = rest.astype(BF16).astype(F32)
            rest = rest - piece
            pieces.append(piece)
        pieces.append(jnp.zeros((13, INNER), F32))
        totals.append((total.astype(BF16), jnp.concatenate(pieces, axis=0).astype(BF16)))
    for d, ref in ((1, m1), (2, m2), (3, m3)):
        for back in (0, 1):

            @pl.when(level + d < LINE if back == 0 else level + d >= LINE)
            def _(ref=ref, back=back):
                ref[:STATE, :] = totals[back][0]
                ref[STATE:, :] = totals[back][1]


def heads_kernel(
    normed, low, high, w_gate, w_q, w_kv, q_row, k_row, near, far, gate, qs, ks, vs
):
    q_gain, k_gain = column(q_row[...]), column(k_row[...])
    turns = column(far[lax.axis_index(SP)])
    far_cos = turns[:HALF, :]
    far_sin = turns[HALF:, :]
    scale = jnp.asarray(HEAD**-0.5, BF16)

    def turn(head, at, size):
        co = near[:HALF, at : at + size]
        so = near[HALF:, at : at + size]
        cos = far_cos * co - far_sin * so
        sin = far_sin * co + far_cos * so
        u, w = head[:HALF], head[HALF:]
        return jnp.concatenate([u * cos - w * sin, w * cos + u * sin], axis=0)

    def head_norm(head, scale):
        mean = jnp.mean(head * head, axis=0, keepdims=True)
        return head * lax.rsqrt(mean + NORM_EPS) * scale

    def keys_values(kv, at, size):
        k = head_norm(kv[:HEAD].astype(F32), k_gain)
        ks[:, at : at + size] = turn(k, at, size).astype(BF16)
        vs[:, at : at + size] = kv[HEAD:]

    for i in range(4):
        at = WINDOW + i * 256
        n = normed[i * 256 : (i + 1) * 256, :]
        keys_values(dot_nt(w_kv[...], n).astype(BF16), at, 256)
        gate[i * 256 : (i + 1) * 256, :] = dot(n, w_gate[...]).astype(BF16)
        q = dot(n, w_q[...]).astype(BF16).astype(F32).T
        for h in range(QHEADS):
            head = turn(head_norm(q[h * HEAD : (h + 1) * HEAD], q_gain), at, 256)
            qs[h * HEAD : (h + 1) * HEAD, i * 256 : (i + 1) * 256] = head.astype(BF16) * scale
    for ref, at in ((low, 0), (high, WINDOW + ROWS)):
        tiles = [ref[EDGE:, k * 128 : (k + 1) * 128] for k in range(WIDTH // 128)]
        keys_values(jnp.concatenate(tiles, axis=0), at, WINDOW)


def attend_kernel(sink, qs, ks, vs, attn_ref, even_mask, odd_mask, even, odd):
    reach = 3 * WINDOW
    pairs = ROWS // WINDOW // 2
    jj = lax.broadcasted_iota(jnp.int32, (reach, WINDOW), 0)
    ii = lax.broadcasted_iota(jnp.int32, (reach, WINDOW), 1)
    band = (jj >= ii) & (jj <= ii + 2 * WINDOW)
    first = lax.axis_index(SP) * ROWS - WINDOW

    def set_mask(mask, j):
        position = jj + (first + j * WINDOW)
        mask[...] = jnp.where(band & (position >= 0) & (position < SEQ), 0.0, NEG_FILL)

    def scores(j, out):
        here = pl.multiple_of(j * WINDOW, 128)
        qb = jnp.concatenate(
            [qs[h * HEAD : (h + 1) * HEAD, pl.ds(here, WINDOW)] for h in range(QHEADS)], axis=1
        )
        out[...] = dot_tn(ks[:, pl.ds(here, reach)], qb)

    def outputs(j, mask, saved):
        here = pl.multiple_of(j * WINDOW, 128)
        weights = []
        for h in range(QHEADS):
            s = saved[:, h * WINDOW : (h + 1) * WINDOW] + mask[...]
            top = jnp.maximum(jnp.max(s, axis=0, keepdims=True), sink[h])
            p = jnp.exp(s - top)
            scale = 1.0 / (jnp.sum(p, axis=0, keepdims=True) + jnp.exp(sink[h] - top))
            weights.append((p * scale).astype(BF16))
        o = dot(vs[:, pl.ds(here, reach)], jnp.concatenate(weights, axis=1))
        o = jnp.concatenate([o[:, h * WINDOW : (h + 1) * WINDOW] for h in range(QHEADS)], axis=0)
        attn_ref[pl.ds(here, WINDOW), :] = o.T.astype(BF16)

    set_mask(even_mask, 0)
    set_mask(odd_mask, 1)
    scores(0, even)

    def pair(i, _):
        @pl.when(i == 1)
        def _():
            set_mask(even_mask, 2)

        @pl.when(i == pairs - 1)
        def _():
            set_mask(odd_mask, 2 * pairs - 1)

        scores(2 * i + 1, odd)
        outputs(2 * i, even_mask, even)
        scores(jnp.minimum(2 * i + 2, 2 * pairs - 1), even)
        outputs(2 * i + 1, odd_mask, odd)
        return 0

    lax.fori_loop(0, pairs, pair, 0)


def mixer_kernel(x_ref, b_ref, c_ref, cum_ref, step_ref, enter_ref, back_ref, spread, y_ref, state):
    state[...] = jnp.zeros_like(state)
    tt = lax.broadcasted_iota(jnp.int32, (CHUNK, CHUNK), 0)
    ss = lax.broadcasted_iota(jnp.int32, (CHUNK, CHUNK), 1)
    below, same, left = tt > ss, tt == ss, ss < HEAD
    nothing = jnp.zeros((CHUNK, CHUNK), BF16)

    def chunk(i, _):
        k = CHUNKS - 1 - i
        at = pl.ds(pl.multiple_of(k * CHUNK, 128), CHUNK)
        c = c_ref[at, :]
        scores = dot_nt(c, b_ref[at, :])
        cum = cum_ref[:, at]
        step = step_ref[:, at]
        f, r = cum[:HEADS], cum[HEADS:]
        sf, sr = step[:HEADS], step[HEADS:]
        row_f = jnp.log(sf) - f
        row_r = jnp.log(sr) - r
        row_d = jnp.log(sf + sr)
        columns = cum.T

        def weights(h):
            lower = columns[:, h : h + 1] + row_f[h : h + 1]
            upper = columns[:, HEADS + h : HEADS + h + 1] + row_r[h : h + 1]
            power = jnp.where(below, lower, jnp.where(same, row_d[h : h + 1], upper))
            return (jnp.exp(power) * scores).astype(BF16)

        wide = widen(jnp.concatenate([jnp.exp(f), jnp.exp(r)], axis=1), spread[...])
        across = wide[:CHUNK] * dot(c, enter_ref[k])
        across = across + wide[CHUNK:] * dot(c, state[...].astype(BF16))
        for pair in range(HEADS // 2):
            cols = slice(pair * 2 * HEAD, (pair + 1) * 2 * HEAD)
            both = jnp.concatenate([weights(2 * pair), weights(2 * pair + 1)], axis=1)
            xp = x_ref[at, cols]
            stacked = jnp.concatenate(
                [jnp.where(left, xp, nothing), jnp.where(left, nothing, xp)], axis=0
            )
            y_ref[at, cols] = dot(both, stacked) + across[:, cols]
        state[...] = state[...] * wide[CHUNK : CHUNK + 1] + back_ref[k].astype(F32)
        return 0

    lax.fori_loop(0, CHUNKS, chunk, 0)


def finish_rows(core, y, c, run, gate, attn, gain, spread, from_low, from_high, out):
    scales = lane_row(gain)
    for i in range(LINE):
        at = pl.ds(pl.multiple_of(i * 256 + core * 128, 128), 128)
        cm = c[at, :]
        reach = jnp.exp(run[:, at])
        wide = widen(jnp.concatenate([reach[:HEADS], reach[HEADS:]], axis=1), spread[...])
        v = y[at, :] + wide[:128] * dot(cm, from_low[...]) + wide[128:] * dot(cm, from_high[...])
        v = v * silu(gate[at, :].astype(F32))
        mean = jnp.mean(v * v, axis=-1, keepdims=True)
        out[i, :, : QHEADS * HEAD] = attn[at, :]
        out[i, :, QHEADS * HEAD :] = (v * lax.rsqrt(mean + NORM_EPS) * scales).astype(BF16)


def theirs_kernel(
    part, d1, d2, d3, y, c, run, gate, attn, gain, spread, theirs, from_low, from_high
):
    got = (None, d1, d2, d3)
    level = lax.axis_index("z")
    for back, keep in ((0, from_low), (1, from_high)):
        count = level if back == 0 else LINE - 1 - level
        prefix = jnp.zeros((STATE, INNER), F32)
        log_prefix = jnp.zeros((1, INNER), F32)
        for d in range(1, LINE):
            r = got[d if back == 0 else LINE - d]
            live = d <= count
            weight = jnp.where(live, jnp.exp(log_prefix), 0.0)
            prefix = prefix + weight * r[:STATE, :].astype(F32)
            tail = r[STATE:, :].astype(F32)
            log = tail[0:1] + tail[1:2] + tail[2:3]
            log_prefix = log_prefix + jnp.where(live, log, 0.0)
        own = part[STATE * back : STATE * (back + 1), :]
        reach = jnp.exp(part[2 * STATE + back : 2 * STATE + back + 1, :])
        keep[...] = (own + reach * prefix).astype(BF16)
    core = 1 - lax.axis_index("c")
    finish_rows(core, y, c, run, gate, attn, gain, spread, from_low, from_high, theirs)


def mine_kernel(y, c, run, gate, attn, gain, spread, from_low, from_high, wa, ws, mine, first):
    finish_rows(lax.axis_index("c"), y, c, run, gate, attn, gain, spread, from_low, from_high, mine)
    first[...] = partial(mine[(lax.axis_index("x") + 2) % LINE], wa, ws)


def sum_kernel(own, direct_right, direct_left, last_right, last_left, out):
    upper = own[:HALVES] + direct_left[...].astype(F32) + last_right[...].astype(F32)
    lower = own[HALVES:] + direct_right[...].astype(F32) + last_left[...].astype(F32)
    out[:HALVES] = upper.astype(BF16)
    out[HALVES:] = lower.astype(BF16)


def partial(v, a, b):
    split = QHEADS * HEAD
    return (dot(v[:, :split], a[...]) + dot(v[:, split:], b[...])).astype(BF16).astype(F32)


def chunk_partial(order, mine, theirs, wa, ws, pa, ps):
    join = lambda ref: jnp.concatenate([ref[index] for index in order], axis=0)
    return partial(join(mine), wa, ws) + partial(join(theirs), pa, ps)


HALVES = 64


def opposite_kernel(first, theirs, pa, ps, right, left):
    value = first[...] + partial(theirs[(lax.axis_index("x") + 2) % LINE], pa, ps)
    right[...] = value[:HALVES].astype(BF16)
    left[...] = value[HALVES:].astype(BF16)


def beside_kernel(mine, theirs, wa, ws, pa, ps, right, left, keep_right, keep_left, own):
    x = lax.axis_index("x")
    order = [(x + 1) % LINE, (x + 3) % LINE, x]
    value = chunk_partial(order, mine, theirs, wa, ws, pa, ps)
    keep_right[...] = value[:HALVES]
    right[...] = value[HALVES : 2 * HALVES].astype(BF16)
    left[...] = value[2 * HALVES : 3 * HALVES].astype(BF16)
    keep_left[...] = value[3 * HALVES : 4 * HALVES]
    own[...] = value[4 * HALVES :]


HBM = pl.BlockSpec(memory_space=pltpu.HBM)


def whole(count):
    return [pl.BlockSpec(memory_space=pltpu.VMEM)] * count


SCALARS = pl.BlockSpec(memory_space=pltpu.SMEM)


def plain(kernel, name, inputs, outs, scalars=0, remote=0, scratch=(), size=8, flops=1e9):
    return pl.pallas_call(
        kernel,
        in_specs=[SCALARS] * scalars + whole(inputs) + [HBM] * remote,
        out_specs=whole(len(outs)),
        out_shape=outs,
        scratch_shapes=list(scratch),
        compiler_params=pltpu.CompilerParams(vmem_limit_bytes=size << 20),
        cost_estimate=cost(flops),
        name=name,
    )


def fixed(shape):
    return pl.BlockSpec(memory_space=pltpu.VMEM)


def params(size):
    return pltpu.CompilerParams(dimension_semantics=("arbitrary",), vmem_limit_bytes=size << 20)


def cost(flops):
    return pl.CostEstimate(flops=int(flops), transcendentals=0, bytes_accessed=8 << 20)


def shaped(shape, dtype):
    return jax.ShapeDtypeStruct(shape, dtype)


def local(
    tokens, norm_gain, query_weight, key_weight, value_weight, query_gain, key_gain, sink_logit,
    gate_weight, inner_weight, input_map, output_map, step_weight, conv_inner, conv_pair,
    decay_rate, decay_jump, inner_gain, attn_out_weight, ssm_out_weight,
):
    up = [(k, k + 1) for k in range(15)]
    down = [(k + 1, k) for k in range(15)]
    swap = [(0, 1), (1, 0)]
    pin = lambda v: pltpu.with_memory_space_constraint(v, pltpu.HBM)
    gain = norm_gain.reshape(WIDTH // 128, 128)
    halo = shaped((EDGE + 8, WIDTH), BF16)
    edge_low, edge_high = plain(
        edge_kernel, "edge", 0, [halo, halo], remote=4,
        scratch=[
            pltpu.VMEM((2 * WINDOW, WIDTH), BF16), pltpu.VMEM((2 * HEAD, WIDTH), BF16),
            pltpu.VMEM((WIDTH // 128, 128), BF16), pltpu.SemaphoreType.DMA((5,)),
        ],
        size=6, flops=1e10,
    )(*map(pin, (gain, tokens, key_weight.T, value_weight.T)))
    halo_low = lax.ppermute(edge_low, SP, up)
    halo_high = lax.ppermute(edge_high, SP, down)
    attn_partner = lax.ppermute(attn_out_weight, "c", swap)
    ssm_partner = lax.ppermute(ssm_out_weight, "c", swap)

    spread = jnp.asarray(head_spread(), BF16)
    step_rows = jnp.transpose(step_weight, (1, 2, 0)).reshape(2 * HEADS, WIDTH)
    jump = jnp.transpose(decay_jump, (1, 2, 0)).reshape(2 * HEADS, ROWS)
    normed, rows, raw, w_gate, w_q, w_kv = plain(
        front_kernel, "front", 5,
        [
            shaped((ROWS, WIDTH), BF16), shaped((CONV // STATE, ROWS, STATE), F32),
            shaped((2 * HEADS, ROWS), F32), shaped((WIDTH, INNER), BF16),
            shaped((WIDTH, QHEADS * HEAD), BF16), shaped((2 * HEAD, WIDTH), BF16),
        ],
        remote=5,
        scratch=[pltpu.VMEM((2 * HEADS, WIDTH), BF16), pltpu.SemaphoreType.DMA((9,))],
        size=8, flops=10e9,
    )(gain, inner_weight, input_map, output_map, tokens, *map(pin, (step_rows, gate_weight, query_weight,
      key_weight.T, value_weight.T)))

    x, b, c, cum, step, run, enter, back, state = plain(
        state_kernel, "state", 12,
        [
            shaped((ROWS, INNER), BF16), shaped((ROWS, STATE), BF16),
            shaped((ROWS, STATE), BF16), shaped((2 * HEADS, ROWS), F32),
            shaped((2 * HEADS, ROWS), F32), shaped((2 * HEADS, ROWS), F32),
            shaped((CHUNKS, STATE, INNER), BF16), shaped((CHUNKS, STATE, INNER), BF16),
            shaped((PACK, INNER), BF16),
        ],
        scalars=1,
        scratch=[pltpu.VMEM((CONV // STATE, CHUNK + 2 * EDGE, STATE), F32)] * 2
        + [pltpu.VMEM((STATE, INNER), F32)] * 2,
        size=8, flops=6e9,
    )(decay_rate, rows, raw, halo_low, halo_high, gain, inner_weight, input_map, output_map, conv_inner, conv_pair,
      jump, spread)

    def along(values, axis):
        sent = {
            d: lax.ppermute(values[d - 1], axis, [(k, (k + d) % LINE) for k in range(LINE)])
            for d in (1, 3, 2)
        }
        return [sent[d] for d in (1, 2, 3)]

    got = along([state] * 3, "y")

    near, far = rope_tables()
    gate, qs, ks, vs = plain(
        heads_kernel, "heads", 10,
        [
            shaped((ROWS, INNER), BF16), shaped((QHEADS * HEAD, ROWS), BF16), shaped((HEAD, ROWS + 2 * WINDOW), BF16),
            shaped((HEAD, ROWS + 2 * WINDOW), BF16),
        ],
        size=6, flops=7e9,
    )(normed, halo_low, halo_high, w_gate, w_q, w_kv, query_gain[None, :], key_gain[None, :],
      jnp.asarray(near), jnp.asarray(far))

    *messages, part = plain(
        line_kernel, "line", 4,
        [shaped((STATE + 16, INNER), BF16)] * 3 + [shaped((PACK, INNER), F32)],
        size=4, flops=1e9,
    )(state, *got)

    far_got = along(messages, "z")

    attn = plain(
        attend_kernel, "attend", 3, [shaped((ROWS, QHEADS * HEAD), BF16)], scalars=1,
        scratch=[pltpu.VMEM((3 * WINDOW, WINDOW), F32)] * 2
        + [pltpu.VMEM((3 * WINDOW, QHEADS * WINDOW), F32)] * 2,
        size=8, flops=7e9,
    )(sink_logit, qs, ks, vs)[0]

    y = plain(
        mixer_kernel, "mixer", 8, [shaped((ROWS, INNER), F32)],
        scratch=[pltpu.VMEM((STATE, INNER), F32)], flops=10e9,
    )(x, b, c, cum, step, enter, back, spread)[0]

    depth = QHEADS * HEAD + INNER
    rest = (y, c, run, gate, attn, inner_gain.reshape(INNER // 128, 128), spread)
    incoming = shaped((STATE, INNER), BF16)
    theirs, from_low, from_high = plain(
        theirs_kernel, "theirs", 11, [shaped((4, 128, depth), BF16), incoming, incoming], flops=2e9
    )(part, *far_got, *rest)
    theirs = lax.ppermute(theirs, "c", swap)
    mine, first = plain(
        mine_kernel, "mine", 11, [shaped((4, 128, depth), BF16), shaped((128, WIDTH), F32)], flops=2e9
    )(*rest, from_low, from_high, attn_out_weight, ssm_out_weight)
    operands = (
        mine, theirs, attn_out_weight, ssm_out_weight, attn_partner, ssm_partner
    )
    sent = shaped((HALVES, WIDTH), BF16)
    kept = shaped((HALVES, WIDTH), F32)
    right = [(k, (k + 1) % LINE) for k in range(LINE)]
    left = [((k + 1) % LINE, k) for k in range(LINE)]
    shift_right = lambda value: lax.ppermute(value, "x", right)
    shift_left = lambda value: lax.ppermute(value, "x", left)
    relay_right, relay_left = plain(
        opposite_kernel, "opposite", 4, [sent, sent], flops=1e9
    )(first, theirs, attn_partner, ssm_partner)
    relay_right = shift_right(relay_right)
    relay_left = shift_left(relay_left)
    direct_right, direct_left, keep_right, keep_left, own = plain(
        beside_kernel, "beside", 6, [sent, sent, kept, kept, shaped((2 * HALVES, WIDTH), F32)],
        flops=3e9,
    )(*operands)
    direct_right = shift_right(direct_right)
    direct_left = shift_left(direct_left)
    last_right = shift_right((keep_right + relay_right.astype(F32)).astype(BF16))
    last_left = shift_left((keep_left + relay_left.astype(F32)).astype(BF16))
    return plain(
        sum_kernel, "sum", 5, [shaped((2 * HALVES, WIDTH), BF16)], size=4, flops=1e6
    )(own, direct_right, direct_left, last_right, last_left)[0]


def solution(mesh):
    split = Mesh(mesh.devices.reshape(4, 4, 4, 2), SP_TP)
    tp = ("x", "c")
    placed = (
        P(SP, None), P(), P(None, tp), P(None, tp), P(None, tp), P(), P(), P(tp),
        P(None, tp), P(None, tp), P(None, tp), P(None, tp), P(None, None, tp), P(None, tp),
        P(None, None, tp), P(None, tp), P(SP, None, tp), P(tp), P(tp, None), P(tp, None),
    )
    return jax.shard_map(
        local, mesh=split, in_specs=placed, out_specs=P(SP_TP, None), check_vma=False
    )
```

```python
import jax
import jax.numpy as jnp
import numpy as np
from jax import lax
from jax.experimental import pallas as pl
from jax.experimental.pallas import tpu as pltpu
from jax.sharding import Mesh
from jax.sharding import PartitionSpec as P

SP = ("z", "y")
SP_TP = ("z", "y", "x", "c")
ROWS = 1024
WIDTH = 2048
SEQ = 16384
HEADS = 8
STATE = 128
INNER = 512
CONV = INNER + 2 * STATE
CHUNK = 128
CHUNKS = ROWS // CHUNK
EDGE = 16
WINDOW = 128
HEAD = 64
HALF = 32
QHEADS = 4
LINE = 4
PACK = 2 * STATE + 16

NORM_EPS = 1e-05
ROPE_BASE = 500000.0
NEG_FILL = -1e30
F32 = jnp.float32
BF16 = jnp.bfloat16


def rope_tables():
    frequency = ROPE_BASE ** (-np.arange(0, HEAD, 2, dtype=np.float64) / HEAD)
    offsets = np.arange(-WINDOW, ROWS + WINDOW, dtype=np.float64)
    near = frequency[:, None] * offsets[None, :]
    far = frequency[None, :] * (ROWS * np.arange(SEQ // ROWS, dtype=np.float64))[:, None]
    near_table = np.concatenate([np.cos(near), np.sin(near)], axis=0).astype(np.float32)
    far_table = np.concatenate([np.cos(far), np.sin(far)], axis=1).astype(np.float32)
    return near_table, far_table[:, None, :]


def head_spread():
    spread = np.repeat(np.eye(HEADS, dtype=np.float32), INNER // HEADS, axis=1)
    return np.concatenate([spread, spread], axis=0)


def dot(a, b):
    return jnp.dot(a, b, preferred_element_type=F32)


def dot_nt(a, b):
    return lax.dot_general(a, b, (((1,), (1,)), ((), ())), preferred_element_type=F32)


def dot_tn(a, b):
    return lax.dot_general(a, b, (((0,), (0,)), ((), ())), preferred_element_type=F32)


def silu(v):
    half = 0.5 * v
    return half + half * jnp.tanh(half)


def normalise(tokens, gain):
    t = tokens.astype(F32)
    mean = jnp.mean(t * t, axis=-1, keepdims=True)
    return (t * lax.rsqrt(mean + NORM_EPS) * gain).astype(BF16)


def lane_row(ref):
    value = ref[...].astype(F32)
    return jnp.concatenate([value[k : k + 1] for k in range(value.shape[0])], axis=1)


def column(row):
    size = row.shape[1]
    a = lax.broadcasted_iota(jnp.int32, (size, size), 0)
    b = lax.broadcasted_iota(jnp.int32, (size, size), 1)
    return jnp.sum(jnp.where(a == b, row, 0.0), axis=1, keepdims=True)


def fetch(pairs, sems):
    copies = [pltpu.make_async_copy(a, b, sems.at[k]) for k, (a, b) in enumerate(pairs)]
    for copy in copies:
        copy.start()
    return copies


def widen(rows, spread):
    high = rows.astype(BF16)
    low = (rows - high.astype(F32)).astype(BF16)
    return dot_tn(jnp.concatenate([high, low], axis=0), spread)


def edge_kernel(h_gain, tok, h_k, h_v, low, high, edge, w_kv, gain, sems):
    copies = fetch(
        [
            (tok.at[pl.ds(ROWS - WINDOW, WINDOW)], edge.at[pl.ds(0, WINDOW)]),
            (tok.at[pl.ds(0, WINDOW)], edge.at[pl.ds(WINDOW, WINDOW)]),
            (h_k, w_kv.at[pl.ds(0, HEAD)]), (h_v, w_kv.at[pl.ds(HEAD, HEAD)]), (h_gain, gain),
        ],
        sems,
    )
    for k in (4, 0, 1):
        copies[k].wait()
    n = normalise(edge[...], lane_row(gain))
    for k in (2, 3):
        copies[k].wait()
    kv = dot_nt(w_kv[...], n).astype(BF16)
    for ref, at, rows in ((low, 0, WINDOW - EDGE), (high, WINDOW, WINDOW)):
        ref[:EDGE, :] = edge[rows : rows + EDGE, :]
        for k in range(WIDTH // 128):
            ref[EDGE:, k * 128 : (k + 1) * 128] = kv[k * 8 : (k + 1) * 8, at : at + WINDOW]


BLOCK = 256


def front_kernel(
    gain, w_inner, w_in, w_out, tok, h_step, h_gate, h_q, h_k, h_v,
    normed, rows, raw, w_gate, w_q, w_kv, w_step, sems,
):
    blocks = [pl.ds(k * BLOCK, BLOCK) for k in range(ROWS // BLOCK)]
    waits = fetch(
        [(h_step, w_step)], sems
    )
    late = [
        pltpu.make_async_copy(a, b, sems.at[5 + k])
        for k, (a, b) in enumerate(
            [
                (h_gate, w_gate), (h_q, w_q), (h_k, w_kv.at[pl.ds(0, HEAD)]),
                (h_v, w_kv.at[pl.ds(HEAD, HEAD)]),
            ]
        )
    ]
    g = lane_row(gain)

    def prepare(i):
        normed[blocks[i], :] = normalise(tok[blocks[i], :], g)

    prepare(0)
    waits[0].wait()
    pair = jnp.concatenate([w_in[...], w_out[...]], axis=1)
    for i, block in enumerate(blocks):
        if i + 1 < len(blocks):
            prepare(i + 1)
        if i == 1:
            for copy in late:
                copy.start()
        n = normed[block, :]
        for k in range(0, INNER, 2 * STATE):
            value = dot(n, w_inner[:, k : k + 2 * STATE]).astype(BF16).astype(F32)
            rows[k // STATE, block, :] = value[:, :STATE]
            rows[k // STATE + 1, block, :] = value[:, STATE:]
        value = dot(n, pair).astype(BF16).astype(F32)
        rows[INNER // STATE, block, :] = value[:, :STATE]
        rows[INNER // STATE + 1, block, :] = value[:, STATE:]
        raw[:, block] = dot_nt(w_step[...], n).astype(BF16).astype(F32)
    for copy in late:
        copy.wait()


def state_kernel(
    rate, rows, raw, low, high, gain, w_inner, w_in, w_out, inner_taps, pair_taps, jump, spread,
    x_ref, b_ref, c_ref, cum_ref, step_ref, run_ref, enter_ref, back_ref, state_ref,
    first, last, state_f, state_b,
):
    g = lane_row(gain)
    edge = normalise(jnp.concatenate([low[:EDGE, :], high[:EDGE, :]], axis=0), g)
    for k in range(CONV // STATE):
        if k < INNER // STATE:
            w = w_inner[:, k * STATE : (k + 1) * STATE]
        else:
            w = (w_in if k == INNER // STATE else w_out)[...]
        value = dot(edge, w).astype(BF16).astype(F32)
        first[k, :EDGE, :] = value[:EDGE]
        first[k, EDGE:, :] = rows[k, : CHUNK + EDGE, :]
        last[k, : CHUNK + EDGE, :] = rows[k, ROWS - CHUNK - EDGE :, :]
        last[k, CHUNK + EDGE :, :] = value[EDGE:]
    taps = jnp.concatenate(
        [inner_taps[...].astype(F32)] + [pair_taps[:, k, :].astype(F32) for k in (0, 1)], axis=1
    )
    rates = [
        jnp.concatenate([jnp.full((1, CHUNK), rate[d, h], F32) for h in range(HEADS)], axis=0)
        for d in (0, 1)
    ]
    v = raw[...]
    step = jnp.maximum(v, 0.0) + jnp.log1p(jnp.exp(-jnp.abs(v)))
    step_ref[...] = step
    lane = lax.broadcasted_iota(jnp.int32, (HEADS, CHUNK), 1)
    cums = []
    for k in range(CHUNKS):
        at = slice(k * CHUNK, (k + 1) * CHUNK)
        f = jump[:HEADS, at] - rates[0] * step[:HEADS, at]
        r = jump[HEADS:, at] - rates[1] * step[HEADS:, at]
        for shift in (1, 2, 4, 8, 16, 32, 64):
            f = f + jnp.where(lane >= shift, pltpu.roll(f, shift, 1), 0.0)
            r = r + jnp.where(lane < CHUNK - shift, pltpu.roll(r, CHUNK - shift, 1), 0.0)
        cums.append((f, r))
        cum_ref[:HEADS, k * CHUNK : (k + 1) * CHUNK] = f
        cum_ref[HEADS:, k * CHUNK : (k + 1) * CHUNK] = r
    totals = [(f[:, CHUNK - 1 :], r[:, :1]) for f, r in cums]
    zero = jnp.zeros((HEADS, 1), F32)
    ahead = zero
    for k in range(CHUNKS):
        run_ref[:HEADS, k * CHUNK : (k + 1) * CHUNK] = cums[k][0] + ahead
        ahead = ahead + totals[k][0]
    behind = zero
    for k in reversed(range(CHUNKS)):
        run_ref[HEADS:, k * CHUNK : (k + 1) * CHUNK] = cums[k][1] + behind
        behind = behind + totals[k][1]
    sp = spread[...]
    state_f[...] = jnp.zeros_like(state_f)
    state_b[...] = jnp.zeros_like(state_b)
    passed = zero
    for k in range(CHUNKS):
        if k == 0:
            source, base = first, EDGE - 2
        elif k == CHUNKS - 1:
            source, base = last, EDGE - 2
        else:
            source, base = rows, k * CHUNK - 2
        here = slice(k * CHUNK, (k + 1) * CHUNK)

        def active(tile):
            cols = slice(tile * STATE, (tile + 1) * STATE)
            acc = source[tile, base : base + CHUNK, :] * taps[0:1, cols]
            for t in range(1, 5):
                acc = acc + source[tile, base + t : base + t + CHUNK, :] * taps[t : t + 1, cols]
            return silu(acc)

        f, r = cums[k]
        tf, tr = totals[k]
        wf = jnp.exp(tf - f) * step[:HEADS, here]
        wr = jnp.exp(tr - r) * step[HEADS:, here]
        df = jnp.where(lane == 0, jnp.exp(tf), jnp.exp(passed))
        bm = active(INNER // STATE).astype(BF16)
        b_ref[here, :] = bm
        c_ref[here, :] = active(INNER // STATE + 1).astype(BF16)
        xf = jnp.concatenate([active(tile) for tile in range(INNER // STATE)], axis=1)
        x_ref[here, :] = xf.astype(BF16)
        wide = widen(jnp.concatenate([wf, wr, df], axis=1), sp)
        fresh_f = dot_tn(bm, (xf * wide[:CHUNK]).astype(BF16))
        fresh_b = dot_tn(bm, (xf * wide[CHUNK : 2 * CHUNK]).astype(BF16))
        enter_ref[k] = state_f[...].astype(BF16)
        back_ref[k] = fresh_b.astype(BF16)
        state_f[...] = state_f[...] * wide[2 * CHUNK : 2 * CHUNK + 1] + fresh_f
        state_b[...] = state_b[...] + fresh_b * wide[2 * CHUNK + 1 : 2 * CHUNK + 2]
        passed = passed + tr
    state_ref[:STATE, :] = state_f[...].astype(BF16)
    state_ref[STATE : 2 * STATE, :] = state_b[...].astype(BF16)
    parts = jnp.zeros((HEADS, CHUNK), F32)
    column = 0
    for total in (ahead, passed):
        rest = total
        for _ in range(3):
            piece = rest.astype(BF16).astype(F32)
            rest = rest - piece
            parts = jnp.where(lane == column, piece, parts)
            column += 1
    state_ref[2 * STATE :, :] = dot_tn(parts.astype(BF16), sp[:HEADS]).astype(BF16)[:16]


def logs_of(ref):
    tail = ref[2 * STATE :, :].astype(F32)
    return tail[0:1] + tail[1:2] + tail[2:3], tail[3:4] + tail[4:5] + tail[5:6]


def line_kernel(own, d1, d2, d3, m1, m2, m3, part_ref):
    place, level = lax.axis_index("y"), lax.axis_index("z")
    got = (own, d1, d2, d3)
    logs = [logs_of(r) for r in got]
    state = lambda r, back: r[STATE * back : STATE * (back + 1), :].astype(F32)
    totals = []
    for back in (0, 1):
        near = (lambda d: d) if back == 0 else (lambda d: LINE - d)
        count = place if back == 0 else LINE - 1 - place
        far_count = LINE - 1 - count
        prefix = jnp.zeros((STATE, INNER), F32)
        log_prefix = jnp.zeros((1, INNER), F32)
        for d in range(1, LINE):
            r = near(d)
            live = d <= count
            weight = jnp.where(live, jnp.exp(log_prefix), 0.0)
            prefix = prefix + weight * state(got[r], back)
            log_prefix = log_prefix + jnp.where(live, logs[r][back], 0.0)
        total = jnp.zeros((STATE, INNER), F32)
        suffix = jnp.zeros((1, INNER), F32)
        for e in reversed(range(1, LINE)):
            r = near(LINE - e)
            live = e <= far_count
            weight = jnp.where(live, jnp.exp(suffix), 0.0)
            total = total + weight * state(got[r], back)
            suffix = suffix + jnp.where(live, logs[r][back], 0.0)
        total = total + jnp.exp(suffix) * state(own, back)
        suffix = suffix + logs[0][back]
        total = total + jnp.exp(suffix) * prefix
        part_ref[STATE * back : STATE * (back + 1), :] = prefix
        part_ref[2 * STATE + back : 2 * STATE + back + 1, :] = log_prefix
        rest = suffix + log_prefix
        pieces = []
        for _ in range(3):
            piece = rest.astype(BF16).astype(F32)
            rest = rest - piece
            pieces.append(piece)
        pieces.append(jnp.zeros((13, INNER), F32))
        totals.append((total.astype(BF16), jnp.concatenate(pieces, axis=0).astype(BF16)))
    for d, ref in ((1, m1), (2, m2), (3, m3)):
        for back in (0, 1):

            @pl.when(level + d < LINE if back == 0 else level + d >= LINE)
            def _(ref=ref, back=back):
                ref[:STATE, :] = totals[back][0]
                ref[STATE:, :] = totals[back][1]


def heads_kernel(
    normed, low, high, w_gate, w_q, w_kv, q_row, k_row, near, far, gate, qs, ks, vs
):
    q_gain, k_gain = column(q_row[...]), column(k_row[...])
    turns = column(far[lax.axis_index(SP)])
    far_cos = turns[:HALF, :]
    far_sin = turns[HALF:, :]
    scale = jnp.asarray(HEAD**-0.5, BF16)

    def turn(head, at, size):
        co = near[:HALF, at : at + size]
        so = near[HALF:, at : at + size]
        cos = far_cos * co - far_sin * so
        sin = far_sin * co + far_cos * so
        u, w = head[:HALF], head[HALF:]
        return jnp.concatenate([u * cos - w * sin, w * cos + u * sin], axis=0)

    def head_norm(head, scale):
        mean = jnp.mean(head * head, axis=0, keepdims=True)
        return head * lax.rsqrt(mean + NORM_EPS) * scale

    def keys_values(kv, at, size):
        k = head_norm(kv[:HEAD].astype(F32), k_gain)
        ks[:, at : at + size] = turn(k, at, size).astype(BF16)
        vs[:, at : at + size] = kv[HEAD:]

    for i in range(4):
        at = WINDOW + i * 256
        n = normed[i * 256 : (i + 1) * 256, :]
        keys_values(dot_nt(w_kv[...], n).astype(BF16), at, 256)
        gate[i * 256 : (i + 1) * 256, :] = dot(n, w_gate[...]).astype(BF16)
        q = dot(n, w_q[...]).astype(BF16).astype(F32).T
        for h in range(QHEADS):
            head = turn(head_norm(q[h * HEAD : (h + 1) * HEAD], q_gain), at, 256)
            qs[h * HEAD : (h + 1) * HEAD, i * 256 : (i + 1) * 256] = head.astype(BF16) * scale
    for ref, at in ((low, 0), (high, WINDOW + ROWS)):
        tiles = [ref[EDGE:, k * 128 : (k + 1) * 128] for k in range(WIDTH // 128)]
        keys_values(jnp.concatenate(tiles, axis=0), at, WINDOW)


def attend_kernel(sink, qs, ks, vs, attn_ref, even_mask, odd_mask, even, odd):
    reach = 3 * WINDOW
    pairs = ROWS // WINDOW // 2
    jj = lax.broadcasted_iota(jnp.int32, (reach, WINDOW), 0)
    ii = lax.broadcasted_iota(jnp.int32, (reach, WINDOW), 1)
    band = (jj >= ii) & (jj <= ii + 2 * WINDOW)
    first = lax.axis_index(SP) * ROWS - WINDOW

    def set_mask(mask, j):
        position = jj + (first + j * WINDOW)
        mask[...] = jnp.where(band & (position >= 0) & (position < SEQ), 0.0, NEG_FILL)

    def scores(j, out):
        here = pl.multiple_of(j * WINDOW, 128)
        qb = jnp.concatenate(
            [qs[h * HEAD : (h + 1) * HEAD, pl.ds(here, WINDOW)] for h in range(QHEADS)], axis=1
        )
        out[...] = dot_tn(ks[:, pl.ds(here, reach)], qb)

    def outputs(j, mask, saved):
        here = pl.multiple_of(j * WINDOW, 128)
        weights = []
        for h in range(QHEADS):
            s = saved[:, h * WINDOW : (h + 1) * WINDOW] + mask[...]
            top = jnp.maximum(jnp.max(s, axis=0, keepdims=True), sink[h])
            p = jnp.exp(s - top)
            scale = 1.0 / (jnp.sum(p, axis=0, keepdims=True) + jnp.exp(sink[h] - top))
            weights.append((p * scale).astype(BF16))
        o = dot(vs[:, pl.ds(here, reach)], jnp.concatenate(weights, axis=1))
        o = jnp.concatenate([o[:, h * WINDOW : (h + 1) * WINDOW] for h in range(QHEADS)], axis=0)
        attn_ref[pl.ds(here, WINDOW), :] = o.T.astype(BF16)

    set_mask(even_mask, 0)
    set_mask(odd_mask, 1)
    scores(0, even)

    def pair(i, _):
        @pl.when(i == 1)
        def _():
            set_mask(even_mask, 2)

        @pl.when(i == pairs - 1)
        def _():
            set_mask(odd_mask, 2 * pairs - 1)

        scores(2 * i + 1, odd)
        outputs(2 * i, even_mask, even)
        scores(jnp.minimum(2 * i + 2, 2 * pairs - 1), even)
        outputs(2 * i + 1, odd_mask, odd)
        return 0

    lax.fori_loop(0, pairs, pair, 0)


def mixer_kernel(x_ref, b_ref, c_ref, cum_ref, step_ref, enter_ref, back_ref, spread, y_ref, state):
    state[...] = jnp.zeros_like(state)
    tt = lax.broadcasted_iota(jnp.int32, (CHUNK, CHUNK), 0)
    ss = lax.broadcasted_iota(jnp.int32, (CHUNK, CHUNK), 1)
    below, same, left = tt > ss, tt == ss, ss < HEAD
    nothing = jnp.zeros((CHUNK, CHUNK), BF16)

    def chunk(i, _):
        k = CHUNKS - 1 - i
        at = pl.ds(pl.multiple_of(k * CHUNK, 128), CHUNK)
        c = c_ref[at, :]
        scores = dot_nt(c, b_ref[at, :])
        cum = cum_ref[:, at]
        step = step_ref[:, at]
        f, r = cum[:HEADS], cum[HEADS:]
        sf, sr = step[:HEADS], step[HEADS:]
        row_f = jnp.log(sf) - f
        row_r = jnp.log(sr) - r
        row_d = jnp.log(sf + sr)
        columns = cum.T

        def weights(h):
            lower = columns[:, h : h + 1] + row_f[h : h + 1]
            upper = columns[:, HEADS + h : HEADS + h + 1] + row_r[h : h + 1]
            power = jnp.where(below, lower, jnp.where(same, row_d[h : h + 1], upper))
            return (jnp.exp(power) * scores).astype(BF16)

        wide = widen(jnp.concatenate([jnp.exp(f), jnp.exp(r)], axis=1), spread[...])
        across = wide[:CHUNK] * dot(c, enter_ref[k])
        across = across + wide[CHUNK:] * dot(c, state[...].astype(BF16))
        for pair in range(HEADS // 2):
            cols = slice(pair * 2 * HEAD, (pair + 1) * 2 * HEAD)
            both = jnp.concatenate([weights(2 * pair), weights(2 * pair + 1)], axis=1)
            xp = x_ref[at, cols]
            stacked = jnp.concatenate(
                [jnp.where(left, xp, nothing), jnp.where(left, nothing, xp)], axis=0
            )
            y_ref[at, cols] = dot(both, stacked) + across[:, cols]
        state[...] = state[...] * wide[CHUNK : CHUNK + 1] + back_ref[k].astype(F32)
        return 0

    lax.fori_loop(0, CHUNKS, chunk, 0)


def finish_rows(core, y, c, run, gate, attn, gain, spread, from_low, from_high, out):
    scales = lane_row(gain)
    for i in range(LINE):
        at = pl.ds(pl.multiple_of(i * 256 + core * 128, 128), 128)
        cm = c[at, :]
        reach = jnp.exp(run[:, at])
        wide = widen(jnp.concatenate([reach[:HEADS], reach[HEADS:]], axis=1), spread[...])
        v = y[at, :] + wide[:128] * dot(cm, from_low[...]) + wide[128:] * dot(cm, from_high[...])
        v = v * silu(gate[at, :].astype(F32))
        mean = jnp.mean(v * v, axis=-1, keepdims=True)
        out[i, :, : QHEADS * HEAD] = attn[at, :]
        out[i, :, QHEADS * HEAD :] = (v * lax.rsqrt(mean + NORM_EPS) * scales).astype(BF16)


def theirs_kernel(
    part, d1, d2, d3, y, c, run, gate, attn, gain, spread, theirs, from_low, from_high
):
    got = (None, d1, d2, d3)
    level = lax.axis_index("z")
    for back, keep in ((0, from_low), (1, from_high)):
        count = level if back == 0 else LINE - 1 - level
        prefix = jnp.zeros((STATE, INNER), F32)
        log_prefix = jnp.zeros((1, INNER), F32)
        for d in range(1, LINE):
            r = got[d if back == 0 else LINE - d]
            live = d <= count
            weight = jnp.where(live, jnp.exp(log_prefix), 0.0)
            prefix = prefix + weight * r[:STATE, :].astype(F32)
            tail = r[STATE:, :].astype(F32)
            log = tail[0:1] + tail[1:2] + tail[2:3]
            log_prefix = log_prefix + jnp.where(live, log, 0.0)
        own = part[STATE * back : STATE * (back + 1), :]
        reach = jnp.exp(part[2 * STATE + back : 2 * STATE + back + 1, :])
        keep[...] = (own + reach * prefix).astype(BF16)
    core = 1 - lax.axis_index("c")
    finish_rows(core, y, c, run, gate, attn, gain, spread, from_low, from_high, theirs)


def mine_kernel(y, c, run, gate, attn, gain, spread, from_low, from_high, wa, ws, mine, first):
    finish_rows(lax.axis_index("c"), y, c, run, gate, attn, gain, spread, from_low, from_high, mine)
    first[...] = partial(mine[(lax.axis_index("x") + 2) % LINE], wa, ws)


def sum_kernel(own, direct_right, direct_left, last_right, last_left, out):
    upper = own[:HALVES] + direct_left[...].astype(F32) + last_right[...].astype(F32)
    lower = own[HALVES:] + direct_right[...].astype(F32) + last_left[...].astype(F32)
    out[:HALVES] = upper.astype(BF16)
    out[HALVES:] = lower.astype(BF16)


def partial(v, a, b):
    split = QHEADS * HEAD
    return (dot(v[:, :split], a[...]) + dot(v[:, split:], b[...])).astype(BF16).astype(F32)


def chunk_partial(order, mine, theirs, wa, ws, pa, ps):
    join = lambda ref: jnp.concatenate([ref[index] for index in order], axis=0)
    return partial(join(mine), wa, ws) + partial(join(theirs), pa, ps)


HALVES = 64


def opposite_kernel(first, theirs, pa, ps, right, left):
    value = first[...] + partial(theirs[(lax.axis_index("x") + 2) % LINE], pa, ps)
    right[...] = value[:HALVES].astype(BF16)
    left[...] = value[HALVES:].astype(BF16)


def beside_kernel(mine, theirs, wa, ws, pa, ps, right, left, keep_right, keep_left, own):
    x = lax.axis_index("x")
    order = [(x + 1) % LINE, (x + 3) % LINE, x]
    value = chunk_partial(order, mine, theirs, wa, ws, pa, ps)
    keep_right[...] = value[:HALVES]
    right[...] = value[HALVES : 2 * HALVES].astype(BF16)
    left[...] = value[2 * HALVES : 3 * HALVES].astype(BF16)
    keep_left[...] = value[3 * HALVES : 4 * HALVES]
    own[...] = value[4 * HALVES :]


HBM = pl.BlockSpec(memory_space=pltpu.HBM)


def whole(count):
    return [pl.BlockSpec(memory_space=pltpu.VMEM)] * count


SCALARS = pl.BlockSpec(memory_space=pltpu.SMEM)


def plain(kernel, name, inputs, outs, scalars=0, remote=0, scratch=(), size=8, flops=1e9):
    return pl.pallas_call(
        kernel,
        in_specs=[SCALARS] * scalars + whole(inputs) + [HBM] * remote,
        out_specs=whole(len(outs)),
        out_shape=outs,
        scratch_shapes=list(scratch),
        compiler_params=pltpu.CompilerParams(vmem_limit_bytes=size << 20),
        cost_estimate=cost(flops),
        name=name,
    )


def fixed(shape):
    return pl.BlockSpec(memory_space=pltpu.VMEM)


def params(size):
    return pltpu.CompilerParams(dimension_semantics=("arbitrary",), vmem_limit_bytes=size << 20)


def cost(flops):
    return pl.CostEstimate(flops=int(flops), transcendentals=0, bytes_accessed=8 << 20)


def shaped(shape, dtype):
    return jax.ShapeDtypeStruct(shape, dtype)


def local(
    tokens, norm_gain, query_weight, key_weight, value_weight, query_gain, key_gain, sink_logit,
    gate_weight, inner_weight, input_map, output_map, step_weight, conv_inner, conv_pair,
    decay_rate, decay_jump, inner_gain, attn_out_weight, ssm_out_weight,
):
    up = [(k, k + 1) for k in range(15)]
    down = [(k + 1, k) for k in range(15)]
    swap = [(0, 1), (1, 0)]
    pin = lambda v: pltpu.with_memory_space_constraint(v, pltpu.HBM)
    gain = norm_gain.reshape(WIDTH // 128, 128)
    halo = shaped((EDGE + 8, WIDTH), BF16)
    edge_low, edge_high = plain(
        edge_kernel, "edge", 0, [halo, halo], remote=4,
        scratch=[
            pltpu.VMEM((2 * WINDOW, WIDTH), BF16), pltpu.VMEM((2 * HEAD, WIDTH), BF16),
            pltpu.VMEM((WIDTH // 128, 128), BF16), pltpu.SemaphoreType.DMA((5,)),
        ],
        size=6, flops=1e10,
    )(*map(pin, (gain, tokens, key_weight.T, value_weight.T)))
    halo_low = lax.ppermute(edge_low, SP, up)
    halo_high = lax.ppermute(edge_high, SP, down)

    spread = jnp.asarray(head_spread(), BF16)
    step_rows = jnp.transpose(step_weight, (1, 2, 0)).reshape(2 * HEADS, WIDTH)
    jump = jnp.transpose(decay_jump, (1, 2, 0)).reshape(2 * HEADS, ROWS)
    normed, rows, raw, w_gate, w_q, w_kv = plain(
        front_kernel, "front", 5,
        [
            shaped((ROWS, WIDTH), BF16), shaped((CONV // STATE, ROWS, STATE), F32),
            shaped((2 * HEADS, ROWS), F32), shaped((WIDTH, INNER), BF16),
            shaped((WIDTH, QHEADS * HEAD), BF16), shaped((2 * HEAD, WIDTH), BF16),
        ],
        remote=5,
        scratch=[pltpu.VMEM((2 * HEADS, WIDTH), BF16), pltpu.SemaphoreType.DMA((9,))],
        size=8, flops=10e9,
    )(gain, inner_weight, input_map, output_map, tokens, *map(pin, (step_rows, gate_weight, query_weight,
      key_weight.T, value_weight.T)))

    x, b, c, cum, step, run, enter, back, state = plain(
        state_kernel, "state", 12,
        [
            shaped((ROWS, INNER), BF16), shaped((ROWS, STATE), BF16),
            shaped((ROWS, STATE), BF16), shaped((2 * HEADS, ROWS), F32),
            shaped((2 * HEADS, ROWS), F32), shaped((2 * HEADS, ROWS), F32),
            shaped((CHUNKS, STATE, INNER), BF16), shaped((CHUNKS, STATE, INNER), BF16),
            shaped((PACK, INNER), BF16),
        ],
        scalars=1,
        scratch=[pltpu.VMEM((CONV // STATE, CHUNK + 2 * EDGE, STATE), F32)] * 2
        + [pltpu.VMEM((STATE, INNER), F32)] * 2,
        size=8, flops=6e9,
    )(decay_rate, rows, raw, halo_low, halo_high, gain, inner_weight, input_map, output_map, conv_inner, conv_pair,
      jump, spread)

    def along(values, axis):
        sent = {
            d: lax.ppermute(values[d - 1], axis, [(k, (k + d) % LINE) for k in range(LINE)])
            for d in (1, 3, 2)
        }
        return [sent[d] for d in (1, 2, 3)]

    got = along([state] * 3, "y")

    near, far = rope_tables()
    gate, qs, ks, vs = plain(
        heads_kernel, "heads", 10,
        [
            shaped((ROWS, INNER), BF16), shaped((QHEADS * HEAD, ROWS), BF16), shaped((HEAD, ROWS + 2 * WINDOW), BF16),
            shaped((HEAD, ROWS + 2 * WINDOW), BF16),
        ],
        size=6, flops=7e9,
    )(normed, halo_low, halo_high, w_gate, w_q, w_kv, query_gain[None, :], key_gain[None, :],
      jnp.asarray(near), jnp.asarray(far))

    *messages, part = plain(
        line_kernel, "line", 4,
        [shaped((STATE + 16, INNER), BF16)] * 3 + [shaped((PACK, INNER), F32)],
        size=4, flops=1e9,
    )(state, *got)

    far_got = along(messages, "z")

    attn = plain(
        attend_kernel, "attend", 3, [shaped((ROWS, QHEADS * HEAD), BF16)], scalars=1,
        scratch=[pltpu.VMEM((3 * WINDOW, WINDOW), F32)] * 2
        + [pltpu.VMEM((3 * WINDOW, QHEADS * WINDOW), F32)] * 2,
        size=8, flops=7e9,
    )(sink_logit, qs, ks, vs)[0]

    y = plain(
        mixer_kernel, "mixer", 8, [shaped((ROWS, INNER), F32)],
        scratch=[pltpu.VMEM((STATE, INNER), F32)], flops=10e9,
    )(x, b, c, cum, step, enter, back, spread)[0]

    attn_own, ssm_own, y = lax.optimization_barrier((attn_out_weight, ssm_out_weight, y))
    attn_partner = lax.ppermute(attn_own, "c", swap)
    ssm_partner = lax.ppermute(ssm_own, "c", swap)

    depth = QHEADS * HEAD + INNER
    rest = (y, c, run, gate, attn, inner_gain.reshape(INNER // 128, 128), spread)
    incoming = shaped((STATE, INNER), BF16)
    theirs, from_low, from_high = plain(
        theirs_kernel, "theirs", 11, [shaped((4, 128, depth), BF16), incoming, incoming], flops=2e9
    )(part, *far_got, *rest)
    theirs = lax.ppermute(theirs, "c", swap)
    mine, first = plain(
        mine_kernel, "mine", 11, [shaped((4, 128, depth), BF16), shaped((128, WIDTH), F32)], flops=2e9
    )(*rest, from_low, from_high, attn_out_weight, ssm_out_weight)
    operands = (
        mine, theirs, attn_out_weight, ssm_out_weight, attn_partner, ssm_partner
    )
    sent = shaped((HALVES, WIDTH), BF16)
    kept = shaped((HALVES, WIDTH), F32)
    right = [(k, (k + 1) % LINE) for k in range(LINE)]
    left = [((k + 1) % LINE, k) for k in range(LINE)]
    shift_right = lambda value: lax.ppermute(value, "x", right)
    shift_left = lambda value: lax.ppermute(value, "x", left)
    relay_right, relay_left = plain(
        opposite_kernel, "opposite", 4, [sent, sent], flops=1e9
    )(first, theirs, attn_partner, ssm_partner)
    relay_right = shift_right(relay_right)
    relay_left = shift_left(relay_left)
    direct_right, direct_left, keep_right, keep_left, own = plain(
        beside_kernel, "beside", 6, [sent, sent, kept, kept, shaped((2 * HALVES, WIDTH), F32)],
        flops=3e9,
    )(*operands)
    direct_right = shift_right(direct_right)
    direct_left = shift_left(direct_left)
    last_right = shift_right((keep_right + relay_right.astype(F32)).astype(BF16))
    last_left = shift_left((keep_left + relay_left.astype(F32)).astype(BF16))
    return plain(
        sum_kernel, "sum", 5, [shaped((2 * HALVES, WIDTH), BF16)], size=4, flops=1e6
    )(own, direct_right, direct_left, last_right, last_left)[0]


def solution(mesh):
    split = Mesh(mesh.devices.reshape(4, 4, 4, 2), SP_TP)
    tp = ("x", "c")
    placed = (
        P(SP, None), P(), P(None, tp), P(None, tp), P(None, tp), P(), P(), P(tp),
        P(None, tp), P(None, tp), P(None, tp), P(None, tp), P(None, None, tp), P(None, tp),
        P(None, None, tp), P(None, tp), P(SP, None, tp), P(tp), P(tp, None), P(tp, None),
    )
    return jax.shard_map(
        local, mesh=split, in_specs=placed, out_specs=P(SP_TP, None), check_vma=False
    )
```

```python
import jax
import jax.numpy as jnp
import numpy as np
from jax import lax
from jax.experimental import pallas as pl
from jax.experimental.pallas import tpu as pltpu
from jax.sharding import Mesh
from jax.sharding import PartitionSpec as P

SP = ("z", "y")
SP_TP = ("z", "y", "x", "c")
ROWS = 1024
WIDTH = 2048
SEQ = 16384
HEADS = 8
STATE = 128
INNER = 512
CONV = INNER + 2 * STATE
CHUNK = 128
CHUNKS = ROWS // CHUNK
EDGE = 16
WINDOW = 128
HEAD = 64
HALF = 32
QHEADS = 4
LINE = 4
PACK = 2 * STATE + 16

NORM_EPS = 1e-05
ROPE_BASE = 500000.0
NEG_FILL = -1e30
F32 = jnp.float32
BF16 = jnp.bfloat16


def rope_tables():
    frequency = ROPE_BASE ** (-np.arange(0, HEAD, 2, dtype=np.float64) / HEAD)
    offsets = np.arange(-WINDOW, ROWS + WINDOW, dtype=np.float64)
    near = frequency[:, None] * offsets[None, :]
    far = frequency[None, :] * (ROWS * np.arange(SEQ // ROWS, dtype=np.float64))[:, None]
    near_table = np.concatenate([np.cos(near), np.sin(near)], axis=0).astype(np.float32)
    far_table = np.concatenate([np.cos(far), np.sin(far)], axis=1).astype(np.float32)
    return near_table, far_table[:, None, :]


def head_spread():
    spread = np.repeat(np.eye(HEADS, dtype=np.float32), INNER // HEADS, axis=1)
    return np.concatenate([spread, spread], axis=0)


def dot(a, b):
    return jnp.dot(a, b, preferred_element_type=F32)


def dot_nt(a, b):
    return lax.dot_general(a, b, (((1,), (1,)), ((), ())), preferred_element_type=F32)


def dot_tn(a, b):
    return lax.dot_general(a, b, (((0,), (0,)), ((), ())), preferred_element_type=F32)


def silu(v):
    half = 0.5 * v
    return half + half * jnp.tanh(half)


def normalise(tokens, gain):
    t = tokens.astype(F32)
    mean = jnp.mean(t * t, axis=-1, keepdims=True)
    return (t * lax.rsqrt(mean + NORM_EPS) * gain).astype(BF16)


def lane_row(ref):
    value = ref[...].astype(F32)
    return jnp.concatenate([value[k : k + 1] for k in range(value.shape[0])], axis=1)


def column(row):
    size = row.shape[1]
    a = lax.broadcasted_iota(jnp.int32, (size, size), 0)
    b = lax.broadcasted_iota(jnp.int32, (size, size), 1)
    return jnp.sum(jnp.where(a == b, row, 0.0), axis=1, keepdims=True)


def fetch(pairs, sems):
    copies = [pltpu.make_async_copy(a, b, sems.at[k]) for k, (a, b) in enumerate(pairs)]
    for copy in copies:
        copy.start()
    return copies


def widen(rows, spread):
    high = rows.astype(BF16)
    low = (rows - high.astype(F32)).astype(BF16)
    return dot_tn(jnp.concatenate([high, low], axis=0), spread)


def edge_kernel(h_gain, tok, h_k, h_v, low, high, edge, w_kv, gain, sems):
    copies = fetch(
        [
            (tok.at[pl.ds(ROWS - WINDOW, WINDOW)], edge.at[pl.ds(0, WINDOW)]),
            (tok.at[pl.ds(0, WINDOW)], edge.at[pl.ds(WINDOW, WINDOW)]),
            (h_k, w_kv.at[pl.ds(0, HEAD)]), (h_v, w_kv.at[pl.ds(HEAD, HEAD)]), (h_gain, gain),
        ],
        sems,
    )
    for k in (4, 0, 1):
        copies[k].wait()
    n = normalise(edge[...], lane_row(gain))
    for k in (2, 3):
        copies[k].wait()
    kv = dot_nt(w_kv[...], n).astype(BF16)
    for ref, at, rows in ((low, 0, WINDOW - EDGE), (high, WINDOW, WINDOW)):
        ref[:EDGE, :] = edge[rows : rows + EDGE, :]
        for k in range(WIDTH // 128):
            ref[EDGE:, k * 128 : (k + 1) * 128] = kv[k * 8 : (k + 1) * 8, at : at + WINDOW]


BLOCK = 256


def front_kernel(
    gain, w_inner, w_in, w_out, tok, h_step, h_gate, h_q, h_k, h_v,
    normed, rows, raw, w_gate, w_q, w_kv, w_step, sems,
):
    blocks = [pl.ds(k * BLOCK, BLOCK) for k in range(ROWS // BLOCK)]
    waits = fetch(
        [(h_step, w_step)], sems
    )
    late = [
        pltpu.make_async_copy(a, b, sems.at[5 + k])
        for k, (a, b) in enumerate(
            [
                (h_gate, w_gate), (h_q, w_q), (h_k, w_kv.at[pl.ds(0, HEAD)]),
                (h_v, w_kv.at[pl.ds(HEAD, HEAD)]),
            ]
        )
    ]
    g = lane_row(gain)

    def prepare(i):
        normed[blocks[i], :] = normalise(tok[blocks[i], :], g)

    prepare(0)
    waits[0].wait()
    pair = jnp.concatenate([w_in[...], w_out[...]], axis=1)
    for i, block in enumerate(blocks):
        if i + 1 < len(blocks):
            prepare(i + 1)
        if i == 1:
            for copy in late:
                copy.start()
        n = normed[block, :]
        for k in range(0, INNER, 2 * STATE):
            value = dot(n, w_inner[:, k : k + 2 * STATE]).astype(BF16).astype(F32)
            rows[k // STATE, block, :] = value[:, :STATE]
            rows[k // STATE + 1, block, :] = value[:, STATE:]
        value = dot(n, pair).astype(BF16).astype(F32)
        rows[INNER // STATE, block, :] = value[:, :STATE]
        rows[INNER // STATE + 1, block, :] = value[:, STATE:]
        raw[:, block] = dot_nt(w_step[...], n).astype(BF16).astype(F32)
    for copy in late:
        copy.wait()


def state_kernel(
    rate, rows, raw, low, high, gain, w_inner, w_in, w_out, inner_taps, pair_taps, jump, spread,
    x_ref, b_ref, c_ref, cum_ref, step_ref, run_ref, enter_ref, back_ref, state_ref,
    first, last, state_f, state_b,
):
    g = lane_row(gain)
    edge = normalise(jnp.concatenate([low[:EDGE, :], high[:EDGE, :]], axis=0), g)
    for k in range(CONV // STATE):
        if k < INNER // STATE:
            w = w_inner[:, k * STATE : (k + 1) * STATE]
        else:
            w = (w_in if k == INNER // STATE else w_out)[...]
        value = dot(edge, w).astype(BF16).astype(F32)
        first[k, :EDGE, :] = value[:EDGE]
        first[k, EDGE:, :] = rows[k, : CHUNK + EDGE, :]
        last[k, : CHUNK + EDGE, :] = rows[k, ROWS - CHUNK - EDGE :, :]
        last[k, CHUNK + EDGE :, :] = value[EDGE:]
    taps = jnp.concatenate(
        [inner_taps[...].astype(F32)] + [pair_taps[:, k, :].astype(F32) for k in (0, 1)], axis=1
    )
    rates = [
        jnp.concatenate([jnp.full((1, CHUNK), rate[d, h], F32) for h in range(HEADS)], axis=0)
        for d in (0, 1)
    ]
    v = raw[...]
    step = jnp.maximum(v, 0.0) + jnp.log1p(jnp.exp(-jnp.abs(v)))
    step_ref[...] = step
    lane = lax.broadcasted_iota(jnp.int32, (HEADS, CHUNK), 1)
    cums = []
    for k in range(CHUNKS):
        at = slice(k * CHUNK, (k + 1) * CHUNK)
        f = jump[:HEADS, at] - rates[0] * step[:HEADS, at]
        r = jump[HEADS:, at] - rates[1] * step[HEADS:, at]
        for shift in (1, 2, 4, 8, 16, 32, 64):
            f = f + jnp.where(lane >= shift, pltpu.roll(f, shift, 1), 0.0)
            r = r + jnp.where(lane < CHUNK - shift, pltpu.roll(r, CHUNK - shift, 1), 0.0)
        cums.append((f, r))
        cum_ref[:HEADS, k * CHUNK : (k + 1) * CHUNK] = f
        cum_ref[HEADS:, k * CHUNK : (k + 1) * CHUNK] = r
    totals = [(f[:, CHUNK - 1 :], r[:, :1]) for f, r in cums]
    zero = jnp.zeros((HEADS, 1), F32)
    ahead = zero
    for k in range(CHUNKS):
        run_ref[:HEADS, k * CHUNK : (k + 1) * CHUNK] = cums[k][0] + ahead
        ahead = ahead + totals[k][0]
    behind = zero
    for k in reversed(range(CHUNKS)):
        run_ref[HEADS:, k * CHUNK : (k + 1) * CHUNK] = cums[k][1] + behind
        behind = behind + totals[k][1]
    sp = spread[...]
    state_f[...] = jnp.zeros_like(state_f)
    state_b[...] = jnp.zeros_like(state_b)
    passed = zero
    for k in range(CHUNKS):
        if k == 0:
            source, base = first, EDGE - 2
        elif k == CHUNKS - 1:
            source, base = last, EDGE - 2
        else:
            source, base = rows, k * CHUNK - 2
        here = slice(k * CHUNK, (k + 1) * CHUNK)

        def active(tile):
            cols = slice(tile * STATE, (tile + 1) * STATE)
            acc = source[tile, base : base + CHUNK, :] * taps[0:1, cols]
            for t in range(1, 5):
                acc = acc + source[tile, base + t : base + t + CHUNK, :] * taps[t : t + 1, cols]
            return silu(acc)

        f, r = cums[k]
        tf, tr = totals[k]
        wf = jnp.exp(tf - f) * step[:HEADS, here]
        wr = jnp.exp(tr - r) * step[HEADS:, here]
        df = jnp.where(lane == 0, jnp.exp(tf), jnp.exp(passed))
        bm = active(INNER // STATE).astype(BF16)
        b_ref[here, :] = bm
        c_ref[here, :] = active(INNER // STATE + 1).astype(BF16)
        xf = jnp.concatenate([active(tile) for tile in range(INNER // STATE)], axis=1)
        x_ref[here, :] = xf.astype(BF16)
        wide = widen(jnp.concatenate([wf, wr, df], axis=1), sp)
        fresh_f = dot_tn(bm, (xf * wide[:CHUNK]).astype(BF16))
        fresh_b = dot_tn(bm, (xf * wide[CHUNK : 2 * CHUNK]).astype(BF16))
        enter_ref[k] = state_f[...].astype(BF16)
        back_ref[k] = fresh_b.astype(BF16)
        state_f[...] = state_f[...] * wide[2 * CHUNK : 2 * CHUNK + 1] + fresh_f
        state_b[...] = state_b[...] + fresh_b * wide[2 * CHUNK + 1 : 2 * CHUNK + 2]
        passed = passed + tr
    state_ref[:STATE, :] = state_f[...].astype(BF16)
    state_ref[STATE : 2 * STATE, :] = state_b[...].astype(BF16)
    parts = jnp.zeros((HEADS, CHUNK), F32)
    column = 0
    for total in (ahead, passed):
        rest = total
        for _ in range(3):
            piece = rest.astype(BF16).astype(F32)
            rest = rest - piece
            parts = jnp.where(lane == column, piece, parts)
            column += 1
    state_ref[2 * STATE :, :] = dot_tn(parts.astype(BF16), sp[:HEADS]).astype(BF16)[:16]


def logs_of(ref):
    tail = ref[2 * STATE :, :].astype(F32)
    return tail[0:1] + tail[1:2] + tail[2:3], tail[3:4] + tail[4:5] + tail[5:6]


def line_kernel(own, d3, d2, d1, m1, m2, m3, part_ref):
    place, level = lax.axis_index("y"), lax.axis_index("z")
    got = (own, d1, d2, d3)
    logs = [logs_of(r) for r in got]
    state = lambda r, back: r[STATE * back : STATE * (back + 1), :].astype(F32)
    totals = []
    for back in (0, 1):
        near = (lambda d: d) if back == 0 else (lambda d: LINE - d)
        count = place if back == 0 else LINE - 1 - place
        far_count = LINE - 1 - count
        prefix = jnp.zeros((STATE, INNER), F32)
        log_prefix = jnp.zeros((1, INNER), F32)
        for d in range(1, LINE):
            r = near(d)
            live = d <= count
            weight = jnp.where(live, jnp.exp(log_prefix), 0.0)
            prefix = prefix + weight * state(got[r], back)
            log_prefix = log_prefix + jnp.where(live, logs[r][back], 0.0)
        total = jnp.zeros((STATE, INNER), F32)
        suffix = jnp.zeros((1, INNER), F32)
        for e in reversed(range(1, LINE)):
            r = near(LINE - e)
            live = e <= far_count
            weight = jnp.where(live, jnp.exp(suffix), 0.0)
            total = total + weight * state(got[r], back)
            suffix = suffix + jnp.where(live, logs[r][back], 0.0)
        total = total + jnp.exp(suffix) * state(own, back)
        suffix = suffix + logs[0][back]
        total = total + jnp.exp(suffix) * prefix
        part_ref[STATE * back : STATE * (back + 1), :] = prefix
        part_ref[2 * STATE + back : 2 * STATE + back + 1, :] = log_prefix
        rest = suffix + log_prefix
        pieces = []
        for _ in range(3):
            piece = rest.astype(BF16).astype(F32)
            rest = rest - piece
            pieces.append(piece)
        pieces.append(jnp.zeros((13, INNER), F32))
        totals.append((total.astype(BF16), jnp.concatenate(pieces, axis=0).astype(BF16)))
    for d, ref in ((1, m1), (2, m2), (3, m3)):
        for back in (0, 1):

            @pl.when(level + d < LINE if back == 0 else level + d >= LINE)
            def _(ref=ref, back=back):
                ref[:STATE, :] = totals[back][0]
                ref[STATE:, :] = totals[back][1]


def heads_kernel(
    normed, low, high, w_gate, w_q, w_kv, q_row, k_row, near, far, gate, qs, ks, vs
):
    q_gain, k_gain = column(q_row[...]), column(k_row[...])
    turns = column(far[lax.axis_index(SP)])
    far_cos = turns[:HALF, :]
    far_sin = turns[HALF:, :]
    scale = jnp.asarray(HEAD**-0.5, BF16)

    def turn(head, at, size):
        co = near[:HALF, at : at + size]
        so = near[HALF:, at : at + size]
        cos = far_cos * co - far_sin * so
        sin = far_sin * co + far_cos * so
        u, w = head[:HALF], head[HALF:]
        return jnp.concatenate([u * cos - w * sin, w * cos + u * sin], axis=0)

    def head_norm(head, scale):
        mean = jnp.mean(head * head, axis=0, keepdims=True)
        return head * lax.rsqrt(mean + NORM_EPS) * scale

    def keys_values(kv, at, size):
        k = head_norm(kv[:HEAD].astype(F32), k_gain)
        ks[:, at : at + size] = turn(k, at, size).astype(BF16)
        vs[:, at : at + size] = kv[HEAD:]

    for i in range(4):
        at = WINDOW + i * 256
        n = normed[i * 256 : (i + 1) * 256, :]
        keys_values(dot_nt(w_kv[...], n).astype(BF16), at, 256)
        gate[i * 256 : (i + 1) * 256, :] = dot(n, w_gate[...]).astype(BF16)
        q = dot(n, w_q[...]).astype(BF16).astype(F32).T
        for h in range(QHEADS):
            head = turn(head_norm(q[h * HEAD : (h + 1) * HEAD], q_gain), at, 256)
            qs[h * HEAD : (h + 1) * HEAD, i * 256 : (i + 1) * 256] = head.astype(BF16) * scale
    for ref, at in ((low, 0), (high, WINDOW + ROWS)):
        tiles = [ref[EDGE:, k * 128 : (k + 1) * 128] for k in range(WIDTH // 128)]
        keys_values(jnp.concatenate(tiles, axis=0), at, WINDOW)


def attend_kernel(sink, qs, ks, vs, attn_ref, even_mask, odd_mask, even, odd):
    reach = 3 * WINDOW
    pairs = ROWS // WINDOW // 2
    jj = lax.broadcasted_iota(jnp.int32, (reach, WINDOW), 0)
    ii = lax.broadcasted_iota(jnp.int32, (reach, WINDOW), 1)
    band = (jj >= ii) & (jj <= ii + 2 * WINDOW)
    first = lax.axis_index(SP) * ROWS - WINDOW

    def set_mask(mask, j):
        position = jj + (first + j * WINDOW)
        mask[...] = jnp.where(band & (position >= 0) & (position < SEQ), 0.0, NEG_FILL)

    def scores(j, out):
        here = pl.multiple_of(j * WINDOW, 128)
        qb = jnp.concatenate(
            [qs[h * HEAD : (h + 1) * HEAD, pl.ds(here, WINDOW)] for h in range(QHEADS)], axis=1
        )
        out[...] = dot_tn(ks[:, pl.ds(here, reach)], qb)

    def outputs(j, mask, saved):
        here = pl.multiple_of(j * WINDOW, 128)
        weights = []
        for h in range(QHEADS):
            s = saved[:, h * WINDOW : (h + 1) * WINDOW] + mask[...]
            top = jnp.maximum(jnp.max(s, axis=0, keepdims=True), sink[h])
            p = jnp.exp(s - top)
            scale = 1.0 / (jnp.sum(p, axis=0, keepdims=True) + jnp.exp(sink[h] - top))
            weights.append((p * scale).astype(BF16))
        o = dot(vs[:, pl.ds(here, reach)], jnp.concatenate(weights, axis=1))
        o = jnp.concatenate([o[:, h * WINDOW : (h + 1) * WINDOW] for h in range(QHEADS)], axis=0)
        attn_ref[pl.ds(here, WINDOW), :] = o.T.astype(BF16)

    set_mask(even_mask, 0)
    set_mask(odd_mask, 1)
    scores(0, even)

    def pair(i, _):
        @pl.when(i == 1)
        def _():
            set_mask(even_mask, 2)

        @pl.when(i == pairs - 1)
        def _():
            set_mask(odd_mask, 2 * pairs - 1)

        scores(2 * i + 1, odd)
        outputs(2 * i, even_mask, even)
        scores(jnp.minimum(2 * i + 2, 2 * pairs - 1), even)
        outputs(2 * i + 1, odd_mask, odd)
        return 0

    lax.fori_loop(0, pairs, pair, 0)


def mixer_kernel(x_ref, b_ref, c_ref, cum_ref, step_ref, enter_ref, back_ref, spread, y_ref, state):
    state[...] = jnp.zeros_like(state)
    tt = lax.broadcasted_iota(jnp.int32, (CHUNK, CHUNK), 0)
    ss = lax.broadcasted_iota(jnp.int32, (CHUNK, CHUNK), 1)
    below, same, left = tt > ss, tt == ss, ss < HEAD
    nothing = jnp.zeros((CHUNK, CHUNK), BF16)

    def chunk(i, _):
        k = CHUNKS - 1 - i
        at = pl.ds(pl.multiple_of(k * CHUNK, 128), CHUNK)
        c = c_ref[at, :]
        scores = dot_nt(c, b_ref[at, :])
        cum = cum_ref[:, at]
        step = step_ref[:, at]
        f, r = cum[:HEADS], cum[HEADS:]
        sf, sr = step[:HEADS], step[HEADS:]
        row_f = jnp.log(sf) - f
        row_r = jnp.log(sr) - r
        row_d = jnp.log(sf + sr)
        columns = cum.T

        def weights(h):
            lower = columns[:, h : h + 1] + row_f[h : h + 1]
            upper = columns[:, HEADS + h : HEADS + h + 1] + row_r[h : h + 1]
            power = jnp.where(below, lower, jnp.where(same, row_d[h : h + 1], upper))
            return (jnp.exp(power) * scores).astype(BF16)

        wide = widen(jnp.concatenate([jnp.exp(f), jnp.exp(r)], axis=1), spread[...])
        across = wide[:CHUNK] * dot(c, enter_ref[k])
        across = across + wide[CHUNK:] * dot(c, state[...].astype(BF16))
        for pair in range(HEADS // 2):
            cols = slice(pair * 2 * HEAD, (pair + 1) * 2 * HEAD)
            both = jnp.concatenate([weights(2 * pair), weights(2 * pair + 1)], axis=1)
            xp = x_ref[at, cols]
            stacked = jnp.concatenate(
                [jnp.where(left, xp, nothing), jnp.where(left, nothing, xp)], axis=0
            )
            y_ref[at, cols] = dot(both, stacked) + across[:, cols]
        state[...] = state[...] * wide[CHUNK : CHUNK + 1] + back_ref[k].astype(F32)
        return 0

    lax.fori_loop(0, CHUNKS, chunk, 0)


def finish_rows(core, y, c, run, gate, attn, gain, spread, from_low, from_high, out):
    scales = lane_row(gain)
    for i in range(LINE):
        at = pl.ds(pl.multiple_of(i * 256 + core * 128, 128), 128)
        cm = c[at, :]
        reach = jnp.exp(run[:, at])
        wide = widen(jnp.concatenate([reach[:HEADS], reach[HEADS:]], axis=1), spread[...])
        v = y[at, :] + wide[:128] * dot(cm, from_low[...]) + wide[128:] * dot(cm, from_high[...])
        v = v * silu(gate[at, :].astype(F32))
        mean = jnp.mean(v * v, axis=-1, keepdims=True)
        out[i, :, : QHEADS * HEAD] = attn[at, :]
        out[i, :, QHEADS * HEAD :] = (v * lax.rsqrt(mean + NORM_EPS) * scales).astype(BF16)


def theirs_kernel(
    part, d1, d2, d3, y, c, run, gate, attn, gain, spread, theirs, from_low, from_high
):
    got = (None, d1, d2, d3)
    level = lax.axis_index("z")
    for back, keep in ((0, from_low), (1, from_high)):
        count = level if back == 0 else LINE - 1 - level
        prefix = jnp.zeros((STATE, INNER), F32)
        log_prefix = jnp.zeros((1, INNER), F32)
        for d in range(1, LINE):
            r = got[d if back == 0 else LINE - d]
            live = d <= count
            weight = jnp.where(live, jnp.exp(log_prefix), 0.0)
            prefix = prefix + weight * r[:STATE, :].astype(F32)
            tail = r[STATE:, :].astype(F32)
            log = tail[0:1] + tail[1:2] + tail[2:3]
            log_prefix = log_prefix + jnp.where(live, log, 0.0)
        own = part[STATE * back : STATE * (back + 1), :]
        reach = jnp.exp(part[2 * STATE + back : 2 * STATE + back + 1, :])
        keep[...] = (own + reach * prefix).astype(BF16)
    core = 1 - lax.axis_index("c")
    finish_rows(core, y, c, run, gate, attn, gain, spread, from_low, from_high, theirs)


def mine_kernel(y, c, run, gate, attn, gain, spread, from_low, from_high, wa, ws, mine, first):
    finish_rows(lax.axis_index("c"), y, c, run, gate, attn, gain, spread, from_low, from_high, mine)
    first[...] = partial(mine[(lax.axis_index("x") + 2) % LINE], wa, ws)


def sum_kernel(own, direct_right, direct_left, last_right, last_left, out):
    upper = own[:HALVES] + direct_left[...].astype(F32) + last_right[...].astype(F32)
    lower = own[HALVES:] + direct_right[...].astype(F32) + last_left[...].astype(F32)
    out[:HALVES] = upper.astype(BF16)
    out[HALVES:] = lower.astype(BF16)


def partial(v, a, b):
    split = QHEADS * HEAD
    return (dot(v[:, :split], a[...]) + dot(v[:, split:], b[...])).astype(BF16).astype(F32)


def chunk_partial(order, mine, theirs, wa, ws, pa, ps):
    join = lambda ref: jnp.concatenate([ref[index] for index in order], axis=0)
    return partial(join(mine), wa, ws) + partial(join(theirs), pa, ps)


HALVES = 64


def opposite_kernel(first, theirs, pa, ps, right, left):
    value = first[...] + partial(theirs[(lax.axis_index("x") + 2) % LINE], pa, ps)
    right[...] = value[:HALVES].astype(BF16)
    left[...] = value[HALVES:].astype(BF16)


def beside_kernel(mine, theirs, wa, ws, pa, ps, right, left, keep_right, keep_left, own):
    x = lax.axis_index("x")
    order = [(x + 1) % LINE, (x + 3) % LINE, x]
    value = chunk_partial(order, mine, theirs, wa, ws, pa, ps)
    keep_right[...] = value[:HALVES]
    right[...] = value[HALVES : 2 * HALVES].astype(BF16)
    left[...] = value[2 * HALVES : 3 * HALVES].astype(BF16)
    keep_left[...] = value[3 * HALVES : 4 * HALVES]
    own[...] = value[4 * HALVES :]


HBM = pl.BlockSpec(memory_space=pltpu.HBM)


def whole(count):
    return [pl.BlockSpec(memory_space=pltpu.VMEM)] * count


SCALARS = pl.BlockSpec(memory_space=pltpu.SMEM)


def plain(kernel, name, inputs, outs, scalars=0, remote=0, scratch=(), size=8, flops=1e9):
    return pl.pallas_call(
        kernel,
        in_specs=[SCALARS] * scalars + whole(inputs) + [HBM] * remote,
        out_specs=whole(len(outs)),
        out_shape=outs,
        scratch_shapes=list(scratch),
        compiler_params=pltpu.CompilerParams(vmem_limit_bytes=size << 20),
        cost_estimate=cost(flops),
        name=name,
    )


def fixed(shape):
    return pl.BlockSpec(memory_space=pltpu.VMEM)


def params(size):
    return pltpu.CompilerParams(dimension_semantics=("arbitrary",), vmem_limit_bytes=size << 20)


def cost(flops):
    return pl.CostEstimate(flops=int(flops), transcendentals=0, bytes_accessed=8 << 20)


def shaped(shape, dtype):
    return jax.ShapeDtypeStruct(shape, dtype)


def local(
    tokens, norm_gain, query_weight, key_weight, value_weight, query_gain, key_gain, sink_logit,
    gate_weight, inner_weight, input_map, output_map, step_weight, conv_inner, conv_pair,
    decay_rate, decay_jump, inner_gain, attn_out_weight, ssm_out_weight,
):
    up = [(k, k + 1) for k in range(15)]
    down = [(k + 1, k) for k in range(15)]
    swap = [(0, 1), (1, 0)]
    pin = lambda v: pltpu.with_memory_space_constraint(v, pltpu.HBM)
    gain = norm_gain.reshape(WIDTH // 128, 128)
    halo = shaped((EDGE + 8, WIDTH), BF16)
    edge_low, edge_high = plain(
        edge_kernel, "edge", 0, [halo, halo], remote=4,
        scratch=[
            pltpu.VMEM((2 * WINDOW, WIDTH), BF16), pltpu.VMEM((2 * HEAD, WIDTH), BF16),
            pltpu.VMEM((WIDTH // 128, 128), BF16), pltpu.SemaphoreType.DMA((5,)),
        ],
        size=6, flops=1e10,
    )(*map(pin, (gain, tokens, key_weight.T, value_weight.T)))
    halo_low = lax.ppermute(edge_low, SP, up)
    halo_high = lax.ppermute(edge_high, SP, down)

    spread = jnp.asarray(head_spread(), BF16)
    step_rows = jnp.transpose(step_weight, (1, 2, 0)).reshape(2 * HEADS, WIDTH)
    jump = jnp.transpose(decay_jump, (1, 2, 0)).reshape(2 * HEADS, ROWS)
    normed, rows, raw, w_gate, w_q, w_kv = plain(
        front_kernel, "front", 5,
        [
            shaped((ROWS, WIDTH), BF16), shaped((CONV // STATE, ROWS, STATE), F32),
            shaped((2 * HEADS, ROWS), F32), shaped((WIDTH, INNER), BF16),
            shaped((WIDTH, QHEADS * HEAD), BF16), shaped((2 * HEAD, WIDTH), BF16),
        ],
        remote=5,
        scratch=[pltpu.VMEM((2 * HEADS, WIDTH), BF16), pltpu.SemaphoreType.DMA((9,))],
        size=8, flops=10e9,
    )(gain, inner_weight, input_map, output_map, tokens, *map(pin, (step_rows, gate_weight, query_weight,
      key_weight.T, value_weight.T)))

    x, b, c, cum, step, run, enter, back, state = plain(
        state_kernel, "state", 12,
        [
            shaped((ROWS, INNER), BF16), shaped((ROWS, STATE), BF16),
            shaped((ROWS, STATE), BF16), shaped((2 * HEADS, ROWS), F32),
            shaped((2 * HEADS, ROWS), F32), shaped((2 * HEADS, ROWS), F32),
            shaped((CHUNKS, STATE, INNER), BF16), shaped((CHUNKS, STATE, INNER), BF16),
            shaped((PACK, INNER), BF16),
        ],
        scalars=1,
        scratch=[pltpu.VMEM((CONV // STATE, CHUNK + 2 * EDGE, STATE), F32)] * 2
        + [pltpu.VMEM((STATE, INNER), F32)] * 2,
        size=8, flops=6e9,
    )(decay_rate, rows, raw, halo_low, halo_high, gain, inner_weight, input_map, output_map, conv_inner, conv_pair,
      jump, spread)

    def along(values, axis):
        sent = {
            d: lax.ppermute(values[d - 1], axis, [(k, (k + d) % LINE) for k in range(LINE)])
            for d in (1, 3, 2)
        }
        return [sent[d] for d in (1, 2, 3)]

    got = along([state] * 3, "y")

    near, far = rope_tables()
    gate, qs, ks, vs = plain(
        heads_kernel, "heads", 10,
        [
            shaped((ROWS, INNER), BF16), shaped((QHEADS * HEAD, ROWS), BF16), shaped((HEAD, ROWS + 2 * WINDOW), BF16),
            shaped((HEAD, ROWS + 2 * WINDOW), BF16),
        ],
        size=6, flops=7e9,
    )(normed, halo_low, halo_high, w_gate, w_q, w_kv, query_gain[None, :], key_gain[None, :],
      jnp.asarray(near), jnp.asarray(far))

    *messages, part = plain(
        line_kernel, "line", 4,
        [shaped((STATE + 16, INNER), BF16)] * 3 + [shaped((PACK, INNER), F32)],
        size=4, flops=1e9,
    )(state, *got[::-1])

    far_got = along(messages, "z")

    attn = plain(
        attend_kernel, "attend", 3, [shaped((ROWS, QHEADS * HEAD), BF16)], scalars=1,
        scratch=[pltpu.VMEM((3 * WINDOW, WINDOW), F32)] * 2
        + [pltpu.VMEM((3 * WINDOW, QHEADS * WINDOW), F32)] * 2,
        size=8, flops=7e9,
    )(sink_logit, qs, ks, vs)[0]

    y = plain(
        mixer_kernel, "mixer", 8, [shaped((ROWS, INNER), F32)],
        scratch=[pltpu.VMEM((STATE, INNER), F32)], flops=10e9,
    )(x, b, c, cum, step, enter, back, spread)[0]

    attn_own, ssm_own, y = lax.optimization_barrier((attn_out_weight, ssm_out_weight, y))
    attn_partner = lax.ppermute(attn_own, "c", swap)
    ssm_partner = lax.ppermute(ssm_own, "c", swap)

    depth = QHEADS * HEAD + INNER
    rest = (y, c, run, gate, attn, inner_gain.reshape(INNER // 128, 128), spread)
    incoming = shaped((STATE, INNER), BF16)
    theirs, from_low, from_high = plain(
        theirs_kernel, "theirs", 11, [shaped((4, 128, depth), BF16), incoming, incoming], flops=2e9
    )(part, *far_got, *rest)
    theirs = lax.ppermute(theirs, "c", swap)
    mine, first = plain(
        mine_kernel, "mine", 11, [shaped((4, 128, depth), BF16), shaped((128, WIDTH), F32)], flops=2e9
    )(*rest, from_low, from_high, attn_out_weight, ssm_out_weight)
    operands = (
        mine, theirs, attn_out_weight, ssm_out_weight, attn_partner, ssm_partner
    )
    sent = shaped((HALVES, WIDTH), BF16)
    kept = shaped((HALVES, WIDTH), F32)
    right = [(k, (k + 1) % LINE) for k in range(LINE)]
    left = [((k + 1) % LINE, k) for k in range(LINE)]
    shift_right = lambda value: lax.ppermute(value, "x", right)
    shift_left = lambda value: lax.ppermute(value, "x", left)
    relay_right, relay_left = plain(
        opposite_kernel, "opposite", 4, [sent, sent], flops=1e9
    )(first, theirs, attn_partner, ssm_partner)
    relay_right = shift_right(relay_right)
    relay_left = shift_left(relay_left)
    direct_right, direct_left, keep_right, keep_left, own = plain(
        beside_kernel, "beside", 6, [sent, sent, kept, kept, shaped((2 * HALVES, WIDTH), F32)],
        flops=3e9,
    )(*operands)
    direct_right = shift_right(direct_right)
    direct_left = shift_left(direct_left)
    last_right = shift_right((keep_right + relay_right.astype(F32)).astype(BF16))
    last_left = shift_left((keep_left + relay_left.astype(F32)).astype(BF16))
    return plain(
        sum_kernel, "sum", 5, [shaped((2 * HALVES, WIDTH), BF16)], size=4, flops=1e6
    )(own, direct_right, direct_left, last_right, last_left)[0]


def solution(mesh):
    split = Mesh(mesh.devices.reshape(4, 4, 4, 2), SP_TP)
    tp = ("x", "c")
    placed = (
        P(SP, None), P(), P(None, tp), P(None, tp), P(None, tp), P(), P(), P(tp),
        P(None, tp), P(None, tp), P(None, tp), P(None, tp), P(None, None, tp), P(None, tp),
        P(None, None, tp), P(None, tp), P(SP, None, tp), P(tp), P(tp, None), P(tp, None),
    )
    return jax.shard_map(
        local, mesh=split, in_specs=placed, out_specs=P(SP_TP, None), check_vma=False
    )
```
